32 devices in a mesh: ep: 8 (over z, core), tp: 4 (over y, x).
Axes of the slice: x: 2, y: 2, z: 4, core: 2. Of those that a mesh axis runs over, the one named last changes fastest.
Arguments:
- mix_rows: bfloat16 [2048, 2048], P('ep', 'tp'), may hold values from -6 to 6
- mix_gain: bfloat16 [2048], replicated, may hold values from 0.099609375 to 1.8984375
- w_query: bfloat16 [2048, 2048], P(None, 'tp'), may hold values from -0.125 to 0.125
- w_forget: bfloat16 [2048, 2048], P(None, 'tp'), may hold values from -0.125 to 0.125
- w_input: bfloat16 [2048, 2048], P(None, 'tp'), may hold values from -0.125 to 0.125
- w_outgate: bfloat16 [2048, 2048], P(None, 'tp'), may hold values from -0.125 to 0.125
- forget_gap: float32 [2048], P('tp'), may hold values from 1e-05 to 0.1
- decay_extra: float32 [16, 2048], P('tp', 'ep'), may hold values from -0.7 to 0, as said below
- head_gain: bfloat16 [128], replicated, may hold values from 0.099609375 to 1.8984375
- w_mixout: bfloat16 [2048, 2048], P('tp'), may hold values from -0.125 to 0.125
- moe_rows: bfloat16 [2048, 2048], P('ep', 'tp'), may hold values from -6 to 6
- moe_gain: bfloat16 [2048], replicated, may hold values from 0.099609375 to 1.8984375
- route_ids: int32 [2048, 2], P('ep'), may hold values from 0 to 7, all different within a row; in each aligned block of 256 rows (0 to 255, 256 to 511, ...) at most 96 rows name the same one
- route_scores: float32 [2048, 2], P('ep'), may hold values from 0.05 to 1
- w_gate: bfloat16 [8, 2048, 3072], P('ep', None, 'tp'), may hold values from -0.125 to 0.125
- w_up: bfloat16 [8, 2048, 3072], P('ep', None, 'tp'), may hold values from -0.125 to 0.125
- w_down: bfloat16 [8, 3072, 2048], P('ep', 'tp'), may hold values from -0.109375 to 0.109375
Outputs:
- mix_out: bfloat16 [2048, 2048], P('ep', 'tp')
- moe_out: bfloat16 [2048, 2048], P('ep', 'tp')
The draws below stay inside these ranges and needn't reach their ends.
Inputs may be any that keep to these rules, and one draw needn't show every extreme that they name: `route_ids`: each row names 2 different experts. Among the rows of one index of ep at most 96 name the same expert, a bound that at least one block reaches. `decay_extra`: never positive.
All inputs are finite; a program needn't handle non-finite values.
Results may differ from the reference program's by a relative error of at most 0.017.
Values may be sent and summed in bfloat16 or wider, within the bound.
A program may use at most 64 MiB of HBM per device.

```python
import math
import jax
import jax.numpy as jnp
import numpy as np
from jax import lax

HEADS = 16
HEAD_DIM = 128
D = 2048
FFE = 3072
EXPERTS = 8
TOP_K = 2
BLOCK = 64
TOK_A = 256
TOK_B = 256
TOKENS_A = 2048
TOKENS_B = 2048
CAP = 96
N_EP = 8
N_TP = 4


def draw_forget_gap(key, part):
    lowest, highest = (1e-05, 0.1)
    unit = jax.random.uniform(key, (D,), jnp.float32)
    return jnp.exp(jnp.log(lowest) + unit * (jnp.log(highest) - jnp.log(lowest)))


def draw_decay_extra(key, part):
    rate_key, spot_key, depth_key = jax.random.split(key, 3)
    lowest, highest = (1e-05, 0.0001)
    block_list = TOKENS_A // TOK_A
    unit = jax.random.uniform(rate_key, (HEADS, block_list, 1), jnp.float32)
    rate = jnp.exp(jnp.log(lowest) + unit * (jnp.log(highest) - jnp.log(lowest)))
    steady = jnp.broadcast_to(-rate, (HEADS, block_list, TOK_A)).reshape(HEADS, TOKENS_A)
    spots = jax.random.randint(spot_key, (3,), 0, TOKENS_A)
    marked = jnp.any(jnp.arange(TOKENS_A)[None, :] == spots[:, None], axis=0)
    depth = jnp.log(jax.random.uniform(depth_key, (HEADS, TOKENS_A), jnp.float32, 0.5, 0.8))
    return steady + jnp.where(marked[None, :], depth, 0.0)


def block_scale(rng, extent, cuts, smallest, largest):
    factor_of = 1.0
    for position, shards_of in cuts:
        draws = jax.random.uniform(jax.random.fold_in(jax.random.fold_in(rng, 6), position), (shards_of,), jnp.float32, smallest / len(cuts), largest / len(cuts))
        factor_of = factor_of * jnp.repeat(jnp.exp(draws), extent[position] // shards_of).reshape((-1,) + (1,) * (len(extent) - 1 - position))
    return factor_of


def assign_block(key, own, number, rows, amount, top, limit, skew):
    ranking = jax.random.permutation(key, amount)
    crowded, common = load_shares(amount, rows * top, limit, skew, True), load_shares(amount, rows * top, limit, skew, False)
    places = jnp.arange(amount)

    def named(tallies, offset_by):
        used = int((tallies > 0).sum())
        fixed = max(1, used // 4)
        moved = fixed + (places - fixed + offset_by * (used - fixed)) % max(1, amount - fixed)
        return jnp.zeros((amount,), jnp.int32).at[ranking[jnp.where(places < fixed, places, moved)]].set(jnp.asarray(tallies, jnp.int32))

    tallies = jnp.where(number % 4 == 0, named(crowded, number // 4), named(common, number - number // 4 - 1))
    mixed = jax.random.permutation(jax.random.fold_in(own, 3), amount)
    source_of, taker = mixed[0:amount // 2 * 2:2], mixed[1:amount // 2 * 2:2]
    margin = jnp.minimum(tallies[source_of] - 1, limit - tallies[taker]) // 2
    margin = jnp.where((source_of == ranking[0]) | (taker == ranking[0]) | (tallies[taker] == 0), 0, jnp.maximum(margin, 0))
    moved = jax.random.randint(jax.random.fold_in(own, 4), (amount // 2,), 0, 1 << 20) % (margin + 1)
    tallies = tallies.at[source_of].add(-moved).at[taker].add(moved)
    members = jnp.searchsorted(jnp.cumsum(tallies), jnp.arange(rows * top), side="right").astype(jnp.int32)
    table = members.reshape(top, rows).T
    table = table[jax.random.permutation(jax.random.fold_in(own, 1), rows)]
    offset_by = jax.random.randint(jax.random.fold_in(own, 2), (rows, 1), 0, top)
    return jnp.take_along_axis(table, (jnp.arange(top)[None, :] + offset_by) % top, axis=1)


def load_shares(count, total, limit, skew, full):
    portions = [(1 << 20) // math.isqrt(standing ** skew) + 1 for standing in range(1, count + 1)]
    largest = limit if full else min(limit, max(-(-total // count), total * portions[0] // sum(portions)))
    least = 1 if total - largest >= count - 1 else 0
    counts, surplus = [largest] + [least] * (count - 1), total - largest - least * (count - 1)
    while surplus > 0:
        candidates = [i for i in range(1, count) if counts[i] < largest] or [i for i in range(1, count) if counts[i] < limit]
        mass, remaining = sum([portions[i] for i in candidates]), surplus
        for i in candidates:
            addition = min(limit - counts[i], max(1, remaining * portions[i] // mass), surplus)
            counts[i] = counts[i] + addition
            surplus = surplus - addition
    return np.array(counts)


def bell_draw(stream_key, extent, scale, bound, shards=(), held_as=jnp.bfloat16):
    loudness = block_scale(stream_key, extent, shards, -0.22, 0.18) if shards else 1.0
    drawn = jax.random.normal(stream_key, extent, jnp.float32) * scale * loudness
    return jnp.minimum(jnp.maximum(drawn, -bound), bound).astype(held_as)


def setup_inputs(seed: int = 0) -> dict:
    splits = jax.random.split(jax.random.key(seed), 18)
    mix_rows = bell_draw(splits[0], (TOKENS_A, D), 1.0, 6.0, ((0, 8), (1, 4)))
    mix_gain = jnp.clip(1.0 + 0.18 * jax.random.normal(splits[1], (D,), jnp.float32), 0.099609375, 1.8984375).astype(jnp.bfloat16)
    w_query = bell_draw(splits[2], (D, D), D ** -0.5, 0.125, ((1, 4),))
    w_forget = bell_draw(splits[3], (D, D), D ** -0.5, 0.125, ((1, 4),))
    w_input = bell_draw(splits[4], (D, D), D ** -0.5, 0.125, ((1, 4),))
    w_outgate = bell_draw(splits[5], (D, D), D ** -0.5, 0.125, ((1, 4),))
    forget_gap = draw_forget_gap(jax.random.fold_in(splits[17], 71), 0)
    decay_extra = draw_decay_extra(jax.random.fold_in(splits[17], 71), 0)
    head_gain = jnp.clip(1.0 + 0.18 * jax.random.normal(splits[8], (HEAD_DIM,), jnp.float32), 0.099609375, 1.8984375).astype(jnp.bfloat16)
    w_mixout = bell_draw(splits[9], (D, D), D ** -0.5, 0.125, ((0, 4),))
    moe_rows = bell_draw(splits[10], (TOKENS_B, D), 1.0, 6.0, ((0, 8), (1, 4)))
    moe_gain = jnp.clip(1.0 + 0.18 * jax.random.normal(splits[11], (D,), jnp.float32), 0.099609375, 1.8984375).astype(jnp.bfloat16)
    route_ids_keys = jax.random.split(jax.random.fold_in(splits[12], 1), TOKENS_B // TOK_B)
    route_ids_turns = jax.random.permutation(jax.random.fold_in(splits[12], 3), TOKENS_B // TOK_B)
    route_ids = jax.vmap(lambda own, number: assign_block(jax.random.fold_in(splits[12], 2), own, number, TOK_B, EXPERTS, TOP_K, CAP, 1))(route_ids_keys, route_ids_turns).reshape((TOKENS_B, TOP_K))
    route_scores = jnp.clip(0.05 + 0.95 * jax.random.uniform(splits[13], (TOKENS_B, TOP_K), jnp.float32) ** block_scale(splits[13], (TOKENS_B, TOP_K), ((0, 8),), -0.2, 0.2), 0.05, 1.0)
    w_gate = bell_draw(splits[14], (EXPERTS, D, FFE), D ** -0.5, 0.125, ((0, 8), (2, 4)))
    w_up = bell_draw(splits[15], (EXPERTS, D, FFE), D ** -0.5, 0.125, ((0, 8), (2, 4)))
    w_down = bell_draw(splits[16], (EXPERTS, FFE, D), FFE ** -0.5, 0.109375, ((0, 8), (1, 4)))
    return dict(mix_rows=mix_rows, mix_gain=mix_gain, w_query=w_query, w_forget=w_forget, w_input=w_input, w_outgate=w_outgate, forget_gap=forget_gap, decay_extra=decay_extra, head_gain=head_gain, w_mixout=w_mixout, moe_rows=moe_rows, moe_gain=moe_gain, route_ids=route_ids, route_scores=route_scores, w_gate=w_gate, w_up=w_up, w_down=w_down)


epsilon = 1e-06
HIGHEST_PRECISION = lax.Precision.HIGHEST

def rms_scale(rows, gain):
    values = rows.astype(jnp.float32)
    scale = lax.rsqrt(lax.optimization_barrier(jnp.mean(values * values, axis=-1, keepdims=True)) + epsilon)
    return values * scale * gain.astype(jnp.float32)

def block_recurrence(query_rows, key_in, value, log_forget, state):
    heads_count, length, key_dim = query_rows.shape
    block_list = length // BLOCK

    def split(values):
        return jnp.moveaxis(values.reshape(heads_count, block_list, BLOCK, values.shape[2]), 1, 0)
    causal = jnp.tril(jnp.ones((BLOCK, BLOCK), dtype=bool))[:, :, None]

    def advance(carry, inputs):
        query_block, key_block, value_block, forget_block = inputs
        running_state = jnp.cumsum(forget_block, axis=1)
        spread = running_state[:, :, None, :] - running_state[:, None, :, :]
        decay = jnp.exp(jnp.where(causal, spread, -jnp.inf))
        scores = jnp.einsum('hid,hjd,hijd->hij', query_block, key_block, decay, precision=HIGHEST_PRECISION)
        output = jnp.einsum('hid,hde->hie', query_block * jnp.exp(running_state), carry, precision=HIGHEST_PRECISION)
        output = output + jnp.einsum('hij,hje->hie', scores, value_block, precision=HIGHEST_PRECISION)
        last = running_state[:, -1:, :]
        carry = carry * jnp.exp(last)[:, 0, :, None] + jnp.einsum('hjd,hje->hde', key_block * jnp.exp(last - running_state), value_block, precision=HIGHEST_PRECISION)
        return (carry, output)
    carry, outputs = lax.scan(advance, state, (split(query_rows), split(key_in), split(value), split(log_forget)))
    return (jnp.moveaxis(outputs, 0, 1).reshape(heads_count, length, value.shape[2]), carry)

def token_mixer(mix_rows, mix_gain, w_query, w_forget, w_input, w_outgate, forget_gap, decay_extra, head_gain, w_mixout):
    normed = rms_scale(mix_rows, mix_gain).astype(jnp.bfloat16)
    length = normed.shape[0]
    query_preactivation = jnp.dot(normed, w_query, preferred_element_type=jnp.float32)
    forget_pre = jnp.dot(normed, w_forget, preferred_element_type=jnp.float32)
    input_pre = jnp.dot(normed, w_input, preferred_element_type=jnp.float32)
    outgate_pre = jnp.dot(normed, w_outgate, preferred_element_type=jnp.float32)

    def heads(values):
        return values.reshape(length, HEADS, HEAD_DIM).transpose(1, 0, 2)
    query_rows = heads(jax.nn.silu(query_preactivation))
    key_in = heads(forget_gap.astype(jnp.float32) * jax.nn.sigmoid(-forget_pre))
    value = heads(input_pre)
    log_forget = jnp.log1p(-key_in) + decay_extra.astype(jnp.float32)[:, :, None]
    start_state = jnp.zeros((HEADS, HEAD_DIM, HEAD_DIM), jnp.float32)
    head_out, _ = block_recurrence(query_rows, key_in, value, log_forget, start_state)
    gated = rms_scale(head_out, head_gain) * heads(jax.nn.silu(outgate_pre))
    gated = gated.transpose(1, 0, 2).reshape(length, D).astype(jnp.bfloat16)
    group = D // N_TP
    total = jnp.zeros((length, D), jnp.float32)
    for index in range(N_TP):
        part = jnp.dot(gated[:, index * group:(index + 1) * group], w_mixout[index * group:(index + 1) * group], preferred_element_type=jnp.float32)
        total = total + lax.optimization_barrier(part.astype(jnp.bfloat16)).astype(jnp.float32)
    return total.astype(jnp.bfloat16)

def expert_layer(moe_rows, moe_gain, route_ids, route_scores, w_gate, w_up, w_down):
    row_total, top_count = route_ids.shape
    expert_count = w_gate.shape[0]
    normed = rms_scale(moe_rows, moe_gain).astype(jnp.bfloat16)
    weights = route_scores / lax.optimization_barrier(jnp.sum(route_scores, axis=1, keepdims=True))
    grouped = route_ids.reshape(N_EP, TOK_B * top_count).astype(jnp.int32)
    onehot = (grouped[:, :, None] == jnp.arange(expert_count, dtype=jnp.int32)[None, None, :]).astype(jnp.int32)
    rank = lax.optimization_barrier(jnp.sum((jnp.cumsum(onehot, axis=1) - 1) * onehot, axis=2)).astype(jnp.int32)
    source = jnp.arange(N_EP, dtype=jnp.int32)[:, None]
    place = (grouped * (N_EP * CAP) + source * CAP + rank).reshape(-1).astype(jnp.int32)
    token = (jnp.arange(row_total * top_count, dtype=jnp.int32) // top_count).astype(jnp.int32)
    table = jnp.full((expert_count * N_EP * CAP,), row_total, jnp.int32).at[place].set(token)
    padded = jnp.concatenate([normed, jnp.zeros((1, D), jnp.bfloat16)], axis=0)
    slots = padded[table].reshape(expert_count, N_EP * CAP, D)
    width = FFE // N_TP

    def one_expert(operands):
        rows, gate_weight, up_weight, down_weight = operands
        gate_acts = jnp.dot(rows, gate_weight, preferred_element_type=jnp.float32)
        up_acts = jnp.dot(rows, up_weight, preferred_element_type=jnp.float32)
        hidden = (jax.nn.silu(gate_acts) * up_acts).astype(jnp.bfloat16)
        total = jnp.zeros((rows.shape[0], D), jnp.float32)
        for index in range(N_TP):
            part = jnp.dot(hidden[:, index * width:(index + 1) * width], down_weight[index * width:(index + 1) * width], preferred_element_type=jnp.float32)
            total = total + lax.optimization_barrier(part.astype(jnp.bfloat16)).astype(jnp.float32)
        return total.astype(jnp.bfloat16)
    results = lax.map(one_expert, (slots, w_gate, w_up, w_down)).reshape(-1, D)
    picked = results[place].astype(jnp.float32).reshape(row_total, top_count, D)
    return lax.optimization_barrier(jnp.sum(picked * weights[:, :, None], axis=1)).astype(jnp.bfloat16)

def reference(mix_rows, mix_gain, w_query, w_forget, w_input, w_outgate, forget_gap, decay_extra, head_gain, w_mixout, moe_rows, moe_gain, route_ids, route_scores, w_gate, w_up, w_down):
    mix_out = token_mixer(mix_rows, mix_gain, w_query, w_forget, w_input, w_outgate, forget_gap, decay_extra, head_gain, w_mixout)
    moe_out = expert_layer(moe_rows, moe_gain, route_ids, route_scores, w_gate, w_up, w_down)
    return (mix_out, moe_out)
```

```python
import functools

import jax
import jax.numpy as jnp
from jax import lax
from jax.experimental import pallas as pl
from jax.experimental.pallas import tpu as pltpu
from jax.sharding import PartitionSpec as P

BLOCK = 64
epsilon = 1e-06
F32 = jnp.float32
BF16 = jnp.bfloat16
VMEM = pl.BlockSpec(memory_space=pltpu.VMEM)
LIMIT = 60 * 1024 * 1024


def dot(a, b, dims=((1,), (0,)), precision=None):
    return lax.dot_general(a, b, (dims, ((), ())), precision=precision, preferred_element_type=F32)


def sigmoid(x):
    return 1.0 / (1.0 + jnp.exp(-x))


def iota(shape, dim):
    return lax.broadcasted_iota(jnp.int32, shape, dim)


def mixer_kernel(per, x_ref, gain_ref, wq_ref, wf_ref, wi_ref, wo_ref, gap_ref, dec_ref,
                 lo_ref, qd_ref, og_ref, st_ref, normed):
    step = pl.program_id(0)
    length = normed.shape[0]
    dim = st_ref.shape[2]
    parts, _, cols = x_ref.shape

    @pl.when(step == 0)
    def _():
        total = jnp.zeros((length, 1), F32)
        for p in range(parts):
            v = x_ref[p].astype(F32)
            total += jnp.sum(v * v, axis=1, keepdims=True)
        scale = lax.rsqrt(total / (parts * cols) + epsilon)
        for p in range(parts):
            g = gain_ref[:, p * cols:(p + 1) * cols].astype(F32)
            normed[:, p * cols:(p + 1) * cols] = (x_ref[p].astype(F32) * scale * g).astype(BF16)

    n = normed[...]
    qp = dot(n, wq_ref[...])
    fp = dot(n, wf_ref[...])
    value = dot(n, wi_ref[...]).astype(BF16)
    op = dot(n, wo_ref[...])
    query = qp * sigmoid(qp)
    key = gap_ref[...] * sigmoid(-fp)
    og_ref[...] = op * sigmoid(op)
    logs = jnp.log1p(-key)
    dec = dec_ref[...]
    tri = (iota((length, length), 0) >= iota((length, length), 1)).astype(F32)
    causal = iota((BLOCK, BLOCK), 0) >= iota((BLOCK, BLOCK), 1)
    half = BLOCK // 2
    for j in range(per):
        c = slice(j * dim, (j + 1) * dim)
        extra = jnp.sum(jnp.where(iota(dec.shape, 1) == step * per + j, dec, 0.0), axis=1, keepdims=True)
        run = dot(tri, logs[:, c] + extra, precision=lax.Precision.HIGHEST)
        q, k, v = query[:, c], key[:, c], value[:, c]
        qd_ref[:, c] = (q * jnp.exp(run)).astype(BF16)
        state = jnp.zeros((dim, dim), F32)
        base = jnp.zeros((1, dim), F32)
        for b in range(length // BLOCK):
            r = slice(b * BLOCK, (b + 1) * BLOCK)
            g, qb, kb, vb = run[r], q[r], k[r], v[r]
            ref = g[half - 1:half]
            last = g[BLOCK - 1:BLOCK]
            qe = (qb * jnp.exp(g - ref)).astype(BF16)
            ke = (kb * jnp.exp(ref - g)).astype(BF16)
            scores = jnp.where(causal, dot(qe, ke, ((1,), (1,))), 0.0).astype(BF16)
            out = dot(scores, vb)
            if b:
                qs = (qb * jnp.exp(g - base)).astype(BF16)
                out += dot(qs, state.astype(BF16), ((1,), (1,)))
            lo_ref[r, c] = out
            kd = (kb * jnp.exp(last - g)).astype(BF16)
            state = state * jnp.exp(last - base) + dot(vb, kd, ((0,), (0,)))
            base = last
        st_ref[j, 0:dim, :] = state.astype(BF16)
        st_ref[j, dim:, :] = jnp.broadcast_to(jnp.exp(base), (st_ref.shape[1] - dim, dim)).astype(BF16)


def mixer(x, gain, wq, wf, wi, wo, gap, dec):
    parts, length, cols = x.shape
    heads, dim = dec.shape[1], wq.shape[1] // dec.shape[1]
    per = 2 if heads % 2 == 0 else 1
    width = per * dim
    depth = wq.shape[0]
    column = pl.BlockSpec((depth, width), lambda i: (0, i))
    rows = pl.BlockSpec((length, width), lambda i: (0, i))
    whole = lambda s: pl.BlockSpec(s, lambda i: (0,) * len(s))
    return pl.pallas_call(
        functools.partial(mixer_kernel, per),
        grid=(heads // per,),
        in_specs=[whole(x.shape), whole((1, depth)), column, column, column, column,
                  pl.BlockSpec((1, width), lambda i: (0, i)), whole(dec.shape)],
        out_specs=[rows, rows, rows, pl.BlockSpec((per, dim + 16, dim), lambda i: (i, 0, 0))],
        out_shape=[jax.ShapeDtypeStruct((length, heads * dim), F32),
                   jax.ShapeDtypeStruct((length, heads * dim), BF16),
                   jax.ShapeDtypeStruct((length, heads * dim), F32),
                   jax.ShapeDtypeStruct((heads, dim + 16, dim), BF16)],
        scratch_shapes=[pltpu.VMEM((length, depth), BF16)],
        compiler_params=pltpu.CompilerParams(vmem_limit_bytes=LIMIT),
        cost_estimate=pl.CostEstimate(flops=10 * 10**9, bytes_accessed=9 * 10**6, transcendentals=10**6),
    )(x, gain.reshape(1, -1), wq, wf, wi, wo, gap.reshape(1, -1), dec)


def tail_kernel(states_ref, lo_ref, qd_ref, og_ref, hg_ref, w_ref, out_ref, gated):
    place = lax.axis_index("ep")
    hops, heads, _, dim = states_ref.shape
    for h in range(heads):
        c = slice(h * dim, (h + 1) * dim)

        def one(hop, state):
            own = states_ref[hop, h, 0:dim, :].astype(F32)
            passing = states_ref[hop, h, dim:dim + 16, :].astype(F32)[0:1]
            return jnp.where(hop < place, state * passing + own, state)

        state = lax.fori_loop(0, hops, one, jnp.zeros((dim, dim), F32))
        out = lo_ref[:, c] + dot(qd_ref[:, c], state.astype(BF16), ((1,), (1,)))
        scale = lax.rsqrt(jnp.mean(out * out, axis=1, keepdims=True) + epsilon)
        gated[:, c] = (out * scale * hg_ref[...].astype(F32) * og_ref[:, c]).astype(BF16)
    parts, _, cols = out_ref.shape
    for p in range(parts):
        out_ref[p] = dot(gated[...], w_ref[:, p * cols:(p + 1) * cols]).astype(BF16)


def tail(states, lo, qd, og, hg, w, parts):
    length, width = lo.shape
    return pl.pallas_call(
        tail_kernel,
        in_specs=[VMEM] * 6,
        out_specs=VMEM,
        out_shape=jax.ShapeDtypeStruct((parts, length, w.shape[1] // parts), BF16),
        scratch_shapes=[pltpu.VMEM((length, width), BF16)],
        compiler_params=pltpu.CompilerParams(vmem_limit_bytes=LIMIT),
        cost_estimate=pl.CostEstimate(flops=10**9, bytes_accessed=5 * 10**6, transcendentals=10**5),
    )(states, lo, qd, og, hg.reshape(1, -1), w)


def ranks(ids, experts):
    tokens = ids.shape[1]
    names = iota((experts, tokens), 0)
    picks = [names == ids[k:k + 1, :] for k in range(ids.shape[0])]
    chosen = functools.reduce(jnp.logical_or, picks)
    before = (iota((tokens, tokens), 0) < iota((tokens, tokens), 1)).astype(BF16)
    return picks, chosen, dot(chosen.astype(BF16), before)


def slot_hits(mask, rank, experts, capacity):
    rows = experts * capacity
    owner = iota((rows, experts), 0) - iota((rows, experts), 1) * capacity
    owner = jnp.logical_and(owner >= 0, owner < capacity).astype(F32)
    tokens = rank.shape[1]
    spread = dot(owner, jnp.where(mask, rank, -1.0))
    spot = dot(owner, iota((experts, tokens), 0).astype(F32)) * capacity
    return (spread >= 0.0) & (spread + spot == iota((rows, tokens), 0).astype(F32))


def dispatch_kernel(experts, capacity, ids_ref, rows_ref, out_ref):
    _, chosen, rank = ranks(ids_ref[...], experts)
    hits = slot_hits(chosen, rank, experts, capacity).astype(BF16)
    out_ref[...] = dot(hits, rows_ref[...]).astype(BF16)


def dispatch(ids, rows, experts, capacity):
    return pl.pallas_call(
        functools.partial(dispatch_kernel, experts, capacity),
        in_specs=[VMEM] * 2,
        out_specs=VMEM,
        out_shape=jax.ShapeDtypeStruct((experts * capacity, rows.shape[1]), BF16),
    )(ids, rows)


def combine_kernel(experts, capacity, ids_ref, scores_ref, back_ref, out_ref):
    picks, _, rank = ranks(ids_ref[...], experts)
    scores = scores_ref[...]
    weights = scores / jnp.sum(scores, axis=1, keepdims=True)
    total = jnp.zeros(out_ref.shape, F32)
    for k, mask in enumerate(picks):
        hits = slot_hits(mask, rank, experts, capacity).astype(BF16)
        total += dot(hits, back_ref[...], ((0,), (0,))) * weights[:, k:k + 1]
    out_ref[...] = total.astype(BF16)


def combine(ids, scores, back, experts, capacity):
    return pl.pallas_call(
        functools.partial(combine_kernel, experts, capacity),
        in_specs=[VMEM] * 3,
        out_specs=VMEM,
        out_shape=jax.ShapeDtypeStruct((ids.shape[1], back.shape[1]), BF16),
    )(ids, scores, back)


def expert_kernel(x_ref, gain_ref, wg_ref, wu_ref, wd_ref, out_ref, normed, total):
    step = pl.program_id(0)
    parts, rows, cols = x_ref.shape

    @pl.when(step == 0)
    def _():
        squares = jnp.zeros((rows, 1), F32)
        for p in range(parts):
            v = x_ref[p].astype(F32)
            squares += jnp.sum(v * v, axis=1, keepdims=True)
        scale = lax.rsqrt(squares / (parts * cols) + epsilon)
        for p in range(parts):
            g = gain_ref[:, p * cols:(p + 1) * cols].astype(F32)
            normed[:, p * cols:(p + 1) * cols] = (x_ref[p].astype(F32) * scale * g).astype(BF16)

    gate = dot(normed[...], wg_ref[0])
    up = dot(normed[...], wu_ref[0])
    hidden = (gate * sigmoid(gate) * up).astype(BF16)
    last = pl.num_programs(0) - 1
    for p in range(parts):
        c = slice(p * cols, (p + 1) * cols)
        part = dot(hidden, wd_ref[0, :, c])

        @pl.when(jnp.logical_and(step == 0, last > 0))
        def _():
            total[:, c] = part

        @pl.when(jnp.logical_and(step > 0, step < last))
        def _():
            total[:, c] += part

        @pl.when(step == last)
        def _():
            out_ref[p] = (jnp.where(step > 0, total[:, c], 0.0) + part).astype(BF16)


def experts_call(x, gain, wg, wu, wd):
    parts, rows, cols = x.shape
    depth, units = wg.shape[1:]
    tile = 256 if units % 256 == 0 else units
    return pl.pallas_call(
        expert_kernel,
        grid=(units // tile,),
        in_specs=[pl.BlockSpec(x.shape, lambda i: (0, 0, 0)), pl.BlockSpec((1, depth), lambda i: (0, 0)),
                  pl.BlockSpec((1, depth, tile), lambda i: (0, 0, i)),
                  pl.BlockSpec((1, depth, tile), lambda i: (0, 0, i)),
                  pl.BlockSpec((1, tile, depth), lambda i: (0, i, 0))],
        out_specs=pl.BlockSpec(x.shape, lambda i: (0, 0, 0)),
        out_shape=jax.ShapeDtypeStruct(x.shape, BF16),
        scratch_shapes=[pltpu.VMEM((rows, depth), BF16), pltpu.VMEM((rows, depth), F32)],
        compiler_params=pltpu.CompilerParams(vmem_limit_bytes=LIMIT),
        cost_estimate=pl.CostEstimate(flops=8 * 10**9, bytes_accessed=10**7, transcendentals=10**6),
    )(x, gain.reshape(1, -1), wg, wu, wd)

MESH = pl.DeviceIdType.MESH
ANY = pl.BlockSpec(memory_space=pl.ANY)
HIGHEST = lax.Precision.HIGHEST
GROUPS = 2


def flip(place, bits):
    bit = 1
    while bit <= bits:
        if bits & bit:
            place = place + bit - 2 * bit * lax.rem(lax.div(place, bit), 2)
        bit *= 2
    return place


def block_kernel(cap, mix_ref, mgain_ref, wq_hbm, wf_hbm, wi_hbm, wo_hbm, gap_ref, dec_ref, hgain_ref, wm_hbm,
                 moe_ref, egain_ref, ids_ref, scores_ref, wg_hbm, wu_hbm, wd_hbm,
                 mix_out, moe_out,
                 wmix, wm, wg, wu, wd, xall, normed, lo, qd, og, st, states, gated, mixed, mixin,
                 gath, slots, hits, enormed, hidden, psend, precv, esum, back, total,
                 wsem, xs, xr, zs, zr, gs, gr, ps, pr, bs, br, ss, sr, ms, mr):
    eps, tps = lax.axis_size("ep"), lax.axis_size("tp")
    me, mt = lax.axis_index("ep"), lax.axis_index("tp")
    length, cols = mix_ref.shape
    rows = eps * cap
    heads, _, dim = st.shape
    depth = tps * cols
    units = wg.shape[1]
    ep_peer = [flip(me, k) for k in range(eps)]
    tp_peer = [flip(mt, r) for r in range(tps)]

    def push(src, dst, send, recv, ep=None, tp=None):
        where = {"ep": ep_peer[ep]} if tp is None else {"tp": tp_peer[tp]}
        return pltpu.make_async_remote_copy(src_ref=src, dst_ref=dst, send_sem=send, recv_sem=recv,
                                            device_id=where, device_id_type=MESH)

    sent = []

    def go(copy):
        copy.start()
        sent.append(copy)

    loads = [pltpu.make_async_copy(s, wmix.at[i], wsem.at[i]) for i, s in enumerate((wq_hbm, wf_hbm, wi_hbm, wo_hbm))]
    loads += [pltpu.make_async_copy(wg_hbm.at[0], wg, wsem.at[4]), pltpu.make_async_copy(wu_hbm.at[0], wu, wsem.at[5]),
              pltpu.make_async_copy(wd_hbm.at[0], wd, wsem.at[6]), pltpu.make_async_copy(wm_hbm, wm, wsem.at[7])]
    for load in loads:
        load.start()

    barrier = pltpu.get_barrier_semaphore()
    for k in range(1, eps):
        pl.semaphore_signal(barrier, inc=1, device_id={"ep": ep_peer[k]}, device_id_type=MESH)
    for r in range(1, tps):
        pl.semaphore_signal(barrier, inc=1, device_id={"tp": tp_peer[r]}, device_id_type=MESH)
    pl.semaphore_wait(barrier, eps + tps - 2)

    half = length // 2
    go(push(mix_ref, xall.at[mt], xs.at[0], xr.at[0], tp=1))
    go(push(mix_ref, xall.at[mt], xs.at[1], xr.at[1], tp=2))

    experts = eps
    names = iota((length, experts), 1)
    ids = ids_ref[...]
    picks = [ids[:, j:j + 1] == names for j in range(ids.shape[1])]
    chosen = functools.reduce(jnp.logical_or, picks)
    before = (iota((length, length), 0) > iota((length, length), 1)).astype(BF16)
    rank = dot(before, chosen.astype(BF16)).astype(jnp.int32)
    spot = rank + jnp.bitwise_xor(names, me) * cap
    both = None
    for j, pick in enumerate(picks):
        at = jnp.sum(jnp.where(pick, spot, 0), axis=1, keepdims=True)
        hit = (iota((length, rows), 1) == at).astype(F32)
        hits[j] = hit.astype(BF16)
        both = hit if both is None else both + hit
    made = dot(both.astype(BF16), moe_ref[...], ((0,), (0,))).astype(BF16)
    slots[...] = made
    gath[mt, 0:cap, :] = made[0:cap]
    for k in range(1, eps):
        r = slice(k * cap, (k + 1) * cap)
        go(push(slots.at[r], gath.at[mt, r], zs.at[k], zr.at[k], ep=k))

    def rowsof(k, part=None):
        if part is None:
            return pl.ds(k * cap, cap)
        return pl.ds(k * cap + part * (cap // 2), cap // 2)

    def spread(k):
        if k:
            push(slots.at[rowsof(k)], gath.at[mt, rowsof(k)], zs.at[k], zr.at[k], ep=k).wait_recv()
        for n, r in enumerate((1, 2)):
            ref = gath.at[mt, rowsof(k)]
            go(push(ref, ref, gs.at[k, n], gr.at[k, n], tp=r))

    def relay(k):
        for n, (source, target) in enumerate(((1, 2), (2, 1))):
            whole = gath.at[tp_peer[source], rowsof(k)]
            push(whole, whole, gs.at[k, n], gr.at[k, n], tp=source).wait_recv()
            ref = gath.at[tp_peer[source], rowsof(k, n)]
            go(push(ref, ref, gs.at[k, 2 + n], gr.at[k, 2 + n], tp=target))

    def complete(k):
        for n, via in enumerate((2, 1)):
            ref = gath.at[tp_peer[3], rowsof(k, n)]
            push(ref, ref, gs.at[k, 2 + n], gr.at[k, 2 + n], tp=via).wait_recv()

    def relay_mix():
        for n, (source, target) in enumerate(((1, 2), (2, 1))):
            whole = xall.at[tp_peer[source]]
            push(whole, whole, xs.at[n], xr.at[n], tp=source).wait_recv()
            ref = xall.at[tp_peer[source], pl.ds(n * half, half)]
            go(push(ref, ref, xs.at[2 + n], xr.at[2 + n], tp=target))

    def complete_mix():
        for n, via in enumerate((2, 1)):
            ref = xall.at[tp_peer[3], pl.ds(n * half, half)]
            push(ref, ref, xs.at[2 + n], xr.at[2 + n], tp=via).wait_recv()

    agenda = [functools.partial(spread, 0), relay_mix, functools.partial(spread, 1), functools.partial(relay, 0)]
    for k in range(2, eps):
        agenda += [functools.partial(spread, k), functools.partial(relay, k - 1)]
    agenda.append(functools.partial(relay, eps - 1))

    def poll(count=1):
        for _ in range(min(count, len(agenda))):
            agenda.pop(0)()

    poll(4)
    xall[mt] = mix_ref[...]
    complete_mix()
    squares = jnp.zeros((length, 1), F32)
    for p in range(tps):
        v = xall[p].astype(F32)
        squares += jnp.sum(v * v, axis=1, keepdims=True)
    scale = lax.rsqrt(squares / depth + epsilon)
    for p in range(tps):
        c = slice(p * cols, (p + 1) * cols)
        normed[:, c] = (xall[p].astype(F32) * scale * mgain_ref[:, c].astype(F32)).astype(BF16)
    poll(1)

    tri = (iota((length, length), 0) >= iota((length, length), 1)).astype(F32)
    extra = dot(tri, dec_ref[...], ((1,), (1,)), precision=HIGHEST)
    causal = iota((BLOCK, BLOCK), 0) >= iota((BLOCK, BLOCK), 1)
    mid = BLOCK // 2
    per = 2 if heads % 2 == 0 else 1
    for load in loads[:4]:
        load.wait()
    for step in range(heads // per):
        w = slice(step * per * dim, (step + 1) * per * dim)
        n = normed[...]
        qp = dot(n, wmix[0, :, w])
        fp = dot(n, wmix[1, :, w])
        value = dot(n, wmix[2, :, w]).astype(BF16)
        op = dot(n, wmix[3, :, w])
        query = qp * sigmoid(qp)
        key = gap_ref[:, w] * sigmoid(-fp)
        og[:, w] = op * sigmoid(op)
        logs = jnp.log1p(-key)
        poll(1)
        for j in range(per):
            h = step * per + j
            cl = slice(j * dim, (j + 1) * dim)
            c = slice(h * dim, (h + 1) * dim)
            run = dot(tri, logs[:, cl], precision=HIGHEST) + extra[:, h:h + 1]
            q, k, v = query[:, cl], key[:, cl], value[:, cl]
            qd[:, c] = (q * jnp.exp(run)).astype(BF16)
            state = jnp.zeros((dim, dim), F32)
            base = jnp.zeros((1, dim), F32)
            for b in range(length // BLOCK):
                r = slice(b * BLOCK, (b + 1) * BLOCK)
                g, qb, kb, vb = run[r], q[r], k[r], v[r]
                ref = g[mid - 1:mid]
                last = g[BLOCK - 1:BLOCK]
                qe = (qb * jnp.exp(g - ref)).astype(BF16)
                ke = (kb * jnp.exp(ref - g)).astype(BF16)
                scores = jnp.where(causal, dot(qe, ke, ((1,), (1,))), 0.0).astype(BF16)
                out = dot(scores, vb)
                if b:
                    qs = (qb * jnp.exp(g - base)).astype(BF16)
                    out += dot(qs, state.astype(BF16), ((1,), (1,)))
                lo[r, c] = out
                kd = (kb * jnp.exp(last - g)).astype(BF16)
                state = state * jnp.exp(last - base) + dot(vb, kd, ((0,), (0,)))
                base = last
            st[h, 0:dim, :] = state.astype(BF16)
            st[h, dim:, :] = jnp.broadcast_to(jnp.exp(base), (st.shape[1] - dim, dim)).astype(BF16)
            poll(1)

    def state_copy(k):
        return push(st, states.at[me], ss.at[k], sr.at[me], ep=k)

    for k in range(1, eps):
        @pl.when(ep_peer[k] > me)
        def _():
            state_copy(k).start()

    def finish_mixer():
        @pl.loop(0, me)
        def _(hop):
            pltpu.make_async_remote_copy(src_ref=st, dst_ref=states.at[hop], send_sem=ss.at[0], recv_sem=sr.at[hop],
                                         device_id={"ep": hop}, device_id_type=MESH).wait_recv()

        for h in range(heads):
            c = slice(h * dim, (h + 1) * dim)

            def one(hop, state):
                own = states[hop, h, 0:dim, :].astype(F32)
                passing = states[hop, h, dim:dim + 16, :].astype(F32)[0:1]
                return state * passing + own

            state = lax.fori_loop(0, me, one, jnp.zeros((dim, dim), F32))
            out = lo[:, c] + dot(qd[:, c], state.astype(BF16), ((1,), (1,)))
            scale = lax.rsqrt(jnp.mean(out * out, axis=1, keepdims=True) + epsilon)
            gated[:, c] = (out * scale * hgain_ref[...].astype(F32) * og[:, c]).astype(BF16)
        loads[7].wait()
        for r in (3, 1, 2, 0):
            block = wm[:, pl.ds(pl.multiple_of(tp_peer[r] * cols, cols), cols)]
            mixed[r] = dot(gated[...], block).astype(BF16)
            if r:
                go(push(mixed.at[r], mixin.at[r], ms.at[r], mr.at[r], tp=r))

    tile = 256 if units % 256 == 0 else units
    chunks = eps // GROUPS
    grows = chunks * cap

    def feed(group):
        for i in range(chunks):
            k = group * chunks + i
            complete(k)
            r = slice(k * cap, (k + 1) * cap)
            squares = jnp.zeros((cap, 1), F32)
            for p in range(tps):
                v = gath[p, r, :].astype(F32)
                squares += jnp.sum(v * v, axis=1, keepdims=True)
            scale = lax.rsqrt(squares / depth + epsilon)
            for p in range(tps):
                c = slice(p * cols, (p + 1) * cols)
                enormed[r, c] = (gath[p, r, :].astype(F32) * scale * egain_ref[:, c].astype(F32)).astype(BF16)

    def upward(group):
        r = slice(group * grows, (group + 1) * grows)
        for u in range(units // tile):
            c = slice(u * tile, (u + 1) * tile)
            gate = dot(enormed[r, :], wg[:, c])
            up = dot(enormed[r, :], wu[:, c])
            hidden[:, c] = (gate * sigmoid(gate) * up).astype(BF16)
            poll(1)

    def downward(group):
        r = slice(group * grows, (group + 1) * grows)
        for t in (3, 1, 2, 0):
            block = wd[:, pl.ds(pl.multiple_of(tp_peer[t] * cols, cols), cols)]
            psend[t, r, :] = dot(hidden[...], block).astype(BF16)
            if t:
                go(push(psend.at[t, r], precv.at[t, r], ps.at[group, t], pr.at[group, t], tp=t))

    def reduce(group):
        r = slice(group * grows, (group + 1) * grows)
        for t in range(1, tps):
            push(psend.at[t, r], precv.at[t, r], ps.at[group, t], pr.at[group, t], tp=t).wait_recv()
        for i in range(chunks):
            k = group * chunks + i
            r = slice(k * cap, (k + 1) * cap)
            value = psend[0, r, :].astype(F32)
            for t in range(1, tps):
                value += precv[t, r, :].astype(F32)
            if k:
                esum[r, :] = value.astype(BF16)
                go(push(esum.at[r], back.at[r], bs.at[k], br.at[k], ep=k))
            else:
                back[r, :] = value.astype(BF16)

    scores = scores_ref[...]
    weights = scores / jnp.sum(scores, axis=1, keepdims=True)

    def combine_group(group):
        for i in range(chunks):
            k = group * chunks + i
            if k:
                r = slice(k * cap, (k + 1) * cap)
                push(esum.at[r], back.at[r], bs.at[k], br.at[k], ep=k).wait_recv()
        r = slice(group * grows, (group + 1) * grows)
        value = jnp.zeros((length, cols), F32)
        for j in range(hits.shape[0]):
            value += dot(hits[j, :, r], back[r, :]) * weights[:, j:j + 1]
        return value

    for load in loads[4:7]:
        load.wait()
    while len(agenda) > 3 * 2:
        poll(1)
    feed(0)
    upward(0)
    downward(0)
    poll(len(agenda))
    feed(1)
    upward(1)
    downward(1)
    finish_mixer()
    reduce(0)
    total[...] = combine_group(0)
    reduce(1)
    for r in range(1, tps):
        push(mixed.at[r], mixin.at[r], ms.at[r], mr.at[r], tp=r).wait_recv()
    value = mixed[0].astype(F32)
    for r in range(1, tps):
        value += mixin[r].astype(F32)
    mix_out[...] = value.astype(BF16)
    moe_out[...] = (total[...] + combine_group(1)).astype(BF16)

    for copy in sent:
        copy.wait_send()
    for k in range(1, eps):
        @pl.when(ep_peer[k] > me)
        def _():
            state_copy(k).wait_send()


def whole_block(mix_rows, mix_gain, wq, wf, wi, wo, gap, dec, hgain, wm, moe_rows, moe_gain, ids, scores, wg, wu, wd):
    eps, tps = lax.axis_size("ep"), lax.axis_size("tp")
    length, cols = mix_rows.shape
    top = ids.shape[1]
    cap = length * top * 3 // (2 * eps)
    rows = eps * cap
    heads = dec.shape[0]
    width = wq.shape[1]
    dim = width // heads
    depth, units = wg.shape[1:]
    dma = lambda *s: pltpu.SemaphoreType.DMA(s)
    out = jax.ShapeDtypeStruct((length, cols), BF16)
    scratch = [
        pltpu.VMEM((4, depth, width), BF16), pltpu.VMEM((width, depth), BF16),
        pltpu.VMEM((depth, units), BF16), pltpu.VMEM((depth, units), BF16), pltpu.VMEM((units, depth), BF16),
        pltpu.VMEM((tps, length, cols), BF16), pltpu.VMEM((length, depth), BF16),
        pltpu.VMEM((length, width), F32), pltpu.VMEM((length, width), BF16), pltpu.VMEM((length, width), F32),
        pltpu.VMEM((heads, dim + 16, dim), BF16), pltpu.VMEM((eps, heads, dim + 16, dim), BF16),
        pltpu.VMEM((length, width), BF16), pltpu.VMEM((tps, length, cols), BF16), pltpu.VMEM((tps, length, cols), BF16),
        pltpu.VMEM((tps, rows, cols), BF16), pltpu.VMEM((rows, cols), BF16), pltpu.VMEM((top, length, rows), BF16),
        pltpu.VMEM((rows, depth), BF16), pltpu.VMEM((rows // GROUPS, units), BF16),
        pltpu.VMEM((tps, rows, cols), BF16), pltpu.VMEM((tps, rows, cols), BF16),
        pltpu.VMEM((rows, cols), BF16), pltpu.VMEM((rows, cols), BF16), pltpu.VMEM((length, cols), F32),
        dma(8), dma(4), dma(4), dma(eps), dma(eps), dma(eps, 4), dma(eps, 4), dma(GROUPS, tps), dma(GROUPS, tps),
        dma(eps), dma(eps), dma(eps), dma(eps), dma(tps), dma(tps),
    ]
    return pl.pallas_call(
        functools.partial(block_kernel, cap),
        in_specs=[VMEM, VMEM, ANY, ANY, ANY, ANY, VMEM, VMEM, VMEM, ANY, VMEM, VMEM, VMEM, VMEM, ANY, ANY, ANY],
        out_specs=[VMEM, VMEM],
        out_shape=[out, out],
        scratch_shapes=scratch,
        compiler_params=pltpu.CompilerParams(vmem_limit_bytes=LIMIT, collective_id=0, has_side_effects=True),
    )(mix_rows, mix_gain.reshape(1, -1), wq, wf, wi, wo, gap.reshape(1, -1), dec, hgain.reshape(1, -1), wm,
      moe_rows, moe_gain.reshape(1, -1), ids, scores, wg, wu, wd)


def fits(eps, tps, mix_rows, dec, route_ids, w_gate):
    tokens, cols = mix_rows.shape
    top = route_ids.shape[1]
    cap = tokens * top * 3 // (2 * eps)
    square = tps == 4 and eps >= 2 and eps & (eps - 1) == 0
    aligned = cap % 32 == 0 and cols % 128 == 0 and tokens % (2 * BLOCK) == 0 and w_gate.shape[2] % 128 == 0
    return square and aligned and w_gate.shape[0] == 1


def per_device(mix_rows, mix_gain, w_query, w_forget, w_input, w_outgate, forget_gap, decay_extra,
               head_gain, w_mixout, moe_rows, moe_gain, route_ids, route_scores, w_gate, w_up, w_down):
    eps, tps = lax.axis_size("ep"), lax.axis_size("tp")
    if fits(eps, tps, mix_rows, decay_extra, route_ids, w_gate):
        return whole_block(mix_rows, mix_gain, w_query, w_forget, w_input, w_outgate, forget_gap, decay_extra,
                           head_gain, w_mixout, moe_rows, moe_gain, route_ids, route_scores, w_gate, w_up, w_down)
    tokens, top = route_ids.shape
    experts = w_gate.shape[0] * eps
    capacity = tokens * top * 3 // (2 * experts)
    cols = mix_rows.shape[1]
    ids = route_ids.T
    slots = dispatch(ids, moe_rows, experts, capacity)
    arrived = lax.all_to_all(slots.reshape(eps, -1, cols), "ep", split_axis=0, concat_axis=0, tiled=True)
    gathered = lax.all_gather(arrived.reshape(-1, cols), "tp", axis=0)
    mix_whole = lax.all_gather(mix_rows, "tp", axis=0)
    lo, qd, og, st = mixer(mix_whole, mix_gain, w_query, w_forget, w_input, w_outgate, forget_gap, decay_extra.T)
    product = experts_call(gathered, moe_gain, w_gate, w_up, w_down)
    expert_sum = lax.psum_scatter(product, "tp", scatter_dimension=0)
    states = lax.all_gather(st, "ep", axis=0)
    mixed = tail(states, lo, qd, og, head_gain, w_mixout, tps)
    mix_out = lax.psum_scatter(mixed, "tp", scatter_dimension=0)
    back = lax.all_to_all(expert_sum.reshape(eps, -1, cols), "ep", split_axis=0, concat_axis=0, tiled=True)
    moe_out = combine(ids, route_scores, back.reshape(-1, cols), experts, capacity)
    return (mix_out, moe_out)


def solution(mesh):
    placed = (
        P("ep", "tp"), P(), P(None, "tp"), P(None, "tp"), P(None, "tp"), P(None, "tp"), P("tp"),
        P("tp", "ep"), P(), P("tp", None), P("ep", "tp"), P(), P("ep", None), P("ep", None),
        P("ep", None, "tp"), P("ep", None, "tp"), P("ep", "tp", None),
    )
    return jax.shard_map(
        per_device, mesh=mesh, in_specs=placed,
        out_specs=(P("ep", "tp"), P("ep", "tp")), check_vma=False,
    )
```

```python
import functools

import jax
import jax.numpy as jnp
from jax import lax
from jax.experimental import pallas as pl
from jax.experimental.pallas import tpu as pltpu
from jax.sharding import PartitionSpec as P

BLOCK = 64
epsilon = 1e-06
F32 = jnp.float32
BF16 = jnp.bfloat16
VMEM = pl.BlockSpec(memory_space=pltpu.VMEM)
LIMIT = 60 * 1024 * 1024


def dot(a, b, dims=((1,), (0,)), precision=None):
    return lax.dot_general(a, b, (dims, ((), ())), precision=precision, preferred_element_type=F32)


def sigmoid(x):
    return 1.0 / (1.0 + jnp.exp(-x))


def iota(shape, dim):
    return lax.broadcasted_iota(jnp.int32, shape, dim)


def mixer_kernel(per, x_ref, gain_ref, wq_ref, wf_ref, wi_ref, wo_ref, gap_ref, dec_ref,
                 lo_ref, qd_ref, og_ref, st_ref, normed):
    step = pl.program_id(0)
    length = normed.shape[0]
    dim = st_ref.shape[2]
    parts, _, cols = x_ref.shape

    @pl.when(step == 0)
    def _():
        total = jnp.zeros((length, 1), F32)
        for p in range(parts):
            v = x_ref[p].astype(F32)
            total += jnp.sum(v * v, axis=1, keepdims=True)
        scale = lax.rsqrt(total / (parts * cols) + epsilon)
        for p in range(parts):
            g = gain_ref[:, p * cols:(p + 1) * cols].astype(F32)
            normed[:, p * cols:(p + 1) * cols] = (x_ref[p].astype(F32) * scale * g).astype(BF16)

    n = normed[...]
    qp = dot(n, wq_ref[...])
    fp = dot(n, wf_ref[...])
    value = dot(n, wi_ref[...]).astype(BF16)
    op = dot(n, wo_ref[...])
    query = qp * sigmoid(qp)
    key = gap_ref[...] * sigmoid(-fp)
    og_ref[...] = op * sigmoid(op)
    logs = jnp.log1p(-key)
    dec = dec_ref[...]
    tri = (iota((length, length), 0) >= iota((length, length), 1)).astype(F32)
    causal = iota((BLOCK, BLOCK), 0) >= iota((BLOCK, BLOCK), 1)
    half = BLOCK // 2
    for j in range(per):
        c = slice(j * dim, (j + 1) * dim)
        extra = jnp.sum(jnp.where(iota(dec.shape, 1) == step * per + j, dec, 0.0), axis=1, keepdims=True)
        run = dot(tri, logs[:, c] + extra, precision=lax.Precision.HIGHEST)
        q, k, v = query[:, c], key[:, c], value[:, c]
        qd_ref[:, c] = (q * jnp.exp(run)).astype(BF16)
        state = jnp.zeros((dim, dim), F32)
        base = jnp.zeros((1, dim), F32)
        for b in range(length // BLOCK):
            r = slice(b * BLOCK, (b + 1) * BLOCK)
            g, qb, kb, vb = run[r], q[r], k[r], v[r]
            ref = g[half - 1:half]
            last = g[BLOCK - 1:BLOCK]
            qe = (qb * jnp.exp(g - ref)).astype(BF16)
            ke = (kb * jnp.exp(ref - g)).astype(BF16)
            scores = jnp.where(causal, dot(qe, ke, ((1,), (1,))), 0.0).astype(BF16)
            out = dot(scores, vb)
            if b:
                qs = (qb * jnp.exp(g - base)).astype(BF16)
                out += dot(qs, state.astype(BF16), ((1,), (1,)))
            lo_ref[r, c] = out
            kd = (kb * jnp.exp(last - g)).astype(BF16)
            state = state * jnp.exp(last - base) + dot(vb, kd, ((0,), (0,)))
            base = last
        st_ref[j, 0:dim, :] = state.astype(BF16)
        st_ref[j, dim:, :] = jnp.broadcast_to(jnp.exp(base), (st_ref.shape[1] - dim, dim)).astype(BF16)


def mixer(x, gain, wq, wf, wi, wo, gap, dec):
    parts, length, cols = x.shape
    heads, dim = dec.shape[1], wq.shape[1] // dec.shape[1]
    per = 2 if heads % 2 == 0 else 1
    width = per * dim
    depth = wq.shape[0]
    column = pl.BlockSpec((depth, width), lambda i: (0, i))
    rows = pl.BlockSpec((length, width), lambda i: (0, i))
    whole = lambda s: pl.BlockSpec(s, lambda i: (0,) * len(s))
    return pl.pallas_call(
        functools.partial(mixer_kernel, per),
        grid=(heads // per,),
        in_specs=[whole(x.shape), whole((1, depth)), column, column, column, column,
                  pl.BlockSpec((1, width), lambda i: (0, i)), whole(dec.shape)],
        out_specs=[rows, rows, rows, pl.BlockSpec((per, dim + 16, dim), lambda i: (i, 0, 0))],
        out_shape=[jax.ShapeDtypeStruct((length, heads * dim), F32),
                   jax.ShapeDtypeStruct((length, heads * dim), BF16),
                   jax.ShapeDtypeStruct((length, heads * dim), F32),
                   jax.ShapeDtypeStruct((heads, dim + 16, dim), BF16)],
        scratch_shapes=[pltpu.VMEM((length, depth), BF16)],
        compiler_params=pltpu.CompilerParams(vmem_limit_bytes=LIMIT),
        cost_estimate=pl.CostEstimate(flops=10 * 10**9, bytes_accessed=9 * 10**6, transcendentals=10**6),
    )(x, gain.reshape(1, -1), wq, wf, wi, wo, gap.reshape(1, -1), dec)


def tail_kernel(states_ref, lo_ref, qd_ref, og_ref, hg_ref, w_ref, out_ref, gated):
    place = lax.axis_index("ep")
    hops, heads, _, dim = states_ref.shape
    for h in range(heads):
        c = slice(h * dim, (h + 1) * dim)

        def one(hop, state):
            own = states_ref[hop, h, 0:dim, :].astype(F32)
            passing = states_ref[hop, h, dim:dim + 16, :].astype(F32)[0:1]
            return jnp.where(hop < place, state * passing + own, state)

        state = lax.fori_loop(0, hops, one, jnp.zeros((dim, dim), F32))
        out = lo_ref[:, c] + dot(qd_ref[:, c], state.astype(BF16), ((1,), (1,)))
        scale = lax.rsqrt(jnp.mean(out * out, axis=1, keepdims=True) + epsilon)
        gated[:, c] = (out * scale * hg_ref[...].astype(F32) * og_ref[:, c]).astype(BF16)
    parts, _, cols = out_ref.shape
    for p in range(parts):
        out_ref[p] = dot(gated[...], w_ref[:, p * cols:(p + 1) * cols]).astype(BF16)


def tail(states, lo, qd, og, hg, w, parts):
    length, width = lo.shape
    return pl.pallas_call(
        tail_kernel,
        in_specs=[VMEM] * 6,
        out_specs=VMEM,
        out_shape=jax.ShapeDtypeStruct((parts, length, w.shape[1] // parts), BF16),
        scratch_shapes=[pltpu.VMEM((length, width), BF16)],
        compiler_params=pltpu.CompilerParams(vmem_limit_bytes=LIMIT),
        cost_estimate=pl.CostEstimate(flops=10**9, bytes_accessed=5 * 10**6, transcendentals=10**5),
    )(states, lo, qd, og, hg.reshape(1, -1), w)


def ranks(ids, experts):
    tokens = ids.shape[1]
    names = iota((experts, tokens), 0)
    picks = [names == ids[k:k + 1, :] for k in range(ids.shape[0])]
    chosen = functools.reduce(jnp.logical_or, picks)
    before = (iota((tokens, tokens), 0) < iota((tokens, tokens), 1)).astype(BF16)
    return picks, chosen, dot(chosen.astype(BF16), before)


def slot_hits(mask, rank, experts, capacity):
    rows = experts * capacity
    owner = iota((rows, experts), 0) - iota((rows, experts), 1) * capacity
    owner = jnp.logical_and(owner >= 0, owner < capacity).astype(F32)
    tokens = rank.shape[1]
    spread = dot(owner, jnp.where(mask, rank, -1.0))
    spot = dot(owner, iota((experts, tokens), 0).astype(F32)) * capacity
    return (spread >= 0.0) & (spread + spot == iota((rows, tokens), 0).astype(F32))


def dispatch_kernel(experts, capacity, ids_ref, rows_ref, out_ref):
    _, chosen, rank = ranks(ids_ref[...], experts)
    hits = slot_hits(chosen, rank, experts, capacity).astype(BF16)
    out_ref[...] = dot(hits, rows_ref[...]).astype(BF16)


def dispatch(ids, rows, experts, capacity):
    return pl.pallas_call(
        functools.partial(dispatch_kernel, experts, capacity),
        in_specs=[VMEM] * 2,
        out_specs=VMEM,
        out_shape=jax.ShapeDtypeStruct((experts * capacity, rows.shape[1]), BF16),
    )(ids, rows)


def combine_kernel(experts, capacity, ids_ref, scores_ref, back_ref, out_ref):
    picks, _, rank = ranks(ids_ref[...], experts)
    scores = scores_ref[...]
    weights = scores / jnp.sum(scores, axis=1, keepdims=True)
    total = jnp.zeros(out_ref.shape, F32)
    for k, mask in enumerate(picks):
        hits = slot_hits(mask, rank, experts, capacity).astype(BF16)
        total += dot(hits, back_ref[...], ((0,), (0,))) * weights[:, k:k + 1]
    out_ref[...] = total.astype(BF16)


def combine(ids, scores, back, experts, capacity):
    return pl.pallas_call(
        functools.partial(combine_kernel, experts, capacity),
        in_specs=[VMEM] * 3,
        out_specs=VMEM,
        out_shape=jax.ShapeDtypeStruct((ids.shape[1], back.shape[1]), BF16),
    )(ids, scores, back)


def expert_kernel(x_ref, gain_ref, wg_ref, wu_ref, wd_ref, out_ref, normed, total):
    step = pl.program_id(0)
    parts, rows, cols = x_ref.shape

    @pl.when(step == 0)
    def _():
        squares = jnp.zeros((rows, 1), F32)
        for p in range(parts):
            v = x_ref[p].astype(F32)
            squares += jnp.sum(v * v, axis=1, keepdims=True)
        scale = lax.rsqrt(squares / (parts * cols) + epsilon)
        for p in range(parts):
            g = gain_ref[:, p * cols:(p + 1) * cols].astype(F32)
            normed[:, p * cols:(p + 1) * cols] = (x_ref[p].astype(F32) * scale * g).astype(BF16)

    gate = dot(normed[...], wg_ref[0])
    up = dot(normed[...], wu_ref[0])
    hidden = (gate * sigmoid(gate) * up).astype(BF16)
    last = pl.num_programs(0) - 1
    for p in range(parts):
        c = slice(p * cols, (p + 1) * cols)
        part = dot(hidden, wd_ref[0, :, c])

        @pl.when(jnp.logical_and(step == 0, last > 0))
        def _():
            total[:, c] = part

        @pl.when(jnp.logical_and(step > 0, step < last))
        def _():
            total[:, c] += part

        @pl.when(step == last)
        def _():
            out_ref[p] = (jnp.where(step > 0, total[:, c], 0.0) + part).astype(BF16)


def experts_call(x, gain, wg, wu, wd):
    parts, rows, cols = x.shape
    depth, units = wg.shape[1:]
    tile = 256 if units % 256 == 0 else units
    return pl.pallas_call(
        expert_kernel,
        grid=(units // tile,),
        in_specs=[pl.BlockSpec(x.shape, lambda i: (0, 0, 0)), pl.BlockSpec((1, depth), lambda i: (0, 0)),
                  pl.BlockSpec((1, depth, tile), lambda i: (0, 0, i)),
                  pl.BlockSpec((1, depth, tile), lambda i: (0, 0, i)),
                  pl.BlockSpec((1, tile, depth), lambda i: (0, i, 0))],
        out_specs=pl.BlockSpec(x.shape, lambda i: (0, 0, 0)),
        out_shape=jax.ShapeDtypeStruct(x.shape, BF16),
        scratch_shapes=[pltpu.VMEM((rows, depth), BF16), pltpu.VMEM((rows, depth), F32)],
        compiler_params=pltpu.CompilerParams(vmem_limit_bytes=LIMIT),
        cost_estimate=pl.CostEstimate(flops=8 * 10**9, bytes_accessed=10**7, transcendentals=10**6),
    )(x, gain.reshape(1, -1), wg, wu, wd)

MESH = pl.DeviceIdType.MESH
ANY = pl.BlockSpec(memory_space=pl.ANY)
HIGHEST = lax.Precision.HIGHEST
GROUPS = 2
PAIR = 2


def flip(place, bits):
    bit = 1
    while bit <= bits:
        if bits & bit:
            place = place + bit - 2 * bit * lax.rem(lax.div(place, bit), 2)
        bit *= 2
    return place


def block_kernel(cap, mix_hbm, mgain_ref, wq_hbm, wf_hbm, wi_hbm, wo_hbm, gap_ref, dec_ref, hgain_ref, wm_hbm,
                 moe_hbm, egain_ref, ids_ref, scores_ref, wg_hbm, wu_hbm, wd_hbm,
                 mix_out, moe_out,
                 mix_ref, moe_ref, wmix, wm, wg, wu, wd, xall, normed, lo, qd, og, st, pst, cst, states, gated, mixed, mixin,
                 gath, slots, hits, enormed, hidden, psend, precv, esum, back, total,
                 wsem, xs, xr, zs, zr, gs, gr, ps, pr, bs, br, ss, sr, ms, mr):
    eps, tps = lax.axis_size("ep"), lax.axis_size("tp")
    me, mt = lax.axis_index("ep"), lax.axis_index("tp")
    length, cols = mix_ref.shape
    rows = eps * cap
    heads, _, dim = st.shape
    depth = tps * cols
    units = wg.shape[1]
    ep_peer = [flip(me, k) for k in range(eps)]
    tp_peer = [flip(mt, r) for r in range(tps)]

    def push(src, dst, send, recv, ep=None, tp=None):
        where = {"ep": ep_peer[ep]} if tp is None else {"tp": tp_peer[tp]}
        return pltpu.make_async_remote_copy(src_ref=src, dst_ref=dst, send_sem=send, recv_sem=recv,
                                            device_id=where, device_id_type=MESH)

    sent = []

    def go(copy):
        copy.start()
        sent.append(copy)

    loads = [pltpu.make_async_copy(s, wmix.at[i], wsem.at[i]) for i, s in enumerate((wq_hbm, wf_hbm, wi_hbm, wo_hbm))]
    loads += [pltpu.make_async_copy(wg_hbm.at[0], wg, wsem.at[4]), pltpu.make_async_copy(wu_hbm.at[0], wu, wsem.at[5]),
              pltpu.make_async_copy(wd_hbm.at[0], wd, wsem.at[6]), pltpu.make_async_copy(wm_hbm, wm, wsem.at[7])]
    rowload = [pltpu.make_async_copy(mix_hbm, mix_ref, wsem.at[8]), pltpu.make_async_copy(moe_hbm, moe_ref, wsem.at[9])]

    barrier = pltpu.get_barrier_semaphore()
    for k in range(1, eps):
        pl.semaphore_signal(barrier, inc=1, device_id={"ep": ep_peer[k]}, device_id_type=MESH)
    for r in range(1, tps):
        pl.semaphore_signal(barrier, inc=1, device_id={"tp": tp_peer[r]}, device_id_type=MESH)
    for load in rowload + loads:
        load.start()
    rowload[0].wait()
    pl.semaphore_wait(barrier, eps + tps - 2)

    half = length // 2
    go(push(mix_ref, xall.at[mt], xs.at[0], xr.at[0], tp=1))
    go(push(mix_ref, xall.at[mt], xs.at[1], xr.at[1], tp=2))

    experts = eps
    names = iota((length, experts), 1)
    eye = iota((length, length), 0) == iota((length, length), 1)
    ids = dot(eye.astype(BF16), ids_ref[...].astype(F32).astype(BF16), ((1,), (1,))).astype(jnp.int32)
    picks = [ids[:, j:j + 1] == names for j in range(ids.shape[1])]
    chosen = functools.reduce(jnp.logical_or, picks)
    before = (iota((length, length), 0) > iota((length, length), 1)).astype(BF16)
    rank = dot(before, chosen.astype(BF16)).astype(jnp.int32)
    spot = rank + jnp.bitwise_xor(names, me) * cap
    rowload[1].wait()
    both = None
    for j, pick in enumerate(picks):
        at = jnp.sum(jnp.where(pick, spot, 0), axis=1, keepdims=True)
        hit = (iota((length, rows), 1) == at).astype(F32)
        hits[j] = hit.astype(BF16)
        both = hit if both is None else both + hit
    made = dot(both.astype(BF16), moe_ref[...], ((0,), (0,))).astype(BF16)
    slots[...] = made
    gath[mt, 0:cap, :] = made[0:cap]
    for k in range(1, eps):
        r = slice(k * cap, (k + 1) * cap)
        go(push(slots.at[r], gath.at[mt, r], zs.at[k], zr.at[k], ep=k))

    def rowsof(k, part=None):
        if part is None:
            return pl.ds(k * cap, cap)
        return pl.ds(k * cap + part * (cap // 2), cap // 2)

    def spread(k):
        if k:
            push(slots.at[rowsof(k)], gath.at[mt, rowsof(k)], zs.at[k], zr.at[k], ep=k).wait_recv()
        for n, r in enumerate((1, 2)):
            ref = gath.at[mt, rowsof(k)]
            go(push(ref, ref, gs.at[k, n], gr.at[k, n], tp=r))

    def relay(k):
        for n, (source, target) in enumerate(((1, 2), (2, 1))):
            whole = gath.at[tp_peer[source], rowsof(k)]
            push(whole, whole, gs.at[k, n], gr.at[k, n], tp=source).wait_recv()
            ref = gath.at[tp_peer[source], rowsof(k, n)]
            go(push(ref, ref, gs.at[k, 2 + n], gr.at[k, 2 + n], tp=target))

    def complete(k):
        for n, via in enumerate((2, 1)):
            ref = gath.at[tp_peer[3], rowsof(k, n)]
            push(ref, ref, gs.at[k, 2 + n], gr.at[k, 2 + n], tp=via).wait_recv()

    def relay_mix():
        for n, (source, target) in enumerate(((1, 2), (2, 1))):
            whole = xall.at[tp_peer[source]]
            push(whole, whole, xs.at[n], xr.at[n], tp=source).wait_recv()
            ref = xall.at[tp_peer[source], pl.ds(n * half, half)]
            go(push(ref, ref, xs.at[2 + n], xr.at[2 + n], tp=target))

    def complete_mix():
        for n, via in enumerate((2, 1)):
            ref = xall.at[tp_peer[3], pl.ds(n * half, half)]
            push(ref, ref, xs.at[2 + n], xr.at[2 + n], tp=via).wait_recv()

    agenda = [functools.partial(spread, 0), relay_mix, functools.partial(spread, 1), functools.partial(relay, 0)]
    for k in range(2, eps):
        agenda += [functools.partial(spread, k), functools.partial(relay, k - 1)]
    agenda.append(functools.partial(relay, eps - 1))

    def poll(count=1):
        for _ in range(min(count, len(agenda))):
            agenda.pop(0)()

    poll(4)
    xall[mt] = mix_ref[...]
    complete_mix()
    squares = jnp.zeros((length, 1), F32)
    for p in range(tps):
        v = xall[p].astype(F32)
        squares += jnp.sum(v * v, axis=1, keepdims=True)
    scale = lax.rsqrt(squares / depth + epsilon)
    mgain, egain = mgain_ref[...].astype(F32), egain_ref[...].astype(F32)
    lanes = mgain.shape[1]
    for p in range(tps):
        for i in range(cols // lanes):
            s = slice(i * lanes, (i + 1) * lanes)
            n = p * (cols // lanes) + i
            normed[:, n * lanes:(n + 1) * lanes] = (xall[p, :, s].astype(F32) * scale * mgain[n:n + 1]).astype(BF16)
    poll(1)

    tri = (iota((length, length), 0) >= iota((length, length), 1)).astype(F32)
    extra = dot(tri, dec_ref[...], ((1,), (1,)), precision=HIGHEST)
    causal = iota((BLOCK, BLOCK), 0) >= iota((BLOCK, BLOCK), 1)
    mid = BLOCK // 2
    per = 2 if heads % 2 == 0 else 1
    for load in loads[:4]:
        load.wait()
    for step in range(heads // per):
        w = slice(step * per * dim, (step + 1) * per * dim)
        n = normed[...]
        qp = dot(n, wmix[0, :, w])
        fp = dot(n, wmix[1, :, w])
        value = dot(n, wmix[2, :, w]).astype(BF16)
        op = dot(n, wmix[3, :, w])
        query = qp * sigmoid(qp)
        key = gap_ref[:, w] * sigmoid(-fp)
        og[:, w] = op * sigmoid(op)
        logs = jnp.log1p(-key)
        poll(1)
        for j in range(per):
            h = step * per + j
            cl = slice(j * dim, (j + 1) * dim)
            c = slice(h * dim, (h + 1) * dim)
            run = dot(tri, logs[:, cl], precision=HIGHEST) + extra[:, h:h + 1]
            q, k, v = query[:, cl], key[:, cl], value[:, cl]
            qd[:, c] = (q * jnp.exp(run)).astype(BF16)
            state = jnp.zeros((dim, dim), F32)
            base = jnp.zeros((1, dim), F32)
            for b in range(length // BLOCK):
                r = slice(b * BLOCK, (b + 1) * BLOCK)
                g, qb, kb, vb = run[r], q[r], k[r], v[r]
                ref = g[mid - 1:mid]
                last = g[BLOCK - 1:BLOCK]
                qe = (qb * jnp.exp(g - ref)).astype(BF16)
                ke = (kb * jnp.exp(ref - g)).astype(BF16)
                scores = jnp.where(causal, dot(qe, ke, ((1,), (1,))), 0.0).astype(BF16)
                out = dot(scores, vb)
                if b:
                    qs = (qb * jnp.exp(g - base)).astype(BF16)
                    out += dot(qs, state.astype(BF16), ((1,), (1,)))
                lo[r, c] = out
                kd = (kb * jnp.exp(last - g)).astype(BF16)
                state = state * jnp.exp(last - base) + dot(vb, kd, ((0,), (0,)))
                base = last
            st[h, 0:dim, :] = state.astype(BF16)
            st[h, dim:, :] = jnp.broadcast_to(jnp.exp(base), (st.shape[1] - dim, dim)).astype(BF16)
            poll(1)

    odd = lax.rem(me, PAIR)
    pair = lax.div(me, PAIR)
    swap = push(st, pst, ss.at[1], sr.at[0], ep=1)
    go(swap)

    def joined_copy(k):
        return push(cst, states.at[pair], ss.at[k], sr.at[1 + pair], ep=k)

    def parts_of(ref, h):
        return ref[h, 0:dim, :].astype(F32), ref[h, dim:dim + 16, :].astype(F32)[0:1]

    def join_states():
        swap.wait_recv()
        for h in range(heads):
            (own, keep), (other, pass_on) = parts_of(st, h), parts_of(pst, h)
            cst[h, 0:dim, :] = jnp.where(odd == 1, other * keep + own, own * pass_on + other).astype(BF16)
            cst[h, dim:, :] = jnp.broadcast_to(keep * pass_on, (st.shape[1] - dim, dim)).astype(BF16)
        for k in range(PAIR, eps, PAIR):
            @pl.when(ep_peer[k] > me)
            def _():
                joined_copy(k).start()

    def finish_mixer():
        @pl.loop(0, pair)
        def _(hop):
            pltpu.make_async_remote_copy(src_ref=cst, dst_ref=states.at[hop], send_sem=ss.at[0], recv_sem=sr.at[1 + hop],
                                         device_id={"ep": hop * PAIR + odd}, device_id_type=MESH).wait_recv()

        for h in range(heads):
            c = slice(h * dim, (h + 1) * dim)

            def one(hop, state):
                own = states[hop, h, 0:dim, :].astype(F32)
                passing = states[hop, h, dim:dim + 16, :].astype(F32)[0:1]
                return state * passing + own

            state = lax.fori_loop(0, pair, one, jnp.zeros((dim, dim), F32))
            other, pass_on = parts_of(pst, h)
            state = jnp.where(odd == 1, state * pass_on + other, state)
            out = lo[:, c] + dot(qd[:, c], state.astype(BF16), ((1,), (1,)))
            scale = lax.rsqrt(jnp.mean(out * out, axis=1, keepdims=True) + epsilon)
            gated[:, c] = (out * scale * hgain_ref[...].astype(F32) * og[:, c]).astype(BF16)
        loads[7].wait()
        for r in (3, 1, 2, 0):
            block = wm[:, pl.ds(pl.multiple_of(tp_peer[r] * cols, cols), cols)]
            mixed[r] = dot(gated[...], block).astype(BF16)

    tile = 256 if units % 256 == 0 else units
    chunks = eps // GROUPS
    grows = chunks * cap

    def feed(group):
        for i in range(chunks):
            k = group * chunks + i
            complete(k)
            r = slice(k * cap, (k + 1) * cap)
            squares = jnp.zeros((cap, 1), F32)
            for p in range(tps):
                v = gath[p, r, :].astype(F32)
                squares += jnp.sum(v * v, axis=1, keepdims=True)
            scale = lax.rsqrt(squares / depth + epsilon)
            for p in range(tps):
                for i in range(cols // lanes):
                    s = slice(i * lanes, (i + 1) * lanes)
                    n = p * (cols // lanes) + i
                    c = slice(n * lanes, (n + 1) * lanes)
                    enormed[r, c] = (gath[p, r, s].astype(F32) * scale * egain[n:n + 1]).astype(BF16)

    def upward(group):
        r = slice(group * grows, (group + 1) * grows)
        for u in range(units // tile):
            c = slice(u * tile, (u + 1) * tile)
            gate = dot(enormed[r, :], wg[:, c])
            up = dot(enormed[r, :], wu[:, c])
            hidden[:, c] = (gate * sigmoid(gate) * up).astype(BF16)
            poll(1)

    def downward(group):
        r = slice(group * grows, (group + 1) * grows)
        for t in (3, 1, 2, 0):
            block = wd[:, pl.ds(pl.multiple_of(tp_peer[t] * cols, cols), cols)]
            psend[t, r, :] = dot(hidden[...], block).astype(BF16)

    def summing(src, dst, a, b, send, recv):
        def part(n, index, target, r, tp):
            return push(src.at[index, r], dst.at[target, r], send.at[n], recv.at[n], tp=tp)

        first = [part(0, 3, 3, a, 1), part(1, 3, 3, b, 2), part(2, 1, 1, a, 1), part(3, 2, 2, b, 2)]
        second = [part(4, 2, 2, a, 2), part(5, 1, 1, b, 1)]

        def start():
            for copy in first:
                go(copy)

        def merge():
            first[0].wait_recv()
            src[2, a, :] = (src[2, a, :].astype(F32) + dst[3, a, :].astype(F32)).astype(BF16)
            first[1].wait_recv()
            src[1, b, :] = (src[1, b, :].astype(F32) + dst[3, b, :].astype(F32)).astype(BF16)
            for copy in second:
                go(copy)

        def finish():
            for copy in first[2:] + second:
                copy.wait_recv()

        def value(r):
            return src[0, r, :].astype(F32) + dst[1, r, :].astype(F32) + dst[2, r, :].astype(F32)

        return start, merge, finish, value

    def chunk(k):
        return slice(k * cap, (k + 1) * cap)

    sums = [summing(psend, precv, chunk(2 * g), chunk(2 * g + 1), ps.at[g], pr.at[g]) for g in range(eps // 2)]
    mixsum = summing(mixed, mixin, slice(0, half), slice(half, length), ms, mr)

    def give_back(g):
        _, _, finish, value = sums[g]
        finish()
        for k in (2 * g, 2 * g + 1):
            r = chunk(k)
            if k:
                esum[r, :] = value(r).astype(BF16)
                go(push(esum.at[r], back.at[r], bs.at[k], br.at[k], ep=k))
            else:
                back[r, :] = value(r).astype(BF16)

    scores = scores_ref[...]
    weights = dot(eye.astype(F32), scores / jnp.sum(scores, axis=0, keepdims=True), ((1,), (1,)), precision=HIGHEST)

    def combine(g):
        for k in (2 * g, 2 * g + 1):
            if k:
                push(esum.at[chunk(k)], back.at[chunk(k)], bs.at[k], br.at[k], ep=k).wait_recv()
        r = slice(2 * g * cap, (2 * g + 2) * cap)
        value = jnp.zeros((length, cols), F32)
        for j in range(hits.shape[0]):
            value += dot(hits[j, :, r], back[r, :]) * weights[:, j:j + 1]
        return value

    far = list(range(eps // 2 - 1, eps // 4 - 1, -1))
    near = list(range(eps // 4 - 1, 0, -1))
    for load in loads[4:7]:
        load.wait()
    join_states()
    while len(agenda) > eps:
        poll(1)
    feed(0)
    upward(0)
    downward(0)
    poll(len(agenda))
    for g in near:
        sums[g][0]()
    feed(1)
    upward(1)
    for g in near:
        sums[g][1]()
    downward(1)
    for g in far:
        sums[g][0]()
    finish_mixer()
    for g in far:
        sums[g][1]()
    mixsum[0]()
    for g in near:
        give_back(g)
    sums[0][0]()
    for g in far:
        give_back(g)
    mixsum[1]()
    sums[0][1]()
    value = None
    for g in near + far:
        value = combine(g) if value is None else value + combine(g)
    total[...] = value
    mixsum[2]()
    mix_out[...] = mixsum[3](slice(0, length)).astype(BF16)
    give_back(0)
    moe_out[...] = (total[...] + combine(0)).astype(BF16)

    for copy in sent:
        copy.wait_send()
    for k in range(PAIR, eps, PAIR):
        @pl.when(ep_peer[k] > me)
        def _():
            joined_copy(k).wait_send()


def whole_block(mix_rows, mix_gain, wq, wf, wi, wo, gap, dec, hgain, wm, moe_rows, moe_gain, ids, scores, wg, wu, wd):
    eps, tps = lax.axis_size("ep"), lax.axis_size("tp")
    length, cols = mix_rows.shape
    top = ids.shape[1]
    cap = length * top * 3 // (2 * eps)
    rows = eps * cap
    heads = dec.shape[0]
    width = wq.shape[1]
    dim = width // heads
    depth, units = wg.shape[1:]
    dma = lambda *s: pltpu.SemaphoreType.DMA(s)
    out = jax.ShapeDtypeStruct((length, cols), BF16)
    scratch = [
        pltpu.VMEM((length, cols), BF16), pltpu.VMEM((length, cols), BF16),
        pltpu.VMEM((4, depth, width), BF16), pltpu.VMEM((width, depth), BF16),
        pltpu.VMEM((depth, units), BF16), pltpu.VMEM((depth, units), BF16), pltpu.VMEM((units, depth), BF16),
        pltpu.VMEM((tps, length, cols), BF16), pltpu.VMEM((length, depth), BF16),
        pltpu.VMEM((length, width), F32), pltpu.VMEM((length, width), BF16), pltpu.VMEM((length, width), F32),
        pltpu.VMEM((heads, dim + 16, dim), BF16), pltpu.VMEM((heads, dim + 16, dim), BF16),
        pltpu.VMEM((heads, dim + 16, dim), BF16), pltpu.VMEM((eps // PAIR, heads, dim + 16, dim), BF16),
        pltpu.VMEM((length, width), BF16), pltpu.VMEM((tps, length, cols), BF16), pltpu.VMEM((tps, length, cols), BF16),
        pltpu.VMEM((tps, rows, cols), BF16), pltpu.VMEM((rows, cols), BF16), pltpu.VMEM((top, length, rows), BF16),
        pltpu.VMEM((rows, depth), BF16), pltpu.VMEM((rows // GROUPS, units), BF16),
        pltpu.VMEM((tps, rows, cols), BF16), pltpu.VMEM((tps, rows, cols), BF16),
        pltpu.VMEM((rows, cols), BF16), pltpu.VMEM((rows, cols), BF16), pltpu.VMEM((length, cols), F32),
        dma(10), dma(4), dma(4), dma(eps), dma(eps), dma(eps, 4), dma(eps, 4), dma(eps // 2, 6), dma(eps // 2, 6),
        dma(eps), dma(eps), dma(eps), dma(eps), dma(6), dma(6),
    ]
    return pl.pallas_call(
        functools.partial(block_kernel, cap),
        in_specs=[ANY, VMEM, ANY, ANY, ANY, ANY, VMEM, VMEM, VMEM, ANY, ANY, VMEM, VMEM, VMEM, ANY, ANY, ANY],
        out_specs=[VMEM, VMEM],
        out_shape=[out, out],
        scratch_shapes=scratch,
        compiler_params=pltpu.CompilerParams(vmem_limit_bytes=LIMIT, collective_id=0, has_side_effects=True),
    )(mix_rows, mix_gain.reshape(-1, 128), wq, wf, wi, wo, gap.reshape(1, -1), dec, hgain.reshape(1, -1), wm,
      moe_rows, moe_gain.reshape(-1, 128), ids.T, scores.T, wg, wu, wd)


def fits(eps, tps, mix_rows, dec, route_ids, w_gate):
    tokens, cols = mix_rows.shape
    top = route_ids.shape[1]
    cap = tokens * top * 3 // (2 * eps)
    square = tps == 4 and eps >= 4 and eps & (eps - 1) == 0
    aligned = cap % 32 == 0 and cols % 128 == 0 and tokens % (2 * BLOCK) == 0 and w_gate.shape[2] % 128 == 0
    return square and aligned and w_gate.shape[0] == 1


def per_device(mix_rows, mix_gain, w_query, w_forget, w_input, w_outgate, forget_gap, decay_extra,
               head_gain, w_mixout, moe_rows, moe_gain, route_ids, route_scores, w_gate, w_up, w_down):
    eps, tps = lax.axis_size("ep"), lax.axis_size("tp")
    if fits(eps, tps, mix_rows, decay_extra, route_ids, w_gate):
        return whole_block(mix_rows, mix_gain, w_query, w_forget, w_input, w_outgate, forget_gap, decay_extra,
                           head_gain, w_mixout, moe_rows, moe_gain, route_ids, route_scores, w_gate, w_up, w_down)
    tokens, top = route_ids.shape
    experts = w_gate.shape[0] * eps
    capacity = tokens * top * 3 // (2 * experts)
    cols = mix_rows.shape[1]
    ids = route_ids.T
    slots = dispatch(ids, moe_rows, experts, capacity)
    arrived = lax.all_to_all(slots.reshape(eps, -1, cols), "ep", split_axis=0, concat_axis=0, tiled=True)
    gathered = lax.all_gather(arrived.reshape(-1, cols), "tp", axis=0)
    mix_whole = lax.all_gather(mix_rows, "tp", axis=0)
    lo, qd, og, st = mixer(mix_whole, mix_gain, w_query, w_forget, w_input, w_outgate, forget_gap, decay_extra.T)
    product = experts_call(gathered, moe_gain, w_gate, w_up, w_down)
    expert_sum = lax.psum_scatter(product, "tp", scatter_dimension=0)
    states = lax.all_gather(st, "ep", axis=0)
    mixed = tail(states, lo, qd, og, head_gain, w_mixout, tps)
    mix_out = lax.psum_scatter(mixed, "tp", scatter_dimension=0)
    back = lax.all_to_all(expert_sum.reshape(eps, -1, cols), "ep", split_axis=0, concat_axis=0, tiled=True)
    moe_out = combine(ids, route_scores, back.reshape(-1, cols), experts, capacity)
    return (mix_out, moe_out)


def solution(mesh):
    placed = (
        P("ep", "tp"), P(), P(None, "tp"), P(None, "tp"), P(None, "tp"), P(None, "tp"), P("tp"),
        P("tp", "ep"), P(), P("tp", None), P("ep", "tp"), P(), P("ep", None), P("ep", None),
        P("ep", None, "tp"), P("ep", None, "tp"), P("ep", "tp", None),
    )
    return jax.shard_map(
        per_device, mesh=mesh, in_specs=placed,
        out_specs=(P("ep", "tp"), P("ep", "tp")), check_vma=False,
    )
```

```python
import functools

import jax
import jax.numpy as jnp
from jax import lax
from jax.experimental import pallas as pl
from jax.experimental.pallas import tpu as pltpu
from jax.sharding import PartitionSpec as P

BLOCK = 64
epsilon = 1e-06
F32 = jnp.float32
BF16 = jnp.bfloat16
VMEM = pl.BlockSpec(memory_space=pltpu.VMEM)
LIMIT = 60 * 1024 * 1024


def dot(a, b, dims=((1,), (0,)), precision=None):
    return lax.dot_general(a, b, (dims, ((), ())), precision=precision, preferred_element_type=F32)


def sigmoid(x):
    return 1.0 / (1.0 + jnp.exp(-x))


def iota(shape, dim):
    return lax.broadcasted_iota(jnp.int32, shape, dim)


def mixer_kernel(per, x_ref, gain_ref, wq_ref, wf_ref, wi_ref, wo_ref, gap_ref, dec_ref,
                 lo_ref, qd_ref, og_ref, st_ref, normed):
    step = pl.program_id(0)
    length = normed.shape[0]
    dim = st_ref.shape[2]
    parts, _, cols = x_ref.shape

    @pl.when(step == 0)
    def _():
        total = jnp.zeros((length, 1), F32)
        for p in range(parts):
            v = x_ref[p].astype(F32)
            total += jnp.sum(v * v, axis=1, keepdims=True)
        scale = lax.rsqrt(total / (parts * cols) + epsilon)
        for p in range(parts):
            g = gain_ref[:, p * cols:(p + 1) * cols].astype(F32)
            normed[:, p * cols:(p + 1) * cols] = (x_ref[p].astype(F32) * scale * g).astype(BF16)

    n = normed[...]
    qp = dot(n, wq_ref[...])
    fp = dot(n, wf_ref[...])
    value = dot(n, wi_ref[...]).astype(BF16)
    op = dot(n, wo_ref[...])
    query = qp * sigmoid(qp)
    key = gap_ref[...] * sigmoid(-fp)
    og_ref[...] = op * sigmoid(op)
    logs = jnp.log1p(-key)
    dec = dec_ref[...]
    tri = (iota((length, length), 0) >= iota((length, length), 1)).astype(F32)
    causal = iota((BLOCK, BLOCK), 0) >= iota((BLOCK, BLOCK), 1)
    half = BLOCK // 2
    for j in range(per):
        c = slice(j * dim, (j + 1) * dim)
        extra = jnp.sum(jnp.where(iota(dec.shape, 1) == step * per + j, dec, 0.0), axis=1, keepdims=True)
        run = dot(tri, logs[:, c] + extra, precision=lax.Precision.HIGHEST)
        q, k, v = query[:, c], key[:, c], value[:, c]
        qd_ref[:, c] = (q * jnp.exp(run)).astype(BF16)
        state = jnp.zeros((dim, dim), F32)
        base = jnp.zeros((1, dim), F32)
        for b in range(length // BLOCK):
            r = slice(b * BLOCK, (b + 1) * BLOCK)
            g, qb, kb, vb = run[r], q[r], k[r], v[r]
            ref = g[half - 1:half]
            last = g[BLOCK - 1:BLOCK]
            qe = (qb * jnp.exp(g - ref)).astype(BF16)
            ke = (kb * jnp.exp(ref - g)).astype(BF16)
            scores = jnp.where(causal, dot(qe, ke, ((1,), (1,))), 0.0).astype(BF16)
            out = dot(scores, vb)
            if b:
                qs = (qb * jnp.exp(g - base)).astype(BF16)
                out += dot(qs, state.astype(BF16), ((1,), (1,)))
            lo_ref[r, c] = out
            kd = (kb * jnp.exp(last - g)).astype(BF16)
            state = state * jnp.exp(last - base) + dot(vb, kd, ((0,), (0,)))
            base = last
        st_ref[j, 0:dim, :] = state.astype(BF16)
        st_ref[j, dim:, :] = jnp.broadcast_to(jnp.exp(base), (st_ref.shape[1] - dim, dim)).astype(BF16)


def mixer(x, gain, wq, wf, wi, wo, gap, dec):
    parts, length, cols = x.shape
    heads, dim = dec.shape[1], wq.shape[1] // dec.shape[1]
    per = 2 if heads % 2 == 0 else 1
    width = per * dim
    depth = wq.shape[0]
    column = pl.BlockSpec((depth, width), lambda i: (0, i))
    rows = pl.BlockSpec((length, width), lambda i: (0, i))
    whole = lambda s: pl.BlockSpec(s, lambda i: (0,) * len(s))
    return pl.pallas_call(
        functools.partial(mixer_kernel, per),
        grid=(heads // per,),
        in_specs=[whole(x.shape), whole((1, depth)), column, column, column, column,
                  pl.BlockSpec((1, width), lambda i: (0, i)), whole(dec.shape)],
        out_specs=[rows, rows, rows, pl.BlockSpec((per, dim + 16, dim), lambda i: (i, 0, 0))],
        out_shape=[jax.ShapeDtypeStruct((length, heads * dim), F32),
                   jax.ShapeDtypeStruct((length, heads * dim), BF16),
                   jax.ShapeDtypeStruct((length, heads * dim), F32),
                   jax.ShapeDtypeStruct((heads, dim + 16, dim), BF16)],
        scratch_shapes=[pltpu.VMEM((length, depth), BF16)],
        compiler_params=pltpu.CompilerParams(vmem_limit_bytes=LIMIT),
        cost_estimate=pl.CostEstimate(flops=10 * 10**9, bytes_accessed=9 * 10**6, transcendentals=10**6),
    )(x, gain.reshape(1, -1), wq, wf, wi, wo, gap.reshape(1, -1), dec)


def tail_kernel(states_ref, lo_ref, qd_ref, og_ref, hg_ref, w_ref, out_ref, gated):
    place = lax.axis_index("ep")
    hops, heads, _, dim = states_ref.shape
    for h in range(heads):
        c = slice(h * dim, (h + 1) * dim)

        def one(hop, state):
            own = states_ref[hop, h, 0:dim, :].astype(F32)
            passing = states_ref[hop, h, dim:dim + 16, :].astype(F32)[0:1]
            return jnp.where(hop < place, state * passing + own, state)

        state = lax.fori_loop(0, hops, one, jnp.zeros((dim, dim), F32))
        out = lo_ref[:, c] + dot(qd_ref[:, c], state.astype(BF16), ((1,), (1,)))
        scale = lax.rsqrt(jnp.mean(out * out, axis=1, keepdims=True) + epsilon)
        gated[:, c] = (out * scale * hg_ref[...].astype(F32) * og_ref[:, c]).astype(BF16)
    parts, _, cols = out_ref.shape
    for p in range(parts):
        out_ref[p] = dot(gated[...], w_ref[:, p * cols:(p + 1) * cols]).astype(BF16)


def tail(states, lo, qd, og, hg, w, parts):
    length, width = lo.shape
    return pl.pallas_call(
        tail_kernel,
        in_specs=[VMEM] * 6,
        out_specs=VMEM,
        out_shape=jax.ShapeDtypeStruct((parts, length, w.shape[1] // parts), BF16),
        scratch_shapes=[pltpu.VMEM((length, width), BF16)],
        compiler_params=pltpu.CompilerParams(vmem_limit_bytes=LIMIT),
        cost_estimate=pl.CostEstimate(flops=10**9, bytes_accessed=5 * 10**6, transcendentals=10**5),
    )(states, lo, qd, og, hg.reshape(1, -1), w)


def ranks(ids, experts):
    tokens = ids.shape[1]
    names = iota((experts, tokens), 0)
    picks = [names == ids[k:k + 1, :] for k in range(ids.shape[0])]
    chosen = functools.reduce(jnp.logical_or, picks)
    before = (iota((tokens, tokens), 0) < iota((tokens, tokens), 1)).astype(BF16)
    return picks, chosen, dot(chosen.astype(BF16), before)


def slot_hits(mask, rank, experts, capacity):
    rows = experts * capacity
    owner = iota((rows, experts), 0) - iota((rows, experts), 1) * capacity
    owner = jnp.logical_and(owner >= 0, owner < capacity).astype(F32)
    tokens = rank.shape[1]
    spread = dot(owner, jnp.where(mask, rank, -1.0))
    spot = dot(owner, iota((experts, tokens), 0).astype(F32)) * capacity
    return (spread >= 0.0) & (spread + spot == iota((rows, tokens), 0).astype(F32))


def dispatch_kernel(experts, capacity, ids_ref, rows_ref, out_ref):
    _, chosen, rank = ranks(ids_ref[...], experts)
    hits = slot_hits(chosen, rank, experts, capacity).astype(BF16)
    out_ref[...] = dot(hits, rows_ref[...]).astype(BF16)


def dispatch(ids, rows, experts, capacity):
    return pl.pallas_call(
        functools.partial(dispatch_kernel, experts, capacity),
        in_specs=[VMEM] * 2,
        out_specs=VMEM,
        out_shape=jax.ShapeDtypeStruct((experts * capacity, rows.shape[1]), BF16),
    )(ids, rows)


def combine_kernel(experts, capacity, ids_ref, scores_ref, back_ref, out_ref):
    picks, _, rank = ranks(ids_ref[...], experts)
    scores = scores_ref[...]
    weights = scores / jnp.sum(scores, axis=1, keepdims=True)
    total = jnp.zeros(out_ref.shape, F32)
    for k, mask in enumerate(picks):
        hits = slot_hits(mask, rank, experts, capacity).astype(BF16)
        total += dot(hits, back_ref[...], ((0,), (0,))) * weights[:, k:k + 1]
    out_ref[...] = total.astype(BF16)


def combine(ids, scores, back, experts, capacity):
    return pl.pallas_call(
        functools.partial(combine_kernel, experts, capacity),
        in_specs=[VMEM] * 3,
        out_specs=VMEM,
        out_shape=jax.ShapeDtypeStruct((ids.shape[1], back.shape[1]), BF16),
    )(ids, scores, back)


def expert_kernel(x_ref, gain_ref, wg_ref, wu_ref, wd_ref, out_ref, normed, total):
    step = pl.program_id(0)
    parts, rows, cols = x_ref.shape

    @pl.when(step == 0)
    def _():
        squares = jnp.zeros((rows, 1), F32)
        for p in range(parts):
            v = x_ref[p].astype(F32)
            squares += jnp.sum(v * v, axis=1, keepdims=True)
        scale = lax.rsqrt(squares / (parts * cols) + epsilon)
        for p in range(parts):
            g = gain_ref[:, p * cols:(p + 1) * cols].astype(F32)
            normed[:, p * cols:(p + 1) * cols] = (x_ref[p].astype(F32) * scale * g).astype(BF16)

    gate = dot(normed[...], wg_ref[0])
    up = dot(normed[...], wu_ref[0])
    hidden = (gate * sigmoid(gate) * up).astype(BF16)
    last = pl.num_programs(0) - 1
    for p in range(parts):
        c = slice(p * cols, (p + 1) * cols)
        part = dot(hidden, wd_ref[0, :, c])

        @pl.when(jnp.logical_and(step == 0, last > 0))
        def _():
            total[:, c] = part

        @pl.when(jnp.logical_and(step > 0, step < last))
        def _():
            total[:, c] += part

        @pl.when(step == last)
        def _():
            out_ref[p] = (jnp.where(step > 0, total[:, c], 0.0) + part).astype(BF16)


def experts_call(x, gain, wg, wu, wd):
    parts, rows, cols = x.shape
    depth, units = wg.shape[1:]
    tile = 256 if units % 256 == 0 else units
    return pl.pallas_call(
        expert_kernel,
        grid=(units // tile,),
        in_specs=[pl.BlockSpec(x.shape, lambda i: (0, 0, 0)), pl.BlockSpec((1, depth), lambda i: (0, 0)),
                  pl.BlockSpec((1, depth, tile), lambda i: (0, 0, i)),
                  pl.BlockSpec((1, depth, tile), lambda i: (0, 0, i)),
                  pl.BlockSpec((1, tile, depth), lambda i: (0, i, 0))],
        out_specs=pl.BlockSpec(x.shape, lambda i: (0, 0, 0)),
        out_shape=jax.ShapeDtypeStruct(x.shape, BF16),
        scratch_shapes=[pltpu.VMEM((rows, depth), BF16), pltpu.VMEM((rows, depth), F32)],
        compiler_params=pltpu.CompilerParams(vmem_limit_bytes=LIMIT),
        cost_estimate=pl.CostEstimate(flops=8 * 10**9, bytes_accessed=10**7, transcendentals=10**6),
    )(x, gain.reshape(1, -1), wg, wu, wd)

MESH = pl.DeviceIdType.MESH
ANY = pl.BlockSpec(memory_space=pl.ANY)
HIGHEST = lax.Precision.HIGHEST
PAIR = 2


def flip(place, bits):
    bit = 1
    while bit <= bits:
        if bits & bit:
            place = place + bit - 2 * bit * lax.rem(lax.div(place, bit), 2)
        bit *= 2
    return place


def block_kernel(cap, mix_hbm, mgain_ref, wq_hbm, wf_hbm, wi_hbm, wo_hbm, gap_ref, dec_ref, hgain_ref, wm_hbm,
                 moe_hbm, egain_ref, ids_ref, scores_ref, wg_hbm, wu_hbm, wd_hbm,
                 mix_out, moe_out,
                 mix_ref, moe_ref, wmix, wm, wg, wu, wd, xall, acc, lo, qd, og, st, pst, cst, fst, states, gated, mixed, mixin,
                 gath, slots, hits, enormed, hidden, psend, precv, nback, tok, tokin, esum, back, total,
                 wsem, xs, xr, zs, zr, gs, gr, ps, pr, bs, br, ss, sr, ms, mr, ts, tr):
    eps, tps = lax.axis_size("ep"), lax.axis_size("tp")
    me, mt = lax.axis_index("ep"), lax.axis_index("tp")
    length, cols = mix_ref.shape
    rows = eps * cap
    heads, _, dim = st.shape
    depth = tps * cols
    units = wg.shape[1]
    ep_peer = [flip(me, k) for k in range(eps)]
    tp_peer = [flip(mt, r) for r in range(tps)]

    def push(src, dst, send, recv, ep=None, tp=None):
        where = {"ep": ep_peer[ep]} if tp is None else {"tp": tp_peer[tp]}
        return pltpu.make_async_remote_copy(src_ref=src, dst_ref=dst, send_sem=send, recv_sem=recv,
                                            device_id=where, device_id_type=MESH)

    sent = []

    def go(copy):
        copy.start()
        sent.append(copy)

    loads = [pltpu.make_async_copy(s, wmix.at[i], wsem.at[i]) for i, s in enumerate((wq_hbm, wf_hbm, wi_hbm, wo_hbm))]
    loads += [pltpu.make_async_copy(wg_hbm.at[0], wg, wsem.at[4]), pltpu.make_async_copy(wu_hbm.at[0], wu, wsem.at[5]),
              pltpu.make_async_copy(wd_hbm.at[0], wd, wsem.at[6]), pltpu.make_async_copy(wm_hbm, wm, wsem.at[7])]
    rowload = [pltpu.make_async_copy(mix_hbm, mix_ref, wsem.at[8]), pltpu.make_async_copy(moe_hbm, moe_ref, wsem.at[9])]

    barrier = pltpu.get_barrier_semaphore()
    for k in range(1, eps):
        pl.semaphore_signal(barrier, inc=1, device_id={"ep": ep_peer[k]}, device_id_type=MESH)
    for r in range(1, tps):
        pl.semaphore_signal(barrier, inc=1, device_id={"tp": tp_peer[r]}, device_id_type=MESH)
    for load in rowload + loads:
        load.start()
    rowload[0].wait()
    pl.semaphore_wait(barrier, eps + tps - 2)

    half = length // 2
    go(push(mix_ref, xall.at[mt], xs.at[0], xr.at[0], tp=1))
    go(push(mix_ref, xall.at[mt], xs.at[1], xr.at[1], tp=2))

    experts = eps
    names = iota((length, experts), 1)
    eye = iota((length, length), 0) == iota((length, length), 1)
    ids = dot(eye.astype(BF16), ids_ref[...].astype(F32).astype(BF16), ((1,), (1,))).astype(jnp.int32)
    picks = [ids[:, j:j + 1] == names for j in range(ids.shape[1])]
    chosen = functools.reduce(jnp.logical_or, picks)
    before = (iota((length, length), 0) > iota((length, length), 1)).astype(BF16)
    rank = dot(before, chosen.astype(BF16)).astype(jnp.int32)
    spot = rank + jnp.bitwise_xor(names, me) * cap
    rowload[1].wait()
    both = None
    for j, pick in enumerate(picks):
        at = jnp.sum(jnp.where(pick, spot, 0), axis=1, keepdims=True)
        hit = (iota((length, rows), 1) == at).astype(F32)
        hits[j] = hit.astype(BF16)
        both = hit if both is None else both + hit
    made = dot(both.astype(BF16), moe_ref[...], ((0,), (0,))).astype(BF16)
    slots[...] = made
    gath[mt, 0:cap, :] = made[0:cap]
    for k in range(1, eps):
        r = slice(k * cap, (k + 1) * cap)
        go(push(slots.at[r], gath.at[mt, r], zs.at[k], zr.at[k], ep=k))

    def rowsof(k, part=None):
        if part is None:
            return pl.ds(k * cap, cap)
        return pl.ds(k * cap + part * (cap // 2), cap // 2)

    def spread(k):
        if k:
            push(slots.at[rowsof(k)], gath.at[mt, rowsof(k)], zs.at[k], zr.at[k], ep=k).wait_recv()
        for n, r in enumerate((1, 2)):
            ref = gath.at[mt, rowsof(k)]
            go(push(ref, ref, gs.at[k, n], gr.at[k, n], tp=r))

    def relay(k):
        for n, (source, target) in enumerate(((1, 2), (2, 1))):
            whole = gath.at[tp_peer[source], rowsof(k)]
            push(whole, whole, gs.at[k, n], gr.at[k, n], tp=source).wait_recv()
            ref = gath.at[tp_peer[source], rowsof(k, n)]
            go(push(ref, ref, gs.at[k, 2 + n], gr.at[k, 2 + n], tp=target))

    def complete(k):
        for n, via in enumerate((2, 1)):
            ref = gath.at[tp_peer[3], rowsof(k, n)]
            push(ref, ref, gs.at[k, 2 + n], gr.at[k, 2 + n], tp=via).wait_recv()

    def relay_mix():
        for n, (source, target) in enumerate(((1, 2), (2, 1))):
            whole = xall.at[tp_peer[source]]
            push(whole, whole, xs.at[n], xr.at[n], tp=source).wait_recv()
            ref = xall.at[tp_peer[source], pl.ds(n * half, half)]
            go(push(ref, ref, xs.at[2 + n], xr.at[2 + n], tp=target))

    def complete_mix():
        for n, via in enumerate((2, 1)):
            ref = xall.at[tp_peer[3], pl.ds(n * half, half)]
            push(ref, ref, xs.at[2 + n], xr.at[2 + n], tp=via).wait_recv()

    S, R = (lambda k: functools.partial(spread, k)), (lambda k: functools.partial(relay, k))
    agenda = []
    for k in range(1, eps):
        agenda += [S(k + 2), R(k)] if k + 2 < eps else [R(k)]
    spot = 2 * (eps // 2 - 1) - 1
    if eps // 2 + 1 < eps:
        agenda[spot - 1:spot + 1] = agenda[spot - 1:spot + 1][::-1]
    near_end = len(agenda) - spot if eps // 2 + 1 < eps else 0

    def poll(count=1):
        for _ in range(min(count, len(agenda))):
            agenda.pop(0)()

    mgain, egain = mgain_ref[...].astype(F32), egain_ref[...].astype(F32)
    lanes = mgain.shape[1]
    per_shard = cols // lanes
    squares = [jnp.zeros((length, 1), F32)]

    def project(r, ref, first):
        p = tp_peer[r]
        v = ref[...].astype(F32)
        squares[0] += jnp.sum(v * v, axis=1, keepdims=True)
        gains = mgain[0:per_shard]
        for i in range(1, tps):
            gains = jnp.where(p == i, mgain[i * per_shard:(i + 1) * per_shard], gains)
        v = jnp.concatenate([v[:, i * lanes:(i + 1) * lanes] * gains[i:i + 1] for i in range(per_shard)], axis=1)
        v = v.astype(BF16)
        w = pl.ds(pl.multiple_of(p * cols, cols), cols)
        for i in range(4):
            part = dot(v, wmix[i, w, :])
            acc[i] = part if first else acc[i] + part

    S(0)()
    for load in loads[:4]:
        load.wait()
    project(0, mix_ref, True)
    relay_mix()
    S(1)()
    project(1, xall.at[tp_peer[1]], False)
    R(0)()
    S(2)()
    project(2, xall.at[tp_peer[2]], False)
    complete_mix()
    poll(1)
    project(3, xall.at[tp_peer[3]], False)
    scale = lax.rsqrt(squares[0] / depth + epsilon)
    poll(1)

    tri = (iota((length, length), 0) >= iota((length, length), 1)).astype(F32)
    extra = dot(tri, dec_ref[...], ((1,), (1,)), precision=HIGHEST)
    causal = iota((BLOCK, BLOCK), 0) >= iota((BLOCK, BLOCK), 1)
    mid = BLOCK // 2
    per = 2 if heads % 2 == 0 else 1

    def mix_step(step):
        w = slice(step * per * dim, (step + 1) * per * dim)
        qp, fp, value, op = [acc[i, :, w] * scale for i in range(4)]
        value = value.astype(BF16)
        query = qp * sigmoid(qp)
        key = gap_ref[:, w] * sigmoid(-fp)
        og[:, w] = op * sigmoid(op)
        logs = jnp.log1p(-key)
        for j in range(per):
            h = step * per + j
            cl = slice(j * dim, (j + 1) * dim)
            c = slice(h * dim, (h + 1) * dim)
            run = dot(tri, logs[:, cl], precision=HIGHEST) + extra[:, h:h + 1]
            q, k, v = query[:, cl], key[:, cl], value[:, cl]
            qd[:, c] = (q * jnp.exp(run)).astype(BF16)
            state = jnp.zeros((dim, dim), F32)
            base = jnp.zeros((1, dim), F32)
            for b in range(length // BLOCK):
                r = slice(b * BLOCK, (b + 1) * BLOCK)
                g, qb, kb, vb = run[r], q[r], k[r], v[r]
                ref = g[mid - 1:mid]
                last = g[BLOCK - 1:BLOCK]
                qe = (qb * jnp.exp(g - ref)).astype(BF16)
                ke = (kb * jnp.exp(ref - g)).astype(BF16)
                scores = jnp.where(causal, dot(qe, ke, ((1,), (1,))), 0.0).astype(BF16)
                out = dot(scores, vb)
                if b:
                    qs = (qb * jnp.exp(g - base)).astype(BF16)
                    out += dot(qs, state.astype(BF16), ((1,), (1,)))
                lo[r, c] = out
                kd = (kb * jnp.exp(last - g)).astype(BF16)
                state = state * jnp.exp(last - base) + dot(vb, kd, ((0,), (0,)))
                base = last
            st[h, 0:dim, :] = state.astype(BF16)
            st[h, dim:, :] = jnp.broadcast_to(jnp.exp(base), (st.shape[1] - dim, dim)).astype(BF16)
            poll(1)

    odd = lax.rem(me, PAIR)
    pair = lax.div(me, PAIR)
    swap = push(st, pst, ss.at[1], sr.at[0], ep=1)
    own_half = pl.ds(odd * (heads // 2), heads // 2)
    other_half = pl.ds((1 - odd) * (heads // 2), heads // 2)
    trade = push(fst.at[own_half], fst.at[own_half], ss.at[0], sr.at[eps - 1], ep=1)

    def joined_copy(k):
        return push(cst, states.at[pair], ss.at[k], sr.at[1 + pair], ep=k)

    def parts_of(ref, h):
        return ref[h, 0:dim, :].astype(F32), ref[h, dim:dim + 16, :].astype(F32)[0:1]

    def join_states():
        swap.wait_recv()
        for i in range(heads // 2):
            h = odd * (heads // 2) + i
            (own, keep), (other, pass_on) = parts_of(st, h), parts_of(pst, h)
            cst[i, 0:dim, :] = jnp.where(odd == 1, other * keep + own, own * pass_on + other).astype(BF16)
            cst[i, dim:, :] = jnp.broadcast_to(keep * pass_on, (st.shape[1] - dim, dim)).astype(BF16)
        for k in range(PAIR, eps, PAIR):
            @pl.when(ep_peer[k] > me)
            def _():
                joined_copy(k).start()

    def fold_states():
        @pl.loop(0, pair)
        def _(hop):
            pltpu.make_async_remote_copy(src_ref=cst, dst_ref=states.at[hop], send_sem=ss.at[0], recv_sem=sr.at[1 + hop],
                                         device_id={"ep": hop * PAIR + odd}, device_id_type=MESH).wait_recv()

        for i in range(heads // 2):
            def one(hop, state):
                own, pass_on = parts_of(states.at[hop], i)
                return state * pass_on + own

            state = lax.fori_loop(0, pair, one, jnp.zeros((dim, dim), F32))
            fst[odd * (heads // 2) + i] = state.astype(BF16)
        go(trade)

    def finish_mixer():
        push(fst.at[other_half], fst.at[other_half], ss.at[0], sr.at[eps - 1], ep=1).wait_recv()
        for h in range(heads):
            c = slice(h * dim, (h + 1) * dim)
            state = fst[h].astype(F32)
            other, pass_on = parts_of(pst, h)
            state = jnp.where(odd == 1, state * pass_on + other, state)
            out = lo[:, c] + dot(qd[:, c], state.astype(BF16), ((1,), (1,)))
            scale = lax.rsqrt(jnp.mean(out * out, axis=1, keepdims=True) + epsilon)
            gated[:, c] = (out * scale * hgain_ref[...].astype(F32) * og[:, c]).astype(BF16)
        loads[7].wait()
        for r in (3, 1, 2, 0):
            block = wm[:, pl.ds(pl.multiple_of(tp_peer[r] * cols, cols), cols)]
            mixed[r] = dot(gated[...], block).astype(BF16)

    tile = 256 if units % 256 == 0 else units
    def feed(chunks, polls=()):
        for k in chunks:
            if k in polls:
                poll(1)
            complete(k)
            r = chunk(k)
            squares = jnp.zeros((cap, 1), F32)
            for p in range(tps):
                v = gath[p, r, :].astype(F32)
                squares += jnp.sum(v * v, axis=1, keepdims=True)
            scale = lax.rsqrt(squares / depth + epsilon)
            for p in range(tps):
                for i in range(cols // lanes):
                    s = slice(i * lanes, (i + 1) * lanes)
                    n = p * (cols // lanes) + i
                    c = slice(n * lanes, (n + 1) * lanes)
                    enormed[r, c] = (gath[p, r, s].astype(F32) * scale * egain[n:n + 1]).astype(BF16)

    def chunk(k):
        return slice(k * cap, (k + 1) * cap)

    def span(chunks):
        return slice(chunks[0] * cap, (chunks[-1] + 1) * cap)

    def upward(chunks, polls=()):
        r = span(chunks)
        for u in range(units // tile):
            c = slice(u * tile, (u + 1) * tile)
            gate = dot(enormed[r, :], wg[:, c])
            up = dot(enormed[r, :], wu[:, c])
            hidden[0:len(chunks) * cap, c] = (gate * sigmoid(gate) * up).astype(BF16)
            if u in polls:
                poll(1)

    def downward(chunks, polls=()):
        r = span(chunks)
        for t in (3, 1, 2, 0):
            block = wd[:, pl.ds(pl.multiple_of(tp_peer[t] * cols, cols), cols)]
            psend[t, r, :] = dot(hidden[0:len(chunks) * cap, :], block).astype(BF16)
            if t in polls:
                poll(1)

    def summing(src, dst, a, b, send, recv):
        def part(n, index, target, r, tp):
            return push(src.at[index, r], dst.at[target, r], send.at[n], recv.at[n], tp=tp)

        first = [part(0, 3, 3, a, 1), part(1, 3, 3, b, 2), part(2, 1, 1, a, 1), part(3, 2, 2, b, 2)]
        second = [part(4, 2, 2, a, 2), part(5, 1, 1, b, 1)]

        def start():
            for copy in first:
                go(copy)

        def merge():
            first[0].wait_recv()
            src[2, a, :] = (src[2, a, :].astype(F32) + dst[3, a, :].astype(F32)).astype(BF16)
            first[1].wait_recv()
            src[1, b, :] = (src[1, b, :].astype(F32) + dst[3, b, :].astype(F32)).astype(BF16)
            for copy in second:
                go(copy)

        def finish():
            for copy in first[2:] + second:
                copy.wait_recv()

        def value(r):
            return src[0, r, :].astype(F32) + dst[1, r, :].astype(F32) + dst[2, r, :].astype(F32)

        return start, merge, finish, value

    near = list(range(eps // 2))
    far = [[k, k + 1] for k in range(eps // 2, eps, 2)]
    nrows = len(near) * cap
    sums = [summing(psend, precv, chunk(a), chunk(b), ps.at[g], pr.at[g]) for g, (a, b) in enumerate(far)]
    mixsum = summing(mixed, mixin, slice(0, half), slice(half, length), ms, mr)
    toksum = summing(tok, tokin, slice(0, half), slice(half, length), ts, tr)

    def near_copy(k):
        return push(psend.at[:, chunk(k)], nback.at[:, chunk(k)], bs.at[k], br.at[k], ep=k)

    def give_near():
        for k in near[1:]:
            go(near_copy(k))
        nback[:, chunk(0), :] = psend[:, chunk(0), :]

    def take_near():
        for k in near[1:]:
            near_copy(k).wait_recv()
        for t in (3, 1, 2, 0):
            value = jnp.zeros((length, cols), F32)
            for j in range(hits.shape[0]):
                value += dot(hits[j, :, 0:nrows], nback[t]) * weights[:, j:j + 1]
            tok[t] = value.astype(BF16)

    def give_far(g):
        _, _, finish, value = sums[g]
        finish()
        for k in far[g]:
            r = chunk(k)
            esum[r, :] = value(r).astype(BF16)
            go(push(esum.at[r], back.at[r], bs.at[k], br.at[k], ep=k))

    def take_far(g):
        for k in far[g]:
            push(esum.at[chunk(k)], back.at[chunk(k)], bs.at[k], br.at[k], ep=k).wait_recv()
        r = span(far[g])
        value = jnp.zeros((length, cols), F32)
        for j in range(hits.shape[0]):
            value += dot(hits[j, :, r], back[r, :]) * weights[:, j:j + 1]
        return value

    scores = scores_ref[...]
    weights = dot(eye.astype(F32), scores / jnp.sum(scores, axis=0, keepdims=True), ((1,), (1,)), precision=HIGHEST)

    for step in range(heads // per):
        mix_step(step)
    go(swap)
    for load in loads[4:7]:
        load.wait()
    poll(len(agenda) - near_end)
    poll(2)
    join_states()
    feed(near, polls=near[-1:])
    upward(near, polls=(0, 1))
    downward(near, polls=(1,))
    give_near()
    poll(len(agenda) - 1)
    for g, chunks in enumerate(far):
        feed(chunks)
        upward(chunks)
        if g == 0:
            poll(1)
        downward(chunks)
        sums[g][0]()
        if g:
            sums[g - 1][1]()
    fold_states()
    sums[-1][1]()
    finish_mixer()
    mixsum[0]()
    for g in range(len(far) - 1):
        give_far(g)
    take_near()
    toksum[0]()
    mixsum[1]()
    give_far(len(far) - 1)
    toksum[1]()
    value = take_far(0)
    for g in range(1, len(far)):
        value += take_far(g)
    total[...] = value
    mixsum[2]()
    mix_out[...] = mixsum[3](slice(0, length)).astype(BF16)
    toksum[2]()
    moe_out[...] = (total[...] + toksum[3](slice(0, length))).astype(BF16)

    for copy in sent:
        copy.wait_send()
    for k in range(PAIR, eps, PAIR):
        @pl.when(ep_peer[k] > me)
        def _():
            joined_copy(k).wait_send()


def whole_block(mix_rows, mix_gain, wq, wf, wi, wo, gap, dec, hgain, wm, moe_rows, moe_gain, ids, scores, wg, wu, wd):
    eps, tps = lax.axis_size("ep"), lax.axis_size("tp")
    length, cols = mix_rows.shape
    top = ids.shape[1]
    cap = length * top * 3 // (2 * eps)
    rows = eps * cap
    heads = dec.shape[0]
    width = wq.shape[1]
    dim = width // heads
    depth, units = wg.shape[1:]
    dma = lambda *s: pltpu.SemaphoreType.DMA(s)
    out = jax.ShapeDtypeStruct((length, cols), BF16)
    scratch = [
        pltpu.VMEM((length, cols), BF16), pltpu.VMEM((length, cols), BF16),
        pltpu.VMEM((4, depth, width), BF16), pltpu.VMEM((width, depth), BF16),
        pltpu.VMEM((depth, units), BF16), pltpu.VMEM((depth, units), BF16), pltpu.VMEM((units, depth), BF16),
        pltpu.VMEM((tps, length, cols), BF16), pltpu.VMEM((4, length, width), F32),
        pltpu.VMEM((length, width), F32), pltpu.VMEM((length, width), BF16), pltpu.VMEM((length, width), F32),
        pltpu.VMEM((heads, dim + 16, dim), BF16), pltpu.VMEM((heads, dim + 16, dim), BF16),
        pltpu.VMEM((heads // 2, dim + 16, dim), BF16), pltpu.VMEM((heads, dim, dim), BF16),
        pltpu.VMEM((eps // PAIR, heads // 2, dim + 16, dim), BF16),
        pltpu.VMEM((length, width), BF16), pltpu.VMEM((tps, length, cols), BF16), pltpu.VMEM((tps, length, cols), BF16),
        pltpu.VMEM((tps, rows, cols), BF16), pltpu.VMEM((rows, cols), BF16), pltpu.VMEM((top, length, rows), BF16),
        pltpu.VMEM((rows, depth), BF16), pltpu.VMEM((rows // 2, units), BF16),
        pltpu.VMEM((tps, rows, cols), BF16), pltpu.VMEM((tps, rows, cols), BF16),
        pltpu.VMEM((tps, rows // 2, cols), BF16), pltpu.VMEM((tps, length, cols), BF16), pltpu.VMEM((tps, length, cols), BF16),
        pltpu.VMEM((rows, cols), BF16), pltpu.VMEM((rows, cols), BF16), pltpu.VMEM((length, cols), F32),
        dma(10), dma(4), dma(4), dma(eps), dma(eps), dma(eps, 4), dma(eps, 4), dma(eps // 2, 6), dma(eps // 2, 6),
        dma(eps), dma(eps), dma(eps), dma(eps), dma(6), dma(6), dma(6), dma(6),
    ]
    return pl.pallas_call(
        functools.partial(block_kernel, cap),
        in_specs=[ANY, VMEM, ANY, ANY, ANY, ANY, VMEM, VMEM, VMEM, ANY, ANY, VMEM, VMEM, VMEM, ANY, ANY, ANY],
        out_specs=[VMEM, VMEM],
        out_shape=[out, out],
        scratch_shapes=scratch,
        compiler_params=pltpu.CompilerParams(vmem_limit_bytes=LIMIT, collective_id=0, has_side_effects=True),
    )(mix_rows, mix_gain.reshape(-1, 128), wq, wf, wi, wo, gap.reshape(1, -1), dec, hgain.reshape(1, -1), wm,
      moe_rows, moe_gain.reshape(-1, 128), ids.T, scores.T, wg, wu, wd)


def fits(eps, tps, mix_rows, dec, route_ids, w_gate):
    tokens, cols = mix_rows.shape
    top = route_ids.shape[1]
    cap = tokens * top * 3 // (2 * eps)
    square = tps == 4 and dec.shape[0] % 2 == 0 and eps >= 4 and eps & (eps - 1) == 0
    aligned = cap % 32 == 0 and cols % 128 == 0 and tokens % (2 * BLOCK) == 0 and w_gate.shape[2] % 128 == 0
    return square and aligned and w_gate.shape[0] == 1


def per_device(mix_rows, mix_gain, w_query, w_forget, w_input, w_outgate, forget_gap, decay_extra,
               head_gain, w_mixout, moe_rows, moe_gain, route_ids, route_scores, w_gate, w_up, w_down):
    eps, tps = lax.axis_size("ep"), lax.axis_size("tp")
    if fits(eps, tps, mix_rows, decay_extra, route_ids, w_gate):
        return whole_block(mix_rows, mix_gain, w_query, w_forget, w_input, w_outgate, forget_gap, decay_extra,
                           head_gain, w_mixout, moe_rows, moe_gain, route_ids, route_scores, w_gate, w_up, w_down)
    tokens, top = route_ids.shape
    experts = w_gate.shape[0] * eps
    capacity = tokens * top * 3 // (2 * experts)
    cols = mix_rows.shape[1]
    ids = route_ids.T
    slots = dispatch(ids, moe_rows, experts, capacity)
    arrived = lax.all_to_all(slots.reshape(eps, -1, cols), "ep", split_axis=0, concat_axis=0, tiled=True)
    gathered = lax.all_gather(arrived.reshape(-1, cols), "tp", axis=0)
    mix_whole = lax.all_gather(mix_rows, "tp", axis=0)
    lo, qd, og, st = mixer(mix_whole, mix_gain, w_query, w_forget, w_input, w_outgate, forget_gap, decay_extra.T)
    product = experts_call(gathered, moe_gain, w_gate, w_up, w_down)
    expert_sum = lax.psum_scatter(product, "tp", scatter_dimension=0)
    states = lax.all_gather(st, "ep", axis=0)
    mixed = tail(states, lo, qd, og, head_gain, w_mixout, tps)
    mix_out = lax.psum_scatter(mixed, "tp", scatter_dimension=0)
    back = lax.all_to_all(expert_sum.reshape(eps, -1, cols), "ep", split_axis=0, concat_axis=0, tiled=True)
    moe_out = combine(ids, route_scores, back.reshape(-1, cols), experts, capacity)
    return (mix_out, moe_out)


def solution(mesh):
    placed = (
        P("ep", "tp"), P(), P(None, "tp"), P(None, "tp"), P(None, "tp"), P(None, "tp"), P("tp"),
        P("tp", "ep"), P(), P("tp", None), P("ep", "tp"), P(), P("ep", None), P("ep", None),
        P("ep", None, "tp"), P("ep", None, "tp"), P("ep", "tp", None),
    )
    return jax.shard_map(
        per_device, mesh=mesh, in_specs=placed,
        out_specs=(P("ep", "tp"), P("ep", "tp")), check_vma=False,
    )
```

```python
import functools

import jax
import jax.numpy as jnp
from jax import lax
from jax.experimental import pallas as pl
from jax.experimental.pallas import tpu as pltpu
from jax.sharding import PartitionSpec as P

BLOCK = 64
epsilon = 1e-06
F32 = jnp.float32
BF16 = jnp.bfloat16
VMEM = pl.BlockSpec(memory_space=pltpu.VMEM)
LIMIT = 60 * 1024 * 1024


def dot(a, b, dims=((1,), (0,)), precision=None):
    return lax.dot_general(a, b, (dims, ((), ())), precision=precision, preferred_element_type=F32)


def sigmoid(x):
    return 1.0 / (1.0 + jnp.exp(-x))


def iota(shape, dim):
    return lax.broadcasted_iota(jnp.int32, shape, dim)


def mixer_kernel(per, x_ref, gain_ref, wq_ref, wf_ref, wi_ref, wo_ref, gap_ref, dec_ref,
                 lo_ref, qd_ref, og_ref, st_ref, normed):
    step = pl.program_id(0)
    length = normed.shape[0]
    dim = st_ref.shape[2]
    parts, _, cols = x_ref.shape

    @pl.when(step == 0)
    def _():
        total = jnp.zeros((length, 1), F32)
        for p in range(parts):
            v = x_ref[p].astype(F32)
            total += jnp.sum(v * v, axis=1, keepdims=True)
        scale = lax.rsqrt(total / (parts * cols) + epsilon)
        for p in range(parts):
            g = gain_ref[:, p * cols:(p + 1) * cols].astype(F32)
            normed[:, p * cols:(p + 1) * cols] = (x_ref[p].astype(F32) * scale * g).astype(BF16)

    n = normed[...]
    qp = dot(n, wq_ref[...])
    fp = dot(n, wf_ref[...])
    value = dot(n, wi_ref[...]).astype(BF16)
    op = dot(n, wo_ref[...])
    query = qp * sigmoid(qp)
    key = gap_ref[...] * sigmoid(-fp)
    og_ref[...] = op * sigmoid(op)
    logs = jnp.log1p(-key)
    dec = dec_ref[...]
    tri = (iota((length, length), 0) >= iota((length, length), 1)).astype(F32)
    causal = iota((BLOCK, BLOCK), 0) >= iota((BLOCK, BLOCK), 1)
    half = BLOCK // 2
    for j in range(per):
        c = slice(j * dim, (j + 1) * dim)
        extra = jnp.sum(jnp.where(iota(dec.shape, 1) == step * per + j, dec, 0.0), axis=1, keepdims=True)
        run = dot(tri, logs[:, c] + extra, precision=lax.Precision.HIGHEST)
        q, k, v = query[:, c], key[:, c], value[:, c]
        qd_ref[:, c] = (q * jnp.exp(run)).astype(BF16)
        state = jnp.zeros((dim, dim), F32)
        base = jnp.zeros((1, dim), F32)
        for b in range(length // BLOCK):
            r = slice(b * BLOCK, (b + 1) * BLOCK)
            g, qb, kb, vb = run[r], q[r], k[r], v[r]
            ref = g[half - 1:half]
            last = g[BLOCK - 1:BLOCK]
            qe = (qb * jnp.exp(g - ref)).astype(BF16)
            ke = (kb * jnp.exp(ref - g)).astype(BF16)
            scores = jnp.where(causal, dot(qe, ke, ((1,), (1,))), 0.0).astype(BF16)
            out = dot(scores, vb)
            if b:
                qs = (qb * jnp.exp(g - base)).astype(BF16)
                out += dot(qs, state.astype(BF16), ((1,), (1,)))
            lo_ref[r, c] = out
            kd = (kb * jnp.exp(last - g)).astype(BF16)
            state = state * jnp.exp(last - base) + dot(vb, kd, ((0,), (0,)))
            base = last
        st_ref[j, 0:dim, :] = state.astype(BF16)
        st_ref[j, dim:, :] = jnp.broadcast_to(jnp.exp(base), (st_ref.shape[1] - dim, dim)).astype(BF16)


def mixer(x, gain, wq, wf, wi, wo, gap, dec):
    parts, length, cols = x.shape
    heads, dim = dec.shape[1], wq.shape[1] // dec.shape[1]
    per = 2 if heads % 2 == 0 else 1
    width = per * dim
    depth = wq.shape[0]
    column = pl.BlockSpec((depth, width), lambda i: (0, i))
    rows = pl.BlockSpec((length, width), lambda i: (0, i))
    whole = lambda s: pl.BlockSpec(s, lambda i: (0,) * len(s))
    return pl.pallas_call(
        functools.partial(mixer_kernel, per),
        grid=(heads // per,),
        in_specs=[whole(x.shape), whole((1, depth)), column, column, column, column,
                  pl.BlockSpec((1, width), lambda i: (0, i)), whole(dec.shape)],
        out_specs=[rows, rows, rows, pl.BlockSpec((per, dim + 16, dim), lambda i: (i, 0, 0))],
        out_shape=[jax.ShapeDtypeStruct((length, heads * dim), F32),
                   jax.ShapeDtypeStruct((length, heads * dim), BF16),
                   jax.ShapeDtypeStruct((length, heads * dim), F32),
                   jax.ShapeDtypeStruct((heads, dim + 16, dim), BF16)],
        scratch_shapes=[pltpu.VMEM((length, depth), BF16)],
        compiler_params=pltpu.CompilerParams(vmem_limit_bytes=LIMIT),
        cost_estimate=pl.CostEstimate(flops=10 * 10**9, bytes_accessed=9 * 10**6, transcendentals=10**6),
    )(x, gain.reshape(1, -1), wq, wf, wi, wo, gap.reshape(1, -1), dec)


def tail_kernel(states_ref, lo_ref, qd_ref, og_ref, hg_ref, w_ref, out_ref, gated):
    place = lax.axis_index("ep")
    hops, heads, _, dim = states_ref.shape
    for h in range(heads):
        c = slice(h * dim, (h + 1) * dim)

        def one(hop, state):
            own = states_ref[hop, h, 0:dim, :].astype(F32)
            passing = states_ref[hop, h, dim:dim + 16, :].astype(F32)[0:1]
            return jnp.where(hop < place, state * passing + own, state)

        state = lax.fori_loop(0, hops, one, jnp.zeros((dim, dim), F32))
        out = lo_ref[:, c] + dot(qd_ref[:, c], state.astype(BF16), ((1,), (1,)))
        scale = lax.rsqrt(jnp.mean(out * out, axis=1, keepdims=True) + epsilon)
        gated[:, c] = (out * scale * hg_ref[...].astype(F32) * og_ref[:, c]).astype(BF16)
    parts, _, cols = out_ref.shape
    for p in range(parts):
        out_ref[p] = dot(gated[...], w_ref[:, p * cols:(p + 1) * cols]).astype(BF16)


def tail(states, lo, qd, og, hg, w, parts):
    length, width = lo.shape
    return pl.pallas_call(
        tail_kernel,
        in_specs=[VMEM] * 6,
        out_specs=VMEM,
        out_shape=jax.ShapeDtypeStruct((parts, length, w.shape[1] // parts), BF16),
        scratch_shapes=[pltpu.VMEM((length, width), BF16)],
        compiler_params=pltpu.CompilerParams(vmem_limit_bytes=LIMIT),
        cost_estimate=pl.CostEstimate(flops=10**9, bytes_accessed=5 * 10**6, transcendentals=10**5),
    )(states, lo, qd, og, hg.reshape(1, -1), w)


def ranks(ids, experts):
    tokens = ids.shape[1]
    names = iota((experts, tokens), 0)
    picks = [names == ids[k:k + 1, :] for k in range(ids.shape[0])]
    chosen = functools.reduce(jnp.logical_or, picks)
    before = (iota((tokens, tokens), 0) < iota((tokens, tokens), 1)).astype(BF16)
    return picks, chosen, dot(chosen.astype(BF16), before)


def slot_hits(mask, rank, experts, capacity):
    rows = experts * capacity
    owner = iota((rows, experts), 0) - iota((rows, experts), 1) * capacity
    owner = jnp.logical_and(owner >= 0, owner < capacity).astype(F32)
    tokens = rank.shape[1]
    spread = dot(owner, jnp.where(mask, rank, -1.0))
    spot = dot(owner, iota((experts, tokens), 0).astype(F32)) * capacity
    return (spread >= 0.0) & (spread + spot == iota((rows, tokens), 0).astype(F32))


def dispatch_kernel(experts, capacity, ids_ref, rows_ref, out_ref):
    _, chosen, rank = ranks(ids_ref[...], experts)
    hits = slot_hits(chosen, rank, experts, capacity).astype(BF16)
    out_ref[...] = dot(hits, rows_ref[...]).astype(BF16)


def dispatch(ids, rows, experts, capacity):
    return pl.pallas_call(
        functools.partial(dispatch_kernel, experts, capacity),
        in_specs=[VMEM] * 2,
        out_specs=VMEM,
        out_shape=jax.ShapeDtypeStruct((experts * capacity, rows.shape[1]), BF16),
    )(ids, rows)


def combine_kernel(experts, capacity, ids_ref, scores_ref, back_ref, out_ref):
    picks, _, rank = ranks(ids_ref[...], experts)
    scores = scores_ref[...]
    weights = scores / jnp.sum(scores, axis=1, keepdims=True)
    total = jnp.zeros(out_ref.shape, F32)
    for k, mask in enumerate(picks):
        hits = slot_hits(mask, rank, experts, capacity).astype(BF16)
        total += dot(hits, back_ref[...], ((0,), (0,))) * weights[:, k:k + 1]
    out_ref[...] = total.astype(BF16)


def combine(ids, scores, back, experts, capacity):
    return pl.pallas_call(
        functools.partial(combine_kernel, experts, capacity),
        in_specs=[VMEM] * 3,
        out_specs=VMEM,
        out_shape=jax.ShapeDtypeStruct((ids.shape[1], back.shape[1]), BF16),
    )(ids, scores, back)


def expert_kernel(x_ref, gain_ref, wg_ref, wu_ref, wd_ref, out_ref, normed, total):
    step = pl.program_id(0)
    parts, rows, cols = x_ref.shape

    @pl.when(step == 0)
    def _():
        squares = jnp.zeros((rows, 1), F32)
        for p in range(parts):
            v = x_ref[p].astype(F32)
            squares += jnp.sum(v * v, axis=1, keepdims=True)
        scale = lax.rsqrt(squares / (parts * cols) + epsilon)
        for p in range(parts):
            g = gain_ref[:, p * cols:(p + 1) * cols].astype(F32)
            normed[:, p * cols:(p + 1) * cols] = (x_ref[p].astype(F32) * scale * g).astype(BF16)

    gate = dot(normed[...], wg_ref[0])
    up = dot(normed[...], wu_ref[0])
    hidden = (gate * sigmoid(gate) * up).astype(BF16)
    last = pl.num_programs(0) - 1
    for p in range(parts):
        c = slice(p * cols, (p + 1) * cols)
        part = dot(hidden, wd_ref[0, :, c])

        @pl.when(jnp.logical_and(step == 0, last > 0))
        def _():
            total[:, c] = part

        @pl.when(jnp.logical_and(step > 0, step < last))
        def _():
            total[:, c] += part

        @pl.when(step == last)
        def _():
            out_ref[p] = (jnp.where(step > 0, total[:, c], 0.0) + part).astype(BF16)


def experts_call(x, gain, wg, wu, wd):
    parts, rows, cols = x.shape
    depth, units = wg.shape[1:]
    tile = 256 if units % 256 == 0 else units
    return pl.pallas_call(
        expert_kernel,
        grid=(units // tile,),
        in_specs=[pl.BlockSpec(x.shape, lambda i: (0, 0, 0)), pl.BlockSpec((1, depth), lambda i: (0, 0)),
                  pl.BlockSpec((1, depth, tile), lambda i: (0, 0, i)),
                  pl.BlockSpec((1, depth, tile), lambda i: (0, 0, i)),
                  pl.BlockSpec((1, tile, depth), lambda i: (0, i, 0))],
        out_specs=pl.BlockSpec(x.shape, lambda i: (0, 0, 0)),
        out_shape=jax.ShapeDtypeStruct(x.shape, BF16),
        scratch_shapes=[pltpu.VMEM((rows, depth), BF16), pltpu.VMEM((rows, depth), F32)],
        compiler_params=pltpu.CompilerParams(vmem_limit_bytes=LIMIT),
        cost_estimate=pl.CostEstimate(flops=8 * 10**9, bytes_accessed=10**7, transcendentals=10**6),
    )(x, gain.reshape(1, -1), wg, wu, wd)

MESH = pl.DeviceIdType.MESH
ANY = pl.BlockSpec(memory_space=pl.ANY)
HIGHEST = lax.Precision.HIGHEST
PAIR = 2


def flip(place, bits):
    bit = 1
    while bit <= bits:
        if bits & bit:
            place = place + bit - 2 * bit * lax.rem(lax.div(place, bit), 2)
        bit *= 2
    return place


def block_kernel(cap, mix_hbm, mgain_hbm, wq_hbm, wf_hbm, wi_hbm, wo_hbm, gap_hbm, dec_hbm, hgain_hbm, wm_hbm,
                 moe_hbm, egain_hbm, ids_hbm, scores_hbm, wg_hbm, wu_hbm, wd_hbm,
                 mix_out, moe_out, mgain_ref, gap_ref, dec_ref, hgain_ref, egain_ref, ids_ref, scores_ref,
                 mix_ref, moe_ref, wmix, wm, wg, wu, wd, xall, acc, lo, qd, og, st, pst, cst, fst, states, gated, mixed, mixin,
                 gath, slots, hits, enormed, hidden, psend, precv, nback, tok, tokin, esum, back, total,
                 wsem, out_sem, xr, zr, gr, pr, br, sr, mr, tr):
    eps, tps = lax.axis_size("ep"), lax.axis_size("tp")
    me, mt = lax.axis_index("ep"), lax.axis_index("tp")
    length, cols = mix_ref.shape
    rows = eps * cap
    heads, _, dim = st.shape
    depth = tps * cols
    units = wg.shape[1]
    ep_peer = [flip(me, k) for k in range(eps)]
    tp_peer = [flip(mt, r) for r in range(tps)]

    def push(src, dst, recv, ep=None, tp=None):
        where = {"ep": ep_peer[ep]} if tp is None else {"tp": tp_peer[tp]}
        return pltpu.make_async_remote_copy(src_ref=src, dst_ref=dst, send_sem=out_sem.at[0], recv_sem=recv,
                                            device_id=where, device_id_type=MESH)

    sent = []

    def go(copy):
        copy.start()
        sent.append(copy)

    loads = [pltpu.make_async_copy(s, wmix.at[i], wsem.at[0]) for i, s in enumerate((wq_hbm, wf_hbm, wi_hbm, wo_hbm))]
    loads += [pltpu.make_async_copy(wg_hbm.at[0], wg, wsem.at[1]), pltpu.make_async_copy(wu_hbm.at[0], wu, wsem.at[2]),
              pltpu.make_async_copy(wd_hbm.at[0], wd, wsem.at[3]), pltpu.make_async_copy(wm_hbm, wm, wsem.at[4])]
    barrier = pltpu.get_barrier_semaphore()
    for k in range(1, eps):
        pl.semaphore_signal(barrier, inc=1, device_id={"ep": ep_peer[k]}, device_id_type=MESH)
    for r in range(1, tps):
        pl.semaphore_signal(barrier, inc=1, device_id={"tp": tp_peer[r]}, device_id_type=MESH)
    small = [(mix_hbm, mix_ref), (ids_hbm, ids_ref), (moe_hbm, moe_ref), (mgain_hbm, mgain_ref), (gap_hbm, gap_ref),
             (dec_hbm, dec_ref), (hgain_hbm, hgain_ref), (egain_hbm, egain_ref), (scores_hbm, scores_ref)]
    rowload = [pltpu.make_async_copy(src, dst, wsem.at[5 + i]) for i, (src, dst) in enumerate(small)]
    for load in rowload + loads:
        load.start()
    rowload[0].wait()
    pl.semaphore_wait(barrier, eps + tps - 2)

    half = length // 2
    go(push(mix_ref, xall.at[mt], xr.at[0], tp=1))
    go(push(mix_ref, xall.at[mt], xr.at[1], tp=2))

    experts = eps
    names = iota((length, experts), 1)
    rowload[1].wait()
    eye = iota((length, length), 0) == iota((length, length), 1)
    ids = dot(eye.astype(BF16), ids_ref[...].astype(F32).astype(BF16), ((1,), (1,))).astype(jnp.int32)
    picks = [ids[:, j:j + 1] == names for j in range(ids.shape[1])]
    chosen = functools.reduce(jnp.logical_or, picks)
    before = (iota((length, length), 0) > iota((length, length), 1)).astype(BF16)
    rank = dot(before, chosen.astype(BF16)).astype(jnp.int32)
    spot = rank + jnp.bitwise_xor(names, me) * cap
    rowload[2].wait()
    both = None
    for j, pick in enumerate(picks):
        at = jnp.sum(jnp.where(pick, spot, 0), axis=1, keepdims=True)
        hit = (iota((length, rows), 1) == at).astype(F32)
        hits[j] = hit.astype(BF16)
        both = hit if both is None else both + hit
    made = dot(both.astype(BF16), moe_ref[...], ((0,), (0,))).astype(BF16)
    slots[...] = made
    gath[mt, 0:cap, :] = made[0:cap]
    for k in range(1, eps):
        r = slice(k * cap, (k + 1) * cap)
        go(push(slots.at[r], gath.at[mt, r], zr.at[k], ep=k))

    def rowsof(k, part=None):
        if part is None:
            return pl.ds(k * cap, cap)
        return pl.ds(k * cap + part * (cap // 2), cap // 2)

    def spread(k):
        if k:
            push(slots.at[rowsof(k)], gath.at[mt, rowsof(k)], zr.at[k], ep=k).wait_recv()
        for n, r in enumerate((1, 2)):
            ref = gath.at[mt, rowsof(k)]
            go(push(ref, ref, gr.at[k, n], tp=r))

    def relay(k):
        for n, (source, target) in enumerate(((1, 2), (2, 1))):
            whole = gath.at[tp_peer[source], rowsof(k)]
            push(whole, whole, gr.at[k, n], tp=source).wait_recv()
            ref = gath.at[tp_peer[source], rowsof(k, n)]
            go(push(ref, ref, gr.at[k, 2], tp=target))

    def complete(k):
        ref = gath.at[tp_peer[3], rowsof(k)]
        push(ref, ref, gr.at[k, 2], tp=1).wait_recv()

    def relay_mix():
        for n, (source, target) in enumerate(((1, 2), (2, 1))):
            whole = xall.at[tp_peer[source]]
            push(whole, whole, xr.at[n], tp=source).wait_recv()
            ref = xall.at[tp_peer[source], pl.ds(n * half, half)]
            go(push(ref, ref, xr.at[2], tp=target))

    def complete_mix():
        ref = xall.at[tp_peer[3]]
        push(ref, ref, xr.at[2], tp=1).wait_recv()

    S, R = (lambda k: functools.partial(spread, k)), (lambda k: functools.partial(relay, k))
    agenda, ahead = [], eps // 2
    for k in range(1, ahead):
        agenda += [S(k + 2), R(k)] if k + 2 < ahead else [R(k)]
    far_start = len(agenda)
    spreads, relays = [S(k) for k in range(max(ahead, 3), eps)], [R(k) for k in range(ahead, eps)]
    agenda += spreads[:3]
    agenda += relays[:2] + spreads[3:] + relays[2:]
    far_end = len(agenda) - far_start

    def poll(count=1):
        for _ in range(min(count, len(agenda))):
            agenda.pop(0)()

    for load in rowload[3:]:
        load.wait()
    mgain, egain = mgain_ref[...].astype(F32), egain_ref[...].astype(F32)
    lanes = mgain.shape[1]
    per_shard = cols // lanes
    squares = [jnp.zeros((length, 1), F32)]

    def project(r, ref, first):
        p = tp_peer[r]
        v = ref[...].astype(F32)
        squares[0] += jnp.sum(v * v, axis=1, keepdims=True)
        gains = mgain[0:per_shard]
        for i in range(1, tps):
            gains = jnp.where(p == i, mgain[i * per_shard:(i + 1) * per_shard], gains)
        v = jnp.concatenate([v[:, i * lanes:(i + 1) * lanes] * gains[i:i + 1] for i in range(per_shard)], axis=1)
        v = v.astype(BF16)
        w = pl.ds(pl.multiple_of(p * cols, cols), cols)
        for i in range(4):
            part = dot(v, wmix[i, w, :])
            acc[i] = part if first else acc[i] + part

    S(0)()
    pltpu.make_async_copy(wmix, wmix, wsem.at[0]).wait()
    project(0, mix_ref, True)
    relay_mix()
    S(1)()
    project(1, xall.at[tp_peer[1]], False)
    R(0)()
    S(2)()
    project(2, xall.at[tp_peer[2]], False)
    complete_mix()
    poll(1)
    project(3, xall.at[tp_peer[3]], False)
    scale = lax.rsqrt(squares[0] / depth + epsilon)
    poll(1)

    tri = (iota((length, length), 0) >= iota((length, length), 1)).astype(F32)
    extra = dot(tri, dec_ref[...], ((1,), (1,)), precision=HIGHEST)
    causal = iota((BLOCK, BLOCK), 0) >= iota((BLOCK, BLOCK), 1)
    mid = BLOCK // 2
    per = 2 if heads % 2 == 0 else 1

    def mix_step(step):
        w = slice(step * per * dim, (step + 1) * per * dim)
        qp, fp, value, op = [acc[i, :, w] * scale for i in range(4)]
        value = value.astype(BF16)
        query = qp * sigmoid(qp)
        key = gap_ref[:, w] * sigmoid(-fp)
        og[:, w] = op * sigmoid(op)
        logs = jnp.log1p(-key)
        for j in range(per):
            h = step * per + j
            cl = slice(j * dim, (j + 1) * dim)
            c = slice(h * dim, (h + 1) * dim)
            run = dot(tri, logs[:, cl], precision=HIGHEST) + extra[:, h:h + 1]
            q, k, v = query[:, cl], key[:, cl], value[:, cl]
            qd[:, c] = (q * jnp.exp(run)).astype(BF16)
            state = jnp.zeros((dim, dim), F32)
            base = jnp.zeros((1, dim), F32)
            for b in range(length // BLOCK):
                r = slice(b * BLOCK, (b + 1) * BLOCK)
                g, qb, kb, vb = run[r], q[r], k[r], v[r]
                ref = g[mid - 1:mid]
                last = g[BLOCK - 1:BLOCK]
                qe = (qb * jnp.exp(g - ref)).astype(BF16)
                ke = (kb * jnp.exp(ref - g)).astype(BF16)
                scores = jnp.where(causal, dot(qe, ke, ((1,), (1,))), 0.0).astype(BF16)
                out = dot(scores, vb)
                if b:
                    qs = (qb * jnp.exp(g - base)).astype(BF16)
                    out += dot(qs, state.astype(BF16), ((1,), (1,)))
                lo[r, c] = out
                kd = (kb * jnp.exp(last - g)).astype(BF16)
                state = state * jnp.exp(last - base) + dot(vb, kd, ((0,), (0,)))
                base = last
            st[h, 0:dim, :] = state.astype(BF16)
            st[h, dim:, :] = jnp.broadcast_to(jnp.exp(base), (st.shape[1] - dim, dim)).astype(BF16)
            if h:
                poll(1)

    odd = lax.rem(me, PAIR)
    pair = lax.div(me, PAIR)
    swap = push(st, pst, sr.at[0], ep=1)
    own_half = pl.ds(odd * (heads // 2), heads // 2)
    other_half = pl.ds((1 - odd) * (heads // 2), heads // 2)
    trade = push(fst.at[own_half], fst.at[own_half], sr.at[1 + eps // PAIR], ep=1)

    def joined_copy(k):
        return push(cst, states.at[pair], sr.at[1 + pair], ep=k)

    def parts_of(ref, h):
        return ref[h, 0:dim, :].astype(F32), ref[h, dim:dim + 16, :].astype(F32)[0:1]

    def join_states():
        swap.wait_recv()
        for i in range(heads // 2):
            h = odd * (heads // 2) + i
            (own, keep), (other, pass_on) = parts_of(st, h), parts_of(pst, h)
            cst[i, 0:dim, :] = jnp.where(odd == 1, other * keep + own, own * pass_on + other).astype(BF16)
            cst[i, dim:, :] = jnp.broadcast_to(keep * pass_on, (st.shape[1] - dim, dim)).astype(BF16)
        for k in range(PAIR, eps, PAIR):
            @pl.when(ep_peer[k] > me)
            def _():
                joined_copy(k).start()

    def fold_states():
        @pl.loop(0, pair)
        def _(hop):
            pltpu.make_async_remote_copy(src_ref=cst, dst_ref=states.at[hop], send_sem=out_sem.at[0], recv_sem=sr.at[1 + hop],
                                         device_id={"ep": hop * PAIR + odd}, device_id_type=MESH).wait_recv()

        for i in range(heads // 2):
            def one(hop, state):
                own, pass_on = parts_of(states.at[hop], i)
                return state * pass_on + own

            state = lax.fori_loop(0, pair, one, jnp.zeros((dim, dim), F32))
            fst[odd * (heads // 2) + i] = state.astype(BF16)
        go(trade)

    def finish_mixer():
        push(fst.at[other_half], fst.at[other_half], sr.at[1 + eps // PAIR], ep=1).wait_recv()
        for h in range(heads):
            c = slice(h * dim, (h + 1) * dim)
            state = fst[h].astype(F32)
            other, pass_on = parts_of(pst, h)
            state = jnp.where(odd == 1, state * pass_on + other, state)
            out = lo[:, c] + dot(qd[:, c], state.astype(BF16), ((1,), (1,)))
            scale = lax.rsqrt(jnp.mean(out * out, axis=1, keepdims=True) + epsilon)
            gated[:, c] = (out * scale * hgain_ref[...].astype(F32) * og[:, c]).astype(BF16)
        loads[7].wait()
        for r in (3, 1, 2, 0):
            block = wm[:, pl.ds(pl.multiple_of(tp_peer[r] * cols, cols), cols)]
            mixed[r] = dot(gated[...], block).astype(BF16)

    tile = 256 if units % 256 == 0 else units
    def feed(chunks):
        for k in chunks:
            complete(k)
            r = chunk(k)
            squares = jnp.zeros((cap, 1), F32)
            for p in range(tps):
                v = gath[p, r, :].astype(F32)
                squares += jnp.sum(v * v, axis=1, keepdims=True)
            scale = lax.rsqrt(squares / depth + epsilon)
            for p in range(tps):
                for i in range(cols // lanes):
                    s = slice(i * lanes, (i + 1) * lanes)
                    n = p * (cols // lanes) + i
                    c = slice(n * lanes, (n + 1) * lanes)
                    enormed[r, c] = (gath[p, r, s].astype(F32) * scale * egain[n:n + 1]).astype(BF16)

    def chunk(k):
        return slice(k * cap, (k + 1) * cap)

    def span(chunks):
        return slice(chunks[0] * cap, (chunks[-1] + 1) * cap)

    def upward(chunks, polls=()):
        r = span(chunks)
        for u in range(units // tile):
            c = slice(u * tile, (u + 1) * tile)
            gate = dot(enormed[r, :], wg[:, c])
            up = dot(enormed[r, :], wu[:, c])
            hidden[0:len(chunks) * cap, c] = (gate * sigmoid(gate) * up).astype(BF16)
            if u in polls:
                poll(1)

    def downward(chunks, polls=()):
        r = span(chunks)
        for t in (3, 1, 2, 0):
            block = wd[:, pl.ds(pl.multiple_of(tp_peer[t] * cols, cols), cols)]
            psend[t, r, :] = dot(hidden[0:len(chunks) * cap, :], block).astype(BF16)
            if t in polls:
                poll(1)

    def summing(src, dst, a, b, recv):
        def part(n, index, target, r, tp):
            return push(src.at[index, r], dst.at[target, r], recv.at[n], tp=tp)

        first = [part(0, 3, 3, a, 1), part(1, 3, 3, b, 2), part(2, 1, 1, a, 1), part(2, 2, 2, b, 2)]
        second = [part(2, 2, 2, a, 2), part(2, 1, 1, b, 1)]
        landed = dst.at[pl.ds(1, 2), slice(a.start, b.stop)]

        def start():
            for copy in first:
                go(copy)

        def merge():
            first[0].wait_recv()
            src[2, a, :] = (src[2, a, :].astype(F32) + dst[3, a, :].astype(F32)).astype(BF16)
            first[1].wait_recv()
            src[1, b, :] = (src[1, b, :].astype(F32) + dst[3, b, :].astype(F32)).astype(BF16)
            for copy in second:
                go(copy)

        def finish():
            push(landed, landed, recv.at[2], tp=1).wait_recv()

        def value(r):
            return src[0, r, :].astype(F32) + dst[1, r, :].astype(F32) + dst[2, r, :].astype(F32)

        return start, merge, finish, value

    near = list(range(eps // 2))
    far = [[k, k + 1] for k in range(eps // 2, eps, 2)]
    nrows = len(near) * cap
    sums = [summing(psend, precv, chunk(a), chunk(b), pr.at[g]) for g, (a, b) in enumerate(far)]
    mixsum = summing(mixed, mixin, slice(0, half), slice(half, length), mr)
    toksum = summing(tok, tokin, slice(0, half), slice(half, length), tr)

    def near_copy(k):
        return push(psend.at[:, chunk(k)], nback.at[:, chunk(k)], br.at[0], ep=k)

    def give_near():
        for k in near[1:]:
            go(near_copy(k))
        nback[:, chunk(0), :] = psend[:, chunk(0), :]

    def take_near():
        landed = nback.at[:, span(near[1:])]
        push(landed, landed, br.at[0], ep=1).wait_recv()
        for t in (3, 1, 2, 0):
            value = jnp.zeros((length, cols), F32)
            for j in range(hits.shape[0]):
                value += dot(hits[j, :, 0:nrows], nback[t]) * weights[:, j:j + 1]
            tok[t] = value.astype(BF16)

    def give_far(g):
        _, _, finish, value = sums[g]
        finish()
        for k in far[g]:
            r = chunk(k)
            esum[r, :] = value(r).astype(BF16)
            go(push(esum.at[r], back.at[r], br.at[1 + g], ep=k))

    def take_far(g):
        r = span(far[g])
        push(back.at[r], back.at[r], br.at[1 + g], ep=1).wait_recv()
        value = jnp.zeros((length, cols), F32)
        for j in range(hits.shape[0]):
            value += dot(hits[j, :, r], back[r, :]) * weights[:, j:j + 1]
        return value

    scores = scores_ref[...]
    weights = dot(eye.astype(F32), scores / jnp.sum(scores, axis=0, keepdims=True), ((1,), (1,)), precision=HIGHEST)

    for step in range(heads // per):
        mix_step(step)
    go(swap)
    for load in loads[4:7]:
        load.wait()
    poll(len(agenda) - far_end)
    poll(2)
    join_states()
    feed(near)
    upward(near, polls=(1,))
    downward(near, polls=(1, 2))
    give_near()
    poll(len(agenda) - 1)
    for g, chunks in enumerate(far):
        feed(chunks)
        upward(chunks, polls=(1,))
        downward(chunks)
        if g == 0:
            poll(len(agenda))
        sums[g][0]()
        if g:
            sums[g - 1][1]()
    fold_states()
    sums[-1][1]()
    finish_mixer()
    mixsum[0]()
    for g in range(len(far) - 1):
        give_far(g)
    take_near()
    toksum[0]()
    mixsum[1]()
    give_far(len(far) - 1)
    toksum[1]()
    value = take_far(0)
    for g in range(1, len(far)):
        value += take_far(g)
    total[...] = value
    mixsum[2]()
    mix_out[...] = mixsum[3](slice(0, length)).astype(BF16)
    toksum[2]()
    moe_out[...] = (total[...] + toksum[3](slice(0, length))).astype(BF16)

    for copy in sent:
        copy.wait_send()
    for k in range(PAIR, eps, PAIR):
        @pl.when(ep_peer[k] > me)
        def _():
            joined_copy(k).wait_send()


def place_kernel(a_ref, b_ref, a_out, b_out, sem):
    copies = [pltpu.make_async_copy(a_ref, a_out, sem.at[0]), pltpu.make_async_copy(b_ref, b_out, sem.at[1])]
    for copy in copies:
        copy.start()
    for copy in copies:
        copy.wait()


def whole_block(mix_rows, mix_gain, wq, wf, wi, wo, gap, dec, hgain, wm, moe_rows, moe_gain, ids, scores, wg, wu, wd):
    eps, tps = lax.axis_size("ep"), lax.axis_size("tp")
    length, cols = mix_rows.shape
    top = ids.shape[1]
    cap = length * top * 3 // (2 * eps)
    rows = eps * cap
    heads = dec.shape[0]
    width = wq.shape[1]
    dim = width // heads
    depth, units = wg.shape[1:]
    dma = lambda *s: pltpu.SemaphoreType.DMA(s)
    out = jax.ShapeDtypeStruct((length, cols), BF16)
    scratch = [
        pltpu.VMEM((depth // 128, 128), BF16), pltpu.VMEM((1, width), F32), pltpu.VMEM(dec.shape, F32),
        pltpu.VMEM((1, dim), BF16), pltpu.VMEM((depth // 128, 128), BF16),
        pltpu.VMEM((top, length), jnp.int32), pltpu.VMEM((top, length), F32),
        pltpu.VMEM((length, cols), BF16), pltpu.VMEM((length, cols), BF16),
        pltpu.VMEM((4, depth, width), BF16), pltpu.VMEM((width, depth), BF16),
        pltpu.VMEM((depth, units), BF16), pltpu.VMEM((depth, units), BF16), pltpu.VMEM((units, depth), BF16),
        pltpu.VMEM((tps, length, cols), BF16), pltpu.VMEM((4, length, width), F32),
        pltpu.VMEM((length, width), F32), pltpu.VMEM((length, width), BF16), pltpu.VMEM((length, width), F32),
        pltpu.VMEM((heads, dim + 16, dim), BF16), pltpu.VMEM((heads, dim + 16, dim), BF16),
        pltpu.VMEM((heads // 2, dim + 16, dim), BF16), pltpu.VMEM((heads, dim, dim), BF16),
        pltpu.VMEM((eps // PAIR, heads // 2, dim + 16, dim), BF16),
        pltpu.VMEM((length, width), BF16), pltpu.VMEM((tps, length, cols), BF16), pltpu.VMEM((tps, length, cols), BF16),
        pltpu.VMEM((tps, rows, cols), BF16), pltpu.VMEM((rows, cols), BF16), pltpu.VMEM((top, length, rows), BF16),
        pltpu.VMEM((rows, depth), BF16), pltpu.VMEM((rows // 2, units), BF16),
        pltpu.VMEM((tps, rows, cols), BF16), pltpu.VMEM((tps, rows, cols), BF16),
        pltpu.VMEM((tps, rows // 2, cols), BF16), pltpu.VMEM((tps, length, cols), BF16), pltpu.VMEM((tps, length, cols), BF16),
        pltpu.VMEM((rows, cols), BF16), pltpu.VMEM((rows, cols), BF16), pltpu.VMEM((length, cols), F32),
        dma(14), dma(1), dma(3), dma(eps), dma(eps, 3), dma(eps // 4, 3), dma(1 + eps // 4),
        dma(2 + eps // PAIR), dma(3), dma(3),
    ]
    results = pl.pallas_call(
        functools.partial(block_kernel, cap),
        in_specs=[pl.BlockSpec(memory_space=pltpu.HBM)] * 17,
        out_specs=[VMEM, VMEM],
        out_shape=[pltpu.VMEM((length, cols), BF16)] * 2,
        scratch_shapes=scratch,
        compiler_params=pltpu.CompilerParams(vmem_limit_bytes=LIMIT, collective_id=0, has_side_effects=True),
    )(mix_rows, mix_gain.reshape(-1, 128), wq, wf, wi, wo, gap.reshape(1, -1), dec, hgain.reshape(1, -1), wm,
      moe_rows, moe_gain.reshape(-1, 128), ids.T, scores.T, wg, wu, wd)
    return pl.pallas_call(
        place_kernel,
        in_specs=[VMEM, VMEM],
        out_specs=[ANY, ANY],
        out_shape=[out, out],
        scratch_shapes=[dma(2)],
        compiler_params=pltpu.CompilerParams(vmem_limit_bytes=1024 * 1024),
    )(*results)


def fits(eps, tps, mix_rows, dec, route_ids, w_gate):
    tokens, cols = mix_rows.shape
    top = route_ids.shape[1]
    cap = tokens * top * 3 // (2 * eps)
    square = tps == 4 and dec.shape[0] % 2 == 0 and eps >= 4 and eps & (eps - 1) == 0
    aligned = cap % 32 == 0 and cols % 128 == 0 and tokens % (2 * BLOCK) == 0 and w_gate.shape[2] % 128 == 0
    return square and aligned and w_gate.shape[0] == 1


def per_device(mix_rows, mix_gain, w_query, w_forget, w_input, w_outgate, forget_gap, decay_extra,
               head_gain, w_mixout, moe_rows, moe_gain, route_ids, route_scores, w_gate, w_up, w_down):
    eps, tps = lax.axis_size("ep"), lax.axis_size("tp")
    if fits(eps, tps, mix_rows, decay_extra, route_ids, w_gate):
        return whole_block(mix_rows, mix_gain, w_query, w_forget, w_input, w_outgate, forget_gap, decay_extra,
                           head_gain, w_mixout, moe_rows, moe_gain, route_ids, route_scores, w_gate, w_up, w_down)
    tokens, top = route_ids.shape
    experts = w_gate.shape[0] * eps
    capacity = tokens * top * 3 // (2 * experts)
    cols = mix_rows.shape[1]
    ids = route_ids.T
    slots = dispatch(ids, moe_rows, experts, capacity)
    arrived = lax.all_to_all(slots.reshape(eps, -1, cols), "ep", split_axis=0, concat_axis=0, tiled=True)
    gathered = lax.all_gather(arrived.reshape(-1, cols), "tp", axis=0)
    mix_whole = lax.all_gather(mix_rows, "tp", axis=0)
    lo, qd, og, st = mixer(mix_whole, mix_gain, w_query, w_forget, w_input, w_outgate, forget_gap, decay_extra.T)
    product = experts_call(gathered, moe_gain, w_gate, w_up, w_down)
    expert_sum = lax.psum_scatter(product, "tp", scatter_dimension=0)
    states = lax.all_gather(st, "ep", axis=0)
    mixed = tail(states, lo, qd, og, head_gain, w_mixout, tps)
    mix_out = lax.psum_scatter(mixed, "tp", scatter_dimension=0)
    back = lax.all_to_all(expert_sum.reshape(eps, -1, cols), "ep", split_axis=0, concat_axis=0, tiled=True)
    moe_out = combine(ids, route_scores, back.reshape(-1, cols), experts, capacity)
    return (mix_out, moe_out)


def solution(mesh):
    placed = (
        P("ep", "tp"), P(), P(None, "tp"), P(None, "tp"), P(None, "tp"), P(None, "tp"), P("tp"),
        P("tp", "ep"), P(), P("tp", None), P("ep", "tp"), P(), P("ep", None), P("ep", None),
        P("ep", None, "tp"), P("ep", None, "tp"), P("ep", "tp", None),
    )
    return jax.shard_map(
        per_device, mesh=mesh, in_specs=placed,
        out_specs=(P("ep", "tp"), P("ep", "tp")), check_vma=False,
    )
```

```python
import functools

import jax
import jax.numpy as jnp
from jax import lax
from jax.experimental import pallas as pl
from jax.experimental.pallas import tpu as pltpu
from jax.sharding import PartitionSpec as P

BLOCK = 64
epsilon = 1e-06
F32 = jnp.float32
BF16 = jnp.bfloat16
VMEM = pl.BlockSpec(memory_space=pltpu.VMEM)
LIMIT = 60 * 1024 * 1024


def dot(a, b, dims=((1,), (0,)), precision=None):
    return lax.dot_general(a, b, (dims, ((), ())), precision=precision, preferred_element_type=F32)


def sigmoid(x):
    return 1.0 / (1.0 + jnp.exp(-x))


def iota(shape, dim):
    return lax.broadcasted_iota(jnp.int32, shape, dim)


def mixer_kernel(per, x_ref, gain_ref, wq_ref, wf_ref, wi_ref, wo_ref, gap_ref, dec_ref,
                 lo_ref, qd_ref, og_ref, st_ref, normed):
    step = pl.program_id(0)
    length = normed.shape[0]
    dim = st_ref.shape[2]
    parts, _, cols = x_ref.shape

    @pl.when(step == 0)
    def _():
        total = jnp.zeros((length, 1), F32)
        for p in range(parts):
            v = x_ref[p].astype(F32)
            total += jnp.sum(v * v, axis=1, keepdims=True)
        scale = lax.rsqrt(total / (parts * cols) + epsilon)
        for p in range(parts):
            g = gain_ref[:, p * cols:(p + 1) * cols].astype(F32)
            normed[:, p * cols:(p + 1) * cols] = (x_ref[p].astype(F32) * scale * g).astype(BF16)

    n = normed[...]
    qp = dot(n, wq_ref[...])
    fp = dot(n, wf_ref[...])
    value = dot(n, wi_ref[...]).astype(BF16)
    op = dot(n, wo_ref[...])
    query = qp * sigmoid(qp)
    key = gap_ref[...] * sigmoid(-fp)
    og_ref[...] = op * sigmoid(op)
    logs = jnp.log1p(-key)
    dec = dec_ref[...]
    tri = (iota((length, length), 0) >= iota((length, length), 1)).astype(F32)
    causal = iota((BLOCK, BLOCK), 0) >= iota((BLOCK, BLOCK), 1)
    half = BLOCK // 2
    for j in range(per):
        c = slice(j * dim, (j + 1) * dim)
        extra = jnp.sum(jnp.where(iota(dec.shape, 1) == step * per + j, dec, 0.0), axis=1, keepdims=True)
        run = dot(tri, logs[:, c] + extra, precision=lax.Precision.HIGHEST)
        q, k, v = query[:, c], key[:, c], value[:, c]
        qd_ref[:, c] = (q * jnp.exp(run)).astype(BF16)
        state = jnp.zeros((dim, dim), F32)
        base = jnp.zeros((1, dim), F32)
        for b in range(length // BLOCK):
            r = slice(b * BLOCK, (b + 1) * BLOCK)
            g, qb, kb, vb = run[r], q[r], k[r], v[r]
            ref = g[half - 1:half]
            last = g[BLOCK - 1:BLOCK]
            qe = (qb * jnp.exp(g - ref)).astype(BF16)
            ke = (kb * jnp.exp(ref - g)).astype(BF16)
            scores = jnp.where(causal, dot(qe, ke, ((1,), (1,))), 0.0).astype(BF16)
            out = dot(scores, vb)
            if b:
                qs = (qb * jnp.exp(g - base)).astype(BF16)
                out += dot(qs, state.astype(BF16), ((1,), (1,)))
            lo_ref[r, c] = out
            kd = (kb * jnp.exp(last - g)).astype(BF16)
            state = state * jnp.exp(last - base) + dot(vb, kd, ((0,), (0,)))
            base = last
        st_ref[j, 0:dim, :] = state.astype(BF16)
        st_ref[j, dim:, :] = jnp.broadcast_to(jnp.exp(base), (st_ref.shape[1] - dim, dim)).astype(BF16)


def mixer(x, gain, wq, wf, wi, wo, gap, dec):
    parts, length, cols = x.shape
    heads, dim = dec.shape[1], wq.shape[1] // dec.shape[1]
    per = 2 if heads % 2 == 0 else 1
    width = per * dim
    depth = wq.shape[0]
    column = pl.BlockSpec((depth, width), lambda i: (0, i))
    rows = pl.BlockSpec((length, width), lambda i: (0, i))
    whole = lambda s: pl.BlockSpec(s, lambda i: (0,) * len(s))
    return pl.pallas_call(
        functools.partial(mixer_kernel, per),
        grid=(heads // per,),
        in_specs=[whole(x.shape), whole((1, depth)), column, column, column, column,
                  pl.BlockSpec((1, width), lambda i: (0, i)), whole(dec.shape)],
        out_specs=[rows, rows, rows, pl.BlockSpec((per, dim + 16, dim), lambda i: (i, 0, 0))],
        out_shape=[jax.ShapeDtypeStruct((length, heads * dim), F32),
                   jax.ShapeDtypeStruct((length, heads * dim), BF16),
                   jax.ShapeDtypeStruct((length, heads * dim), F32),
                   jax.ShapeDtypeStruct((heads, dim + 16, dim), BF16)],
        scratch_shapes=[pltpu.VMEM((length, depth), BF16)],
        compiler_params=pltpu.CompilerParams(vmem_limit_bytes=LIMIT),
        cost_estimate=pl.CostEstimate(flops=10 * 10**9, bytes_accessed=9 * 10**6, transcendentals=10**6),
    )(x, gain.reshape(1, -1), wq, wf, wi, wo, gap.reshape(1, -1), dec)


def tail_kernel(states_ref, lo_ref, qd_ref, og_ref, hg_ref, w_ref, out_ref, gated):
    place = lax.axis_index("ep")
    hops, heads, _, dim = states_ref.shape
    for h in range(heads):
        c = slice(h * dim, (h + 1) * dim)

        def one(hop, state):
            own = states_ref[hop, h, 0:dim, :].astype(F32)
            passing = states_ref[hop, h, dim:dim + 16, :].astype(F32)[0:1]
            return jnp.where(hop < place, state * passing + own, state)

        state = lax.fori_loop(0, hops, one, jnp.zeros((dim, dim), F32))
        out = lo_ref[:, c] + dot(qd_ref[:, c], state.astype(BF16), ((1,), (1,)))
        scale = lax.rsqrt(jnp.mean(out * out, axis=1, keepdims=True) + epsilon)
        gated[:, c] = (out * scale * hg_ref[...].astype(F32) * og_ref[:, c]).astype(BF16)
    parts, _, cols = out_ref.shape
    for p in range(parts):
        out_ref[p] = dot(gated[...], w_ref[:, p * cols:(p + 1) * cols]).astype(BF16)


def tail(states, lo, qd, og, hg, w, parts):
    length, width = lo.shape
    return pl.pallas_call(
        tail_kernel,
        in_specs=[VMEM] * 6,
        out_specs=VMEM,
        out_shape=jax.ShapeDtypeStruct((parts, length, w.shape[1] // parts), BF16),
        scratch_shapes=[pltpu.VMEM((length, width), BF16)],
        compiler_params=pltpu.CompilerParams(vmem_limit_bytes=LIMIT),
        cost_estimate=pl.CostEstimate(flops=10**9, bytes_accessed=5 * 10**6, transcendentals=10**5),
    )(states, lo, qd, og, hg.reshape(1, -1), w)


def ranks(ids, experts):
    tokens = ids.shape[1]
    names = iota((experts, tokens), 0)
    picks = [names == ids[k:k + 1, :] for k in range(ids.shape[0])]
    chosen = functools.reduce(jnp.logical_or, picks)
    before = (iota((tokens, tokens), 0) < iota((tokens, tokens), 1)).astype(BF16)
    return picks, chosen, dot(chosen.astype(BF16), before)


def slot_hits(mask, rank, experts, capacity):
    rows = experts * capacity
    owner = iota((rows, experts), 0) - iota((rows, experts), 1) * capacity
    owner = jnp.logical_and(owner >= 0, owner < capacity).astype(F32)
    tokens = rank.shape[1]
    spread = dot(owner, jnp.where(mask, rank, -1.0))
    spot = dot(owner, iota((experts, tokens), 0).astype(F32)) * capacity
    return (spread >= 0.0) & (spread + spot == iota((rows, tokens), 0).astype(F32))


def dispatch_kernel(experts, capacity, ids_ref, rows_ref, out_ref):
    _, chosen, rank = ranks(ids_ref[...], experts)
    hits = slot_hits(chosen, rank, experts, capacity).astype(BF16)
    out_ref[...] = dot(hits, rows_ref[...]).astype(BF16)


def dispatch(ids, rows, experts, capacity):
    return pl.pallas_call(
        functools.partial(dispatch_kernel, experts, capacity),
        in_specs=[VMEM] * 2,
        out_specs=VMEM,
        out_shape=jax.ShapeDtypeStruct((experts * capacity, rows.shape[1]), BF16),
    )(ids, rows)


def combine_kernel(experts, capacity, ids_ref, scores_ref, back_ref, out_ref):
    picks, _, rank = ranks(ids_ref[...], experts)
    scores = scores_ref[...]
    weights = scores / jnp.sum(scores, axis=1, keepdims=True)
    total = jnp.zeros(out_ref.shape, F32)
    for k, mask in enumerate(picks):
        hits = slot_hits(mask, rank, experts, capacity).astype(BF16)
        total += dot(hits, back_ref[...], ((0,), (0,))) * weights[:, k:k + 1]
    out_ref[...] = total.astype(BF16)


def combine(ids, scores, back, experts, capacity):
    return pl.pallas_call(
        functools.partial(combine_kernel, experts, capacity),
        in_specs=[VMEM] * 3,
        out_specs=VMEM,
        out_shape=jax.ShapeDtypeStruct((ids.shape[1], back.shape[1]), BF16),
    )(ids, scores, back)


def expert_kernel(x_ref, gain_ref, wg_ref, wu_ref, wd_ref, out_ref, normed, total):
    step = pl.program_id(0)
    parts, rows, cols = x_ref.shape

    @pl.when(step == 0)
    def _():
        squares = jnp.zeros((rows, 1), F32)
        for p in range(parts):
            v = x_ref[p].astype(F32)
            squares += jnp.sum(v * v, axis=1, keepdims=True)
        scale = lax.rsqrt(squares / (parts * cols) + epsilon)
        for p in range(parts):
            g = gain_ref[:, p * cols:(p + 1) * cols].astype(F32)
            normed[:, p * cols:(p + 1) * cols] = (x_ref[p].astype(F32) * scale * g).astype(BF16)

    gate = dot(normed[...], wg_ref[0])
    up = dot(normed[...], wu_ref[0])
    hidden = (gate * sigmoid(gate) * up).astype(BF16)
    last = pl.num_programs(0) - 1
    for p in range(parts):
        c = slice(p * cols, (p + 1) * cols)
        part = dot(hidden, wd_ref[0, :, c])

        @pl.when(jnp.logical_and(step == 0, last > 0))
        def _():
            total[:, c] = part

        @pl.when(jnp.logical_and(step > 0, step < last))
        def _():
            total[:, c] += part

        @pl.when(step == last)
        def _():
            out_ref[p] = (jnp.where(step > 0, total[:, c], 0.0) + part).astype(BF16)


def experts_call(x, gain, wg, wu, wd):
    parts, rows, cols = x.shape
    depth, units = wg.shape[1:]
    tile = 256 if units % 256 == 0 else units
    return pl.pallas_call(
        expert_kernel,
        grid=(units // tile,),
        in_specs=[pl.BlockSpec(x.shape, lambda i: (0, 0, 0)), pl.BlockSpec((1, depth), lambda i: (0, 0)),
                  pl.BlockSpec((1, depth, tile), lambda i: (0, 0, i)),
                  pl.BlockSpec((1, depth, tile), lambda i: (0, 0, i)),
                  pl.BlockSpec((1, tile, depth), lambda i: (0, i, 0))],
        out_specs=pl.BlockSpec(x.shape, lambda i: (0, 0, 0)),
        out_shape=jax.ShapeDtypeStruct(x.shape, BF16),
        scratch_shapes=[pltpu.VMEM((rows, depth), BF16), pltpu.VMEM((rows, depth), F32)],
        compiler_params=pltpu.CompilerParams(vmem_limit_bytes=LIMIT),
        cost_estimate=pl.CostEstimate(flops=8 * 10**9, bytes_accessed=10**7, transcendentals=10**6),
    )(x, gain.reshape(1, -1), wg, wu, wd)

MESH = pl.DeviceIdType.MESH
ANY = pl.BlockSpec(memory_space=pl.ANY)
HIGHEST = lax.Precision.HIGHEST
PAIR = 2


def flip(place, bits):
    bit = 1
    while bit <= bits:
        if bits & bit:
            place = place + bit - 2 * bit * lax.rem(lax.div(place, bit), 2)
        bit *= 2
    return place


def block_kernel(cap, mix_hbm, mgain_hbm, wq_hbm, wf_hbm, wi_hbm, wo_hbm, gap_hbm, dec_hbm, hgain_hbm, wm_hbm,
                 moe_hbm, egain_hbm, ids_hbm, scores_hbm, wg_hbm, wu_hbm, wd_hbm,
                 mix_out, moe_out, mgain_ref, gap_ref, dec_ref, hgain_ref, egain_ref, ids_ref, scores_ref,
                 mix_ref, moe_ref, wmix, wm, wg, wu, wd, xall, acc, lo, qd, og, st, pst, cst, fst, states, gated, mixed, mixin,
                 gath, slots, hits, enormed, hidden, psend, precv, nback, tok, tokin, esum, back, total,
                 wsem, out_sem, xr, zr, gr, pr, br, sr, mr, tr):
    eps, tps = lax.axis_size("ep"), lax.axis_size("tp")
    me, mt = lax.axis_index("ep"), lax.axis_index("tp")
    length, cols = mix_ref.shape
    rows = eps * cap
    heads, _, dim = st.shape
    depth = tps * cols
    units = wg.shape[1]
    ep_peer = [flip(me, k) for k in range(eps)]
    tp_peer = [flip(mt, r) for r in range(tps)]

    def push(src, dst, recv, ep=None, tp=None):
        where = {"ep": ep_peer[ep]} if tp is None else {"tp": tp_peer[tp]}
        return pltpu.make_async_remote_copy(src_ref=src, dst_ref=dst, send_sem=out_sem.at[0], recv_sem=recv,
                                            device_id=where, device_id_type=MESH)

    sent = []

    def go(copy):
        copy.start()
        sent.append(copy)

    loads = [pltpu.make_async_copy(s, wmix.at[i], wsem.at[0]) for i, s in enumerate((wq_hbm, wf_hbm, wi_hbm, wo_hbm))]
    loads += [pltpu.make_async_copy(wg_hbm.at[0], wg, wsem.at[1]), pltpu.make_async_copy(wu_hbm.at[0], wu, wsem.at[2]),
              pltpu.make_async_copy(wd_hbm.at[0], wd, wsem.at[3]), pltpu.make_async_copy(wm_hbm, wm, wsem.at[4])]
    barrier = pltpu.get_barrier_semaphore()
    for k in range(1, eps):
        pl.semaphore_signal(barrier, inc=1, device_id={"ep": ep_peer[k]}, device_id_type=MESH)
    for r in range(1, tps):
        pl.semaphore_signal(barrier, inc=1, device_id={"tp": tp_peer[r]}, device_id_type=MESH)
    small = [(mix_hbm, mix_ref), (ids_hbm, ids_ref), (moe_hbm, moe_ref), (mgain_hbm, mgain_ref), (gap_hbm, gap_ref),
             (dec_hbm, dec_ref), (hgain_hbm, hgain_ref), (egain_hbm, egain_ref), (scores_hbm, scores_ref)]
    rowload = [pltpu.make_async_copy(src, dst, wsem.at[5 + i]) for i, (src, dst) in enumerate(small)]
    for load in rowload + loads:
        load.start()
    rowload[0].wait()
    pl.semaphore_wait(barrier, eps + tps - 2)

    half = length // 2
    go(push(mix_ref, xall.at[mt], xr.at[0], tp=1))
    go(push(mix_ref, xall.at[mt], xr.at[1], tp=2))

    experts = eps
    names = iota((length, experts), 1)
    rowload[1].wait()
    eye = iota((length, length), 0) == iota((length, length), 1)
    ids = dot(eye.astype(BF16), ids_ref[...].astype(F32).astype(BF16), ((1,), (1,))).astype(jnp.int32)
    picks = [ids[:, j:j + 1] == names for j in range(ids.shape[1])]
    chosen = functools.reduce(jnp.logical_or, picks)
    before = (iota((length, length), 0) > iota((length, length), 1)).astype(BF16)
    rank = dot(before, chosen.astype(BF16)).astype(jnp.int32)
    spot = rank + jnp.bitwise_xor(names, me) * cap
    rowload[2].wait()
    both = None
    for j, pick in enumerate(picks):
        at = jnp.sum(jnp.where(pick, spot, 0), axis=1, keepdims=True)
        hit = (iota((length, rows), 1) == at).astype(F32)
        hits[j] = hit.astype(BF16)
        both = hit if both is None else both + hit
    made = dot(both.astype(BF16), moe_ref[...], ((0,), (0,))).astype(BF16)
    slots[...] = made
    gath[mt, 0:cap, :] = made[0:cap]
    for k in range(1, eps):
        r = slice(k * cap, (k + 1) * cap)
        go(push(slots.at[r], gath.at[mt, r], zr.at[k], ep=k))

    def rowsof(k, part=None):
        if part is None:
            return pl.ds(k * cap, cap)
        return pl.ds(k * cap + part * (cap // 2), cap // 2)

    def spread(k):
        if k:
            push(slots.at[rowsof(k)], gath.at[mt, rowsof(k)], zr.at[k], ep=k).wait_recv()
        for n, r in enumerate((1, 2)):
            ref = gath.at[mt, rowsof(k)]
            go(push(ref, ref, gr.at[k, n], tp=r))

    def relay(k):
        for n, (source, target) in enumerate(((1, 2), (2, 1))):
            whole = gath.at[tp_peer[source], rowsof(k)]
            push(whole, whole, gr.at[k, n], tp=source).wait_recv()
            ref = gath.at[tp_peer[source], rowsof(k, n)]
            go(push(ref, ref, gr.at[k, 2], tp=target))

    def complete(k):
        ref = gath.at[tp_peer[3], rowsof(k)]
        push(ref, ref, gr.at[k, 2], tp=1).wait_recv()

    def relay_mix():
        for n, (source, target) in enumerate(((1, 2), (2, 1))):
            whole = xall.at[tp_peer[source]]
            push(whole, whole, xr.at[n], tp=source).wait_recv()
            ref = xall.at[tp_peer[source], pl.ds(n * half, half)]
            go(push(ref, ref, xr.at[2], tp=target))

    def complete_mix():
        ref = xall.at[tp_peer[3]]
        push(ref, ref, xr.at[2], tp=1).wait_recv()

    S, R = (lambda k: functools.partial(spread, k)), (lambda k: functools.partial(relay, k))
    agenda, ahead = [], eps // 2
    for k in range(1, ahead):
        agenda += [S(k + 2), R(k)] if k + 2 < ahead else [R(k)]
    far_start = len(agenda)
    spreads, relays = [S(k) for k in range(max(ahead, 3), eps)], [R(k) for k in range(ahead, eps)]
    agenda += spreads[:3]
    agenda += relays[:2] + spreads[3:] + relays[2:]
    far_end = len(agenda) - far_start

    def poll(count=1):
        for _ in range(min(count, len(agenda))):
            agenda.pop(0)()

    for load in rowload[3:]:
        load.wait()
    mgain, egain = mgain_ref[...].astype(F32), egain_ref[...].astype(F32)
    lanes = mgain.shape[1]
    per_shard = cols // lanes
    squares = [jnp.zeros((length, 1), F32)]

    def project(r, ref, first):
        p = tp_peer[r]
        v = ref[...].astype(F32)
        squares[0] += jnp.sum(v * v, axis=1, keepdims=True)
        gains = mgain[0:per_shard]
        for i in range(1, tps):
            gains = jnp.where(p == i, mgain[i * per_shard:(i + 1) * per_shard], gains)
        v = jnp.concatenate([v[:, i * lanes:(i + 1) * lanes] * gains[i:i + 1] for i in range(per_shard)], axis=1)
        v = v.astype(BF16)
        w = pl.ds(pl.multiple_of(p * cols, cols), cols)
        for i in range(4):
            part = dot(v, wmix[i, w, :])
            acc[i] = part if first else acc[i] + part

    S(0)()
    pltpu.make_async_copy(wmix, wmix, wsem.at[0]).wait()
    project(0, mix_ref, True)
    S(1)()
    relay_mix()
    project(1, xall.at[tp_peer[1]], False)
    R(0)()
    S(2)()
    project(2, xall.at[tp_peer[2]], False)
    complete_mix()
    poll(1)
    project(3, xall.at[tp_peer[3]], False)
    scale = lax.rsqrt(squares[0] / depth + epsilon)
    poll(1)

    tri = (iota((length, length), 0) >= iota((length, length), 1)).astype(F32)
    extra = dot(tri, dec_ref[...], ((1,), (1,)), precision=HIGHEST)
    causal = iota((BLOCK, BLOCK), 0) >= iota((BLOCK, BLOCK), 1)
    mid = BLOCK // 2
    per = 2 if heads % 2 == 0 else 1

    def mix_step(step):
        w = slice(step * per * dim, (step + 1) * per * dim)
        qp, fp, value, op = [acc[i, :, w] * scale for i in range(4)]
        value = value.astype(BF16)
        query = qp * sigmoid(qp)
        key = gap_ref[:, w] * sigmoid(-fp)
        og[:, w] = op * sigmoid(op)
        logs = jnp.log1p(-key)
        for j in range(per):
            h = step * per + j
            cl = slice(j * dim, (j + 1) * dim)
            c = slice(h * dim, (h + 1) * dim)
            run = dot(tri, logs[:, cl], precision=HIGHEST) + extra[:, h:h + 1]
            q, k, v = query[:, cl], key[:, cl], value[:, cl]
            qd[:, c] = (q * jnp.exp(run)).astype(BF16)
            state = jnp.zeros((dim, dim), F32)
            base = jnp.zeros((1, dim), F32)
            for b in range(length // BLOCK):
                r = slice(b * BLOCK, (b + 1) * BLOCK)
                g, qb, kb, vb = run[r], q[r], k[r], v[r]
                ref = g[mid - 1:mid]
                last = g[BLOCK - 1:BLOCK]
                qe = (qb * jnp.exp(g - ref)).astype(BF16)
                ke = (kb * jnp.exp(ref - g)).astype(BF16)
                scores = jnp.where(causal, dot(qe, ke, ((1,), (1,))), 0.0).astype(BF16)
                out = dot(scores, vb)
                if b:
                    qs = (qb * jnp.exp(g - base)).astype(BF16)
                    out += dot(qs, state.astype(BF16), ((1,), (1,)))
                lo[r, c] = out
                kd = (kb * jnp.exp(last - g)).astype(BF16)
                state = state * jnp.exp(last - base) + dot(vb, kd, ((0,), (0,)))
                base = last
            st[h, 0:dim, :] = state.astype(BF16)
            st[h, dim:, :] = jnp.broadcast_to(jnp.exp(base), (st.shape[1] - dim, dim)).astype(BF16)
            if h:
                poll(1)

    odd = lax.rem(me, PAIR)
    pair = lax.div(me, PAIR)
    swap = push(st, pst, sr.at[0], ep=1)
    own_half = pl.ds(odd * (heads // 2), heads // 2)
    other_half = pl.ds((1 - odd) * (heads // 2), heads // 2)
    trade = push(fst.at[own_half], fst.at[own_half], sr.at[1 + eps // PAIR], ep=1)

    def joined_copy(k):
        return push(cst, states.at[pair], sr.at[1 + pair], ep=k)

    def parts_of(ref, h):
        return ref[h, 0:dim, :].astype(F32), ref[h, dim:dim + 16, :].astype(F32)[0:1]

    def join_states():
        swap.wait_recv()
        for i in range(heads // 2):
            h = odd * (heads // 2) + i
            (own, keep), (other, pass_on) = parts_of(st, h), parts_of(pst, h)
            cst[i, 0:dim, :] = jnp.where(odd == 1, other * keep + own, own * pass_on + other).astype(BF16)
            cst[i, dim:, :] = jnp.broadcast_to(keep * pass_on, (st.shape[1] - dim, dim)).astype(BF16)
        for k in range(PAIR, eps, PAIR):
            @pl.when(ep_peer[k] > me)
            def _():
                joined_copy(k).start()

    def fold_states():
        @pl.loop(0, pair)
        def _(hop):
            pltpu.make_async_remote_copy(src_ref=cst, dst_ref=states.at[hop], send_sem=out_sem.at[0], recv_sem=sr.at[1 + hop],
                                         device_id={"ep": hop * PAIR + odd}, device_id_type=MESH).wait_recv()

        for i in range(heads // 2):
            def one(hop, state):
                own, pass_on = parts_of(states.at[hop], i)
                return state * pass_on + own

            state = lax.fori_loop(0, pair, one, jnp.zeros((dim, dim), F32))
            fst[odd * (heads // 2) + i] = state.astype(BF16)
        go(trade)

    def finish_mixer():
        push(fst.at[other_half], fst.at[other_half], sr.at[1 + eps // PAIR], ep=1).wait_recv()
        for h in range(heads):
            c = slice(h * dim, (h + 1) * dim)
            state = fst[h].astype(F32)
            other, pass_on = parts_of(pst, h)
            state = jnp.where(odd == 1, state * pass_on + other, state)
            out = lo[:, c] + dot(qd[:, c], state.astype(BF16), ((1,), (1,)))
            scale = lax.rsqrt(jnp.mean(out * out, axis=1, keepdims=True) + epsilon)
            gated[:, c] = (out * scale * hgain_ref[...].astype(F32) * og[:, c]).astype(BF16)
        loads[7].wait()
        for r in (3, 1, 2, 0):
            block = wm[:, pl.ds(pl.multiple_of(tp_peer[r] * cols, cols), cols)]
            mixed[r] = dot(gated[...], block).astype(BF16)

    tile = 256 if units % 256 == 0 else units
    def feed(chunks):
        for k in chunks:
            complete(k)
            r = chunk(k)
            squares = jnp.zeros((cap, 1), F32)
            for p in range(tps):
                v = gath[p, r, :].astype(F32)
                squares += jnp.sum(v * v, axis=1, keepdims=True)
            scale = lax.rsqrt(squares / depth + epsilon)
            for p in range(tps):
                for i in range(cols // lanes):
                    s = slice(i * lanes, (i + 1) * lanes)
                    n = p * (cols // lanes) + i
                    c = slice(n * lanes, (n + 1) * lanes)
                    enormed[r, c] = (gath[p, r, s].astype(F32) * scale * egain[n:n + 1]).astype(BF16)

    def chunk(k):
        return slice(k * cap, (k + 1) * cap)

    def span(chunks):
        return slice(chunks[0] * cap, (chunks[-1] + 1) * cap)

    def upward(chunks, polls=()):
        r = span(chunks)
        for u in range(units // tile):
            c = slice(u * tile, (u + 1) * tile)
            gate = dot(enormed[r, :], wg[:, c])
            up = dot(enormed[r, :], wu[:, c])
            hidden[0:len(chunks) * cap, c] = (gate * sigmoid(gate) * up).astype(BF16)
            if u in polls:
                poll(1)

    def downward(chunks, polls=()):
        r = span(chunks)
        for t in (3, 1, 2, 0):
            block = wd[:, pl.ds(pl.multiple_of(tp_peer[t] * cols, cols), cols)]
            psend[t, r, :] = dot(hidden[0:len(chunks) * cap, :], block).astype(BF16)
            if t in polls:
                poll(1)

    def summing(src, dst, a, b, recv):
        def part(n, index, target, r, tp):
            return push(src.at[index, r], dst.at[target, r], recv.at[n], tp=tp)

        first = [part(0, 3, 3, a, 1), part(1, 3, 3, b, 2), part(2, 1, 1, a, 1), part(2, 2, 2, b, 2)]
        second = [part(2, 2, 2, a, 2), part(2, 1, 1, b, 1)]
        landed = dst.at[pl.ds(1, 2), slice(a.start, b.stop)]

        def start(pieces=slice(0, 4)):
            for copy in first[pieces]:
                go(copy)

        def merge():
            first[0].wait_recv()
            src[2, a, :] = (src[2, a, :].astype(F32) + dst[3, a, :].astype(F32)).astype(BF16)
            first[1].wait_recv()
            src[1, b, :] = (src[1, b, :].astype(F32) + dst[3, b, :].astype(F32)).astype(BF16)
            for copy in second:
                go(copy)

        def finish():
            push(landed, landed, recv.at[2], tp=1).wait_recv()

        def value(r):
            return src[0, r, :].astype(F32) + dst[1, r, :].astype(F32) + dst[2, r, :].astype(F32)

        return start, merge, finish, value

    near = list(range(eps // 2))
    far = [[k, k + 1] for k in range(eps // 2, eps, 2)]
    nrows = len(near) * cap
    sums = [summing(psend, precv, chunk(a), chunk(b), pr.at[g]) for g, (a, b) in enumerate(far)]
    mixsum = summing(mixed, mixin, slice(0, half), slice(half, length), mr)
    toksum = summing(tok, tokin, slice(0, half), slice(half, length), tr)

    def near_copy(k):
        return push(psend.at[:, chunk(k)], nback.at[:, chunk(k)], br.at[0], ep=k)

    def give_near():
        for k in near[1:]:
            go(near_copy(k))
        nback[:, chunk(0), :] = psend[:, chunk(0), :]

    def take_near():
        landed = nback.at[:, span(near[1:])]
        push(landed, landed, br.at[0], ep=1).wait_recv()
        for t in (3, 1, 2, 0):
            value = jnp.zeros((length, cols), F32)
            for j in range(hits.shape[0]):
                value += dot(hits[j, :, 0:nrows], nback[t]) * weights[:, j:j + 1]
            tok[t] = value.astype(BF16)

    def give_far(g):
        _, _, finish, value = sums[g]
        finish()
        for k in far[g]:
            r = chunk(k)
            esum[r, :] = value(r).astype(BF16)
            go(push(esum.at[r], back.at[r], br.at[1 + g], ep=k))

    def take_far(g):
        r = span(far[g])
        push(back.at[r], back.at[r], br.at[1 + g], ep=1).wait_recv()
        value = jnp.zeros((length, cols), F32)
        for j in range(hits.shape[0]):
            value += dot(hits[j, :, r], back[r, :]) * weights[:, j:j + 1]
        return value

    scores = scores_ref[...]
    weights = dot(eye.astype(F32), scores / jnp.sum(scores, axis=0, keepdims=True), ((1,), (1,)), precision=HIGHEST)

    for step in range(heads // per):
        mix_step(step)
    go(swap)
    for load in loads[4:7]:
        load.wait()
    poll(len(agenda) - far_end)
    poll(2)
    join_states()
    feed(near)
    upward(near, polls=(1,))
    downward(near, polls=(1, 2))
    give_near()
    poll(len(agenda) - 1)
    fold_states()
    finish_mixer()
    mixsum[0](slice(0, 2))
    for g, chunks in enumerate(far):
        feed(chunks)
        upward(chunks, polls=(1,))
        if g:
            sums[g - 1][1]()
        downward(chunks)
        if g == 0:
            poll(len(agenda))
        sums[g][0]()
    mixsum[0](slice(2, 4))
    for g in range(len(far) - 1):
        give_far(g)
    sums[-1][1]()
    mixsum[1]()
    take_near()
    toksum[0]()
    give_far(len(far) - 1)
    toksum[1]()
    value = take_far(0)
    for g in range(1, len(far)):
        value += take_far(g)
    total[...] = value
    mixsum[2]()
    mix_out[...] = mixsum[3](slice(0, length)).astype(BF16)
    toksum[2]()
    moe_out[...] = (total[...] + toksum[3](slice(0, length))).astype(BF16)

    for copy in sent:
        copy.wait_send()
    for k in range(PAIR, eps, PAIR):
        @pl.when(ep_peer[k] > me)
        def _():
            joined_copy(k).wait_send()


def place_kernel(a_ref, b_ref, a_out, b_out, sem):
    copies = [pltpu.make_async_copy(a_ref, a_out, sem.at[0]), pltpu.make_async_copy(b_ref, b_out, sem.at[1])]
    for copy in copies:
        copy.start()
    for copy in copies:
        copy.wait()


def whole_block(mix_rows, mix_gain, wq, wf, wi, wo, gap, dec, hgain, wm, moe_rows, moe_gain, ids, scores, wg, wu, wd):
    eps, tps = lax.axis_size("ep"), lax.axis_size("tp")
    length, cols = mix_rows.shape
    top = ids.shape[1]
    cap = length * top * 3 // (2 * eps)
    rows = eps * cap
    heads = dec.shape[0]
    width = wq.shape[1]
    dim = width // heads
    depth, units = wg.shape[1:]
    dma = lambda *s: pltpu.SemaphoreType.DMA(s)
    out = jax.ShapeDtypeStruct((length, cols), BF16)
    scratch = [
        pltpu.VMEM((depth // 128, 128), BF16), pltpu.VMEM((1, width), F32), pltpu.VMEM(dec.shape, F32),
        pltpu.VMEM((1, dim), BF16), pltpu.VMEM((depth // 128, 128), BF16),
        pltpu.VMEM((top, length), jnp.int32), pltpu.VMEM((top, length), F32),
        pltpu.VMEM((length, cols), BF16), pltpu.VMEM((length, cols), BF16),
        pltpu.VMEM((4, depth, width), BF16), pltpu.VMEM((width, depth), BF16),
        pltpu.VMEM((depth, units), BF16), pltpu.VMEM((depth, units), BF16), pltpu.VMEM((units, depth), BF16),
        pltpu.VMEM((tps, length, cols), BF16), pltpu.VMEM((4, length, width), F32),
        pltpu.VMEM((length, width), F32), pltpu.VMEM((length, width), BF16), pltpu.VMEM((length, width), F32),
        pltpu.VMEM((heads, dim + 16, dim), BF16), pltpu.VMEM((heads, dim + 16, dim), BF16),
        pltpu.VMEM((heads // 2, dim + 16, dim), BF16), pltpu.VMEM((heads, dim, dim), BF16),
        pltpu.VMEM((eps // PAIR, heads // 2, dim + 16, dim), BF16),
        pltpu.VMEM((length, width), BF16), pltpu.VMEM((tps, length, cols), BF16), pltpu.VMEM((tps, length, cols), BF16),
        pltpu.VMEM((tps, rows, cols), BF16), pltpu.VMEM((rows, cols), BF16), pltpu.VMEM((top, length, rows), BF16),
        pltpu.VMEM((rows, depth), BF16), pltpu.VMEM((rows // 2, units), BF16),
        pltpu.VMEM((tps, rows, cols), BF16), pltpu.VMEM((tps, rows, cols), BF16),
        pltpu.VMEM((tps, rows // 2, cols), BF16), pltpu.VMEM((tps, length, cols), BF16), pltpu.VMEM((tps, length, cols), BF16),
        pltpu.VMEM((rows, cols), BF16), pltpu.VMEM((rows, cols), BF16), pltpu.VMEM((length, cols), F32),
        dma(14), dma(1), dma(3), dma(eps), dma(eps, 3), dma(eps // 4, 3), dma(1 + eps // 4),
        dma(2 + eps // PAIR), dma(3), dma(3),
    ]
    results = pl.pallas_call(
        functools.partial(block_kernel, cap),
        in_specs=[pl.BlockSpec(memory_space=pltpu.HBM)] * 17,
        out_specs=[VMEM, VMEM],
        out_shape=[pltpu.VMEM((length, cols), BF16)] * 2,
        scratch_shapes=scratch,
        compiler_params=pltpu.CompilerParams(vmem_limit_bytes=LIMIT, collective_id=0, has_side_effects=True),
    )(mix_rows, mix_gain.reshape(-1, 128), wq, wf, wi, wo, gap.reshape(1, -1), dec, hgain.reshape(1, -1), wm,
      moe_rows, moe_gain.reshape(-1, 128), ids.T, scores.T, wg, wu, wd)
    return pl.pallas_call(
        place_kernel,
        in_specs=[VMEM, VMEM],
        out_specs=[ANY, ANY],
        out_shape=[out, out],
        scratch_shapes=[dma(2)],
        compiler_params=pltpu.CompilerParams(vmem_limit_bytes=1024 * 1024),
    )(*results)


def fits(eps, tps, mix_rows, dec, route_ids, w_gate):
    tokens, cols = mix_rows.shape
    top = route_ids.shape[1]
    cap = tokens * top * 3 // (2 * eps)
    square = tps == 4 and dec.shape[0] % 2 == 0 and eps >= 4 and eps & (eps - 1) == 0
    aligned = cap % 32 == 0 and cols % 128 == 0 and tokens % (2 * BLOCK) == 0 and w_gate.shape[2] % 128 == 0
    return square and aligned and w_gate.shape[0] == 1


def per_device(mix_rows, mix_gain, w_query, w_forget, w_input, w_outgate, forget_gap, decay_extra,
               head_gain, w_mixout, moe_rows, moe_gain, route_ids, route_scores, w_gate, w_up, w_down):
    eps, tps = lax.axis_size("ep"), lax.axis_size("tp")
    if fits(eps, tps, mix_rows, decay_extra, route_ids, w_gate):
        return whole_block(mix_rows, mix_gain, w_query, w_forget, w_input, w_outgate, forget_gap, decay_extra,
                           head_gain, w_mixout, moe_rows, moe_gain, route_ids, route_scores, w_gate, w_up, w_down)
    tokens, top = route_ids.shape
    experts = w_gate.shape[0] * eps
    capacity = tokens * top * 3 // (2 * experts)
    cols = mix_rows.shape[1]
    ids = route_ids.T
    slots = dispatch(ids, moe_rows, experts, capacity)
    arrived = lax.all_to_all(slots.reshape(eps, -1, cols), "ep", split_axis=0, concat_axis=0, tiled=True)
    gathered = lax.all_gather(arrived.reshape(-1, cols), "tp", axis=0)
    mix_whole = lax.all_gather(mix_rows, "tp", axis=0)
    lo, qd, og, st = mixer(mix_whole, mix_gain, w_query, w_forget, w_input, w_outgate, forget_gap, decay_extra.T)
    product = experts_call(gathered, moe_gain, w_gate, w_up, w_down)
    expert_sum = lax.psum_scatter(product, "tp", scatter_dimension=0)
    states = lax.all_gather(st, "ep", axis=0)
    mixed = tail(states, lo, qd, og, head_gain, w_mixout, tps)
    mix_out = lax.psum_scatter(mixed, "tp", scatter_dimension=0)
    back = lax.all_to_all(expert_sum.reshape(eps, -1, cols), "ep", split_axis=0, concat_axis=0, tiled=True)
    moe_out = combine(ids, route_scores, back.reshape(-1, cols), experts, capacity)
    return (mix_out, moe_out)


def solution(mesh):
    placed = (
        P("ep", "tp"), P(), P(None, "tp"), P(None, "tp"), P(None, "tp"), P(None, "tp"), P("tp"),
        P("tp", "ep"), P(), P("tp", None), P("ep", "tp"), P(), P("ep", None), P("ep", None),
        P("ep", None, "tp"), P("ep", None, "tp"), P("ep", "tp", None),
    )
    return jax.shard_map(
        per_device, mesh=mesh, in_specs=placed,
        out_specs=(P("ep", "tp"), P("ep", "tp")), check_vma=False,
    )
```

```python
import functools

import jax
import jax.numpy as jnp
from jax import lax
from jax.experimental import pallas as pl
from jax.experimental.pallas import tpu as pltpu
from jax.sharding import PartitionSpec as P

BLOCK = 64
epsilon = 1e-06
F32 = jnp.float32
BF16 = jnp.bfloat16
VMEM = pl.BlockSpec(memory_space=pltpu.VMEM)
LIMIT = 60 * 1024 * 1024


def dot(a, b, dims=((1,), (0,)), precision=None):
    return lax.dot_general(a, b, (dims, ((), ())), precision=precision, preferred_element_type=F32)


def sigmoid(x):
    return 1.0 / (1.0 + jnp.exp(-x))


def iota(shape, dim):
    return lax.broadcasted_iota(jnp.int32, shape, dim)


def mixer_kernel(per, x_ref, gain_ref, wq_ref, wf_ref, wi_ref, wo_ref, gap_ref, dec_ref,
                 lo_ref, qd_ref, og_ref, st_ref, normed):
    step = pl.program_id(0)
    length = normed.shape[0]
    dim = st_ref.shape[2]
    parts, _, cols = x_ref.shape

    @pl.when(step == 0)
    def _():
        total = jnp.zeros((length, 1), F32)
        for p in range(parts):
            v = x_ref[p].astype(F32)
            total += jnp.sum(v * v, axis=1, keepdims=True)
        scale = lax.rsqrt(total / (parts * cols) + epsilon)
        for p in range(parts):
            g = gain_ref[:, p * cols:(p + 1) * cols].astype(F32)
            normed[:, p * cols:(p + 1) * cols] = (x_ref[p].astype(F32) * scale * g).astype(BF16)

    n = normed[...]
    qp = dot(n, wq_ref[...])
    fp = dot(n, wf_ref[...])
    value = dot(n, wi_ref[...]).astype(BF16)
    op = dot(n, wo_ref[...])
    query = qp * sigmoid(qp)
    key = gap_ref[...] * sigmoid(-fp)
    og_ref[...] = op * sigmoid(op)
    logs = jnp.log1p(-key)
    dec = dec_ref[...]
    tri = (iota((length, length), 0) >= iota((length, length), 1)).astype(F32)
    causal = iota((BLOCK, BLOCK), 0) >= iota((BLOCK, BLOCK), 1)
    half = BLOCK // 2
    for j in range(per):
        c = slice(j * dim, (j + 1) * dim)
        extra = jnp.sum(jnp.where(iota(dec.shape, 1) == step * per + j, dec, 0.0), axis=1, keepdims=True)
        run = dot(tri, logs[:, c] + extra, precision=lax.Precision.HIGHEST)
        q, k, v = query[:, c], key[:, c], value[:, c]
        qd_ref[:, c] = (q * jnp.exp(run)).astype(BF16)
        state = jnp.zeros((dim, dim), F32)
        base = jnp.zeros((1, dim), F32)
        for b in range(length // BLOCK):
            r = slice(b * BLOCK, (b + 1) * BLOCK)
            g, qb, kb, vb = run[r], q[r], k[r], v[r]
            ref = g[half - 1:half]
            last = g[BLOCK - 1:BLOCK]
            qe = (qb * jnp.exp(g - ref)).astype(BF16)
            ke = (kb * jnp.exp(ref - g)).astype(BF16)
            scores = jnp.where(causal, dot(qe, ke, ((1,), (1,))), 0.0).astype(BF16)
            out = dot(scores, vb)
            if b:
                qs = (qb * jnp.exp(g - base)).astype(BF16)
                out += dot(qs, state.astype(BF16), ((1,), (1,)))
            lo_ref[r, c] = out
            kd = (kb * jnp.exp(last - g)).astype(BF16)
            state = state * jnp.exp(last - base) + dot(vb, kd, ((0,), (0,)))
            base = last
        st_ref[j, 0:dim, :] = state.astype(BF16)
        st_ref[j, dim:, :] = jnp.broadcast_to(jnp.exp(base), (st_ref.shape[1] - dim, dim)).astype(BF16)


def mixer(x, gain, wq, wf, wi, wo, gap, dec):
    parts, length, cols = x.shape
    heads, dim = dec.shape[1], wq.shape[1] // dec.shape[1]
    per = 2 if heads % 2 == 0 else 1
    width = per * dim
    depth = wq.shape[0]
    column = pl.BlockSpec((depth, width), lambda i: (0, i))
    rows = pl.BlockSpec((length, width), lambda i: (0, i))
    whole = lambda s: pl.BlockSpec(s, lambda i: (0,) * len(s))
    return pl.pallas_call(
        functools.partial(mixer_kernel, per),
        grid=(heads // per,),
        in_specs=[whole(x.shape), whole((1, depth)), column, column, column, column,
                  pl.BlockSpec((1, width), lambda i: (0, i)), whole(dec.shape)],
        out_specs=[rows, rows, rows, pl.BlockSpec((per, dim + 16, dim), lambda i: (i, 0, 0))],
        out_shape=[jax.ShapeDtypeStruct((length, heads * dim), F32),
                   jax.ShapeDtypeStruct((length, heads * dim), BF16),
                   jax.ShapeDtypeStruct((length, heads * dim), F32),
                   jax.ShapeDtypeStruct((heads, dim + 16, dim), BF16)],
        scratch_shapes=[pltpu.VMEM((length, depth), BF16)],
        compiler_params=pltpu.CompilerParams(vmem_limit_bytes=LIMIT),
        cost_estimate=pl.CostEstimate(flops=10 * 10**9, bytes_accessed=9 * 10**6, transcendentals=10**6),
    )(x, gain.reshape(1, -1), wq, wf, wi, wo, gap.reshape(1, -1), dec)


def tail_kernel(states_ref, lo_ref, qd_ref, og_ref, hg_ref, w_ref, out_ref, gated):
    place = lax.axis_index("ep")
    hops, heads, _, dim = states_ref.shape
    for h in range(heads):
        c = slice(h * dim, (h + 1) * dim)

        def one(hop, state):
            own = states_ref[hop, h, 0:dim, :].astype(F32)
            passing = states_ref[hop, h, dim:dim + 16, :].astype(F32)[0:1]
            return jnp.where(hop < place, state * passing + own, state)

        state = lax.fori_loop(0, hops, one, jnp.zeros((dim, dim), F32))
        out = lo_ref[:, c] + dot(qd_ref[:, c], state.astype(BF16), ((1,), (1,)))
        scale = lax.rsqrt(jnp.mean(out * out, axis=1, keepdims=True) + epsilon)
        gated[:, c] = (out * scale * hg_ref[...].astype(F32) * og_ref[:, c]).astype(BF16)
    parts, _, cols = out_ref.shape
    for p in range(parts):
        out_ref[p] = dot(gated[...], w_ref[:, p * cols:(p + 1) * cols]).astype(BF16)


def tail(states, lo, qd, og, hg, w, parts):
    length, width = lo.shape
    return pl.pallas_call(
        tail_kernel,
        in_specs=[VMEM] * 6,
        out_specs=VMEM,
        out_shape=jax.ShapeDtypeStruct((parts, length, w.shape[1] // parts), BF16),
        scratch_shapes=[pltpu.VMEM((length, width), BF16)],
        compiler_params=pltpu.CompilerParams(vmem_limit_bytes=LIMIT),
        cost_estimate=pl.CostEstimate(flops=10**9, bytes_accessed=5 * 10**6, transcendentals=10**5),
    )(states, lo, qd, og, hg.reshape(1, -1), w)


def ranks(ids, experts):
    tokens = ids.shape[1]
    names = iota((experts, tokens), 0)
    picks = [names == ids[k:k + 1, :] for k in range(ids.shape[0])]
    chosen = functools.reduce(jnp.logical_or, picks)
    before = (iota((tokens, tokens), 0) < iota((tokens, tokens), 1)).astype(BF16)
    return picks, chosen, dot(chosen.astype(BF16), before)


def slot_hits(mask, rank, experts, capacity):
    rows = experts * capacity
    owner = iota((rows, experts), 0) - iota((rows, experts), 1) * capacity
    owner = jnp.logical_and(owner >= 0, owner < capacity).astype(F32)
    tokens = rank.shape[1]
    spread = dot(owner, jnp.where(mask, rank, -1.0))
    spot = dot(owner, iota((experts, tokens), 0).astype(F32)) * capacity
    return (spread >= 0.0) & (spread + spot == iota((rows, tokens), 0).astype(F32))


def dispatch_kernel(experts, capacity, ids_ref, rows_ref, out_ref):
    _, chosen, rank = ranks(ids_ref[...], experts)
    hits = slot_hits(chosen, rank, experts, capacity).astype(BF16)
    out_ref[...] = dot(hits, rows_ref[...]).astype(BF16)


def dispatch(ids, rows, experts, capacity):
    return pl.pallas_call(
        functools.partial(dispatch_kernel, experts, capacity),
        in_specs=[VMEM] * 2,
        out_specs=VMEM,
        out_shape=jax.ShapeDtypeStruct((experts * capacity, rows.shape[1]), BF16),
    )(ids, rows)


def combine_kernel(experts, capacity, ids_ref, scores_ref, back_ref, out_ref):
    picks, _, rank = ranks(ids_ref[...], experts)
    scores = scores_ref[...]
    weights = scores / jnp.sum(scores, axis=1, keepdims=True)
    total = jnp.zeros(out_ref.shape, F32)
    for k, mask in enumerate(picks):
        hits = slot_hits(mask, rank, experts, capacity).astype(BF16)
        total += dot(hits, back_ref[...], ((0,), (0,))) * weights[:, k:k + 1]
    out_ref[...] = total.astype(BF16)


def combine(ids, scores, back, experts, capacity):
    return pl.pallas_call(
        functools.partial(combine_kernel, experts, capacity),
        in_specs=[VMEM] * 3,
        out_specs=VMEM,
        out_shape=jax.ShapeDtypeStruct((ids.shape[1], back.shape[1]), BF16),
    )(ids, scores, back)


def expert_kernel(x_ref, gain_ref, wg_ref, wu_ref, wd_ref, out_ref, normed, total):
    step = pl.program_id(0)
    parts, rows, cols = x_ref.shape

    @pl.when(step == 0)
    def _():
        squares = jnp.zeros((rows, 1), F32)
        for p in range(parts):
            v = x_ref[p].astype(F32)
            squares += jnp.sum(v * v, axis=1, keepdims=True)
        scale = lax.rsqrt(squares / (parts * cols) + epsilon)
        for p in range(parts):
            g = gain_ref[:, p * cols:(p + 1) * cols].astype(F32)
            normed[:, p * cols:(p + 1) * cols] = (x_ref[p].astype(F32) * scale * g).astype(BF16)

    gate = dot(normed[...], wg_ref[0])
    up = dot(normed[...], wu_ref[0])
    hidden = (gate * sigmoid(gate) * up).astype(BF16)
    last = pl.num_programs(0) - 1
    for p in range(parts):
        c = slice(p * cols, (p + 1) * cols)
        part = dot(hidden, wd_ref[0, :, c])

        @pl.when(jnp.logical_and(step == 0, last > 0))
        def _():
            total[:, c] = part

        @pl.when(jnp.logical_and(step > 0, step < last))
        def _():
            total[:, c] += part

        @pl.when(step == last)
        def _():
            out_ref[p] = (jnp.where(step > 0, total[:, c], 0.0) + part).astype(BF16)


def experts_call(x, gain, wg, wu, wd):
    parts, rows, cols = x.shape
    depth, units = wg.shape[1:]
    tile = 256 if units % 256 == 0 else units
    return pl.pallas_call(
        expert_kernel,
        grid=(units // tile,),
        in_specs=[pl.BlockSpec(x.shape, lambda i: (0, 0, 0)), pl.BlockSpec((1, depth), lambda i: (0, 0)),
                  pl.BlockSpec((1, depth, tile), lambda i: (0, 0, i)),
                  pl.BlockSpec((1, depth, tile), lambda i: (0, 0, i)),
                  pl.BlockSpec((1, tile, depth), lambda i: (0, i, 0))],
        out_specs=pl.BlockSpec(x.shape, lambda i: (0, 0, 0)),
        out_shape=jax.ShapeDtypeStruct(x.shape, BF16),
        scratch_shapes=[pltpu.VMEM((rows, depth), BF16), pltpu.VMEM((rows, depth), F32)],
        compiler_params=pltpu.CompilerParams(vmem_limit_bytes=LIMIT),
        cost_estimate=pl.CostEstimate(flops=8 * 10**9, bytes_accessed=10**7, transcendentals=10**6),
    )(x, gain.reshape(1, -1), wg, wu, wd)

MESH = pl.DeviceIdType.MESH
ANY = pl.BlockSpec(memory_space=pl.ANY)
HIGHEST = lax.Precision.HIGHEST
PAIR = 2


def flip(place, bits):
    bit = 1
    while bit <= bits:
        if bits & bit:
            place = place + bit - 2 * bit * lax.rem(lax.div(place, bit), 2)
        bit *= 2
    return place


def block_kernel(cap, mix_hbm, mgain_hbm, wq_hbm, wf_hbm, wi_hbm, wo_hbm, gap_hbm, dec_hbm, hgain_hbm, wm_hbm,
                 moe_hbm, egain_hbm, ids_hbm, scores_hbm, wg_hbm, wu_hbm, wd_hbm,
                 mix_out, moe_out, mgain_ref, gap_ref, dec_ref, hgain_ref, egain_ref, ids_ref, scores_ref,
                 mix_ref, moe_ref, wmix, wm, wg, wu, wd, xall, acc, lo, qd, og, st, pst, cst, fst, states, gated, mixed, mixin,
                 gath, slots, hits, enormed, hidden, psend, precv, nback, tok, tokin, esum, back, total,
                 wsem, free_sem, out_sem, xr, zr, gr, pr, br, sr, mr, tr):
    eps, tps = lax.axis_size("ep"), lax.axis_size("tp")
    me, mt = lax.axis_index("ep"), lax.axis_index("tp")
    length, cols = mix_ref.shape
    rows = eps * cap
    heads, _, dim = st.shape
    depth = tps * cols
    units = wg.shape[1]
    ep_peer = [flip(me, k) for k in range(eps)]
    tp_peer = [flip(mt, r) for r in range(tps)]

    def push(src, dst, recv, ep=None, tp=None):
        where = {"ep": ep_peer[ep]} if tp is None else {"tp": tp_peer[tp]}
        return pltpu.make_async_remote_copy(src_ref=src, dst_ref=dst, send_sem=out_sem.at[0], recv_sem=recv,
                                            device_id=where, device_id_type=MESH)

    sent = []

    def go(copy):
        copy.start()
        sent.append(copy)

    loads = [pltpu.make_async_copy(s, wmix.at[i], wsem.at[0]) for i, s in enumerate((wq_hbm, wf_hbm, wi_hbm, wo_hbm))]
    loads += [pltpu.make_async_copy(wg_hbm.at[0], wg, wsem.at[1]), pltpu.make_async_copy(wu_hbm.at[0], wu, wsem.at[2]),
              pltpu.make_async_copy(wd_hbm.at[0], wd, wsem.at[3]), pltpu.make_async_copy(wm_hbm, wm, wsem.at[4])]
    barrier = pltpu.get_barrier_semaphore()
    leader = tps - 1
    leads = jnp.logical_and(lax.rem(me, PAIR) == 0, mt == leader)
    for j in range(eps // PAIR):
        @pl.when(jnp.logical_or(me != j * PAIR, mt != leader))
        def _():
            pl.semaphore_signal(barrier, inc=1, device_id={"ep": j * PAIR, "tp": leader}, device_id_type=MESH)
    for r in (1, 2):
        pl.semaphore_signal(barrier, inc=1, device_id={"tp": tp_peer[r]}, device_id_type=MESH)
    pl.semaphore_signal(barrier, inc=1, device_id={"ep": ep_peer[1]}, device_id_type=MESH)
    small = [(mix_hbm, mix_ref), (ids_hbm, ids_ref), (moe_hbm, moe_ref), (mgain_hbm, mgain_ref), (gap_hbm, gap_ref),
             (dec_hbm, dec_ref), (hgain_hbm, hgain_ref), (egain_hbm, egain_ref), (scores_hbm, scores_ref)]
    rowload = [pltpu.make_async_copy(src, dst, wsem.at[5 + i]) for i, (src, dst) in enumerate(small)]
    for load in rowload + loads:
        load.start()
    rowload[0].wait()

    @pl.when(leads)
    def _():
        pl.semaphore_wait(barrier, 3 + eps * tps - 1)
        for c in range(PAIR):
            for t in range(tps):
                if c or t != leader:
                    pl.semaphore_signal(free_sem, inc=1, device_id={"ep": me + c, "tp": t}, device_id_type=MESH)

    @pl.when(jnp.logical_not(leads))
    def _():
        pl.semaphore_wait(barrier, 3)


    half = length // 2
    go(push(mix_ref, xall.at[mt], xr.at[0], tp=1))
    go(push(mix_ref, xall.at[mt], xr.at[1], tp=2))

    experts = eps
    names = iota((length, experts), 1)
    rowload[1].wait()
    eye = iota((length, length), 0) == iota((length, length), 1)
    ids = dot(eye.astype(BF16), ids_ref[...].astype(F32).astype(BF16), ((1,), (1,))).astype(jnp.int32)
    picks = [ids[:, j:j + 1] == names for j in range(ids.shape[1])]
    chosen = functools.reduce(jnp.logical_or, picks)
    before = (iota((length, length), 0) > iota((length, length), 1)).astype(BF16)
    rank = dot(before, chosen.astype(BF16)).astype(jnp.int32)
    spot = rank + jnp.bitwise_xor(names, me) * cap
    rowload[2].wait()
    both = None
    for j, pick in enumerate(picks):
        at = jnp.sum(jnp.where(pick, spot, 0), axis=1, keepdims=True)
        hit = (iota((length, rows), 1) == at).astype(F32)
        hits[j] = hit.astype(BF16)
        both = hit if both is None else both + hit
    made = dot(both.astype(BF16), moe_ref[...], ((0,), (0,))).astype(BF16)
    slots[...] = made
    gath[mt, 0:cap, :] = made[0:cap]
    def send_slots(k):
        r = slice(k * cap, (k + 1) * cap)
        go(push(slots.at[r], gath.at[mt, r], zr.at[k], ep=k))

    def rowsof(k, part=None):
        if part is None:
            return pl.ds(k * cap, cap)
        return pl.ds(k * cap + part * (cap // 2), cap // 2)

    def spread(k):
        if k:
            push(slots.at[rowsof(k)], gath.at[mt, rowsof(k)], zr.at[k], ep=k).wait_recv()
        for n, r in enumerate((1, 2)):
            ref = gath.at[mt, rowsof(k)]
            go(push(ref, ref, gr.at[k, n], tp=r))

    def relay(k):
        for n, (source, target) in enumerate(((1, 2), (2, 1))):
            whole = gath.at[tp_peer[source], rowsof(k)]
            push(whole, whole, gr.at[k, n], tp=source).wait_recv()
            ref = gath.at[tp_peer[source], rowsof(k, n)]
            go(push(ref, ref, gr.at[k, 2], tp=target))

    def complete(k):
        ref = gath.at[tp_peer[3], rowsof(k)]
        push(ref, ref, gr.at[k, 2], tp=1).wait_recv()

    def relay_mix():
        for n, (source, target) in enumerate(((1, 2), (2, 1))):
            whole = xall.at[tp_peer[source]]
            push(whole, whole, xr.at[n], tp=source).wait_recv()
            ref = xall.at[tp_peer[source], pl.ds(n * half, half)]
            go(push(ref, ref, xr.at[2], tp=target))

    def complete_mix():
        ref = xall.at[tp_peer[3]]
        push(ref, ref, xr.at[2], tp=1).wait_recv()

    S, R = (lambda k: functools.partial(spread, k)), (lambda k: functools.partial(relay, k))
    agenda, ahead = [], eps // 2
    for k in range(1, ahead):
        agenda += [S(k + 2), R(k)] if k + 2 < ahead else [R(k)]
    far_start = len(agenda)
    spreads, relays = [S(k) for k in range(max(ahead, 3), eps)], [R(k) for k in range(ahead, eps)]
    agenda += spreads[:3]
    agenda += relays[:2] + spreads[3:] + relays[2:]
    far_end = len(agenda) - far_start

    def poll(count=1):
        for _ in range(min(count, len(agenda))):
            agenda.pop(0)()

    for load in rowload[3:]:
        load.wait()
    mgain, egain = mgain_ref[...].astype(F32), egain_ref[...].astype(F32)
    lanes = mgain.shape[1]
    per_shard = cols // lanes
    squares = [jnp.zeros((length, 1), F32)]

    def project(r, ref, first):
        p = tp_peer[r]
        v = ref[...].astype(F32)
        squares[0] += jnp.sum(v * v, axis=1, keepdims=True)
        gains = mgain[0:per_shard]
        for i in range(1, tps):
            gains = jnp.where(p == i, mgain[i * per_shard:(i + 1) * per_shard], gains)
        v = jnp.concatenate([v[:, i * lanes:(i + 1) * lanes] * gains[i:i + 1] for i in range(per_shard)], axis=1)
        v = v.astype(BF16)
        w = pl.ds(pl.multiple_of(p * cols, cols), cols)
        for i in range(4):
            part = dot(v, wmix[i, w, :])
            acc[i] = part if first else acc[i] + part

    send_slots(1)
    S(0)()

    @pl.when(jnp.logical_not(leads))
    def _():
        pl.semaphore_wait(free_sem, 1)

    for k in range(2, eps):
        send_slots(k)
    pltpu.make_async_copy(wmix, wmix, wsem.at[0]).wait()
    project(0, mix_ref, True)
    S(1)()
    relay_mix()
    project(1, xall.at[tp_peer[1]], False)
    R(0)()
    S(2)()
    project(2, xall.at[tp_peer[2]], False)
    complete_mix()
    poll(1)
    project(3, xall.at[tp_peer[3]], False)
    scale = lax.rsqrt(squares[0] / depth + epsilon)
    poll(1)

    tri = (iota((length, length), 0) >= iota((length, length), 1)).astype(F32)
    extra = dot(tri, dec_ref[...], ((1,), (1,)), precision=HIGHEST)
    causal = iota((BLOCK, BLOCK), 0) >= iota((BLOCK, BLOCK), 1)
    mid = BLOCK // 2
    per = 2 if heads % 2 == 0 else 1

    def mix_step(step):
        w = slice(step * per * dim, (step + 1) * per * dim)
        qp, fp, value, op = [acc[i, :, w] * scale for i in range(4)]
        value = value.astype(BF16)
        query = qp * sigmoid(qp)
        key = gap_ref[:, w] * sigmoid(-fp)
        og[:, w] = op * sigmoid(op)
        logs = jnp.log1p(-key)
        for j in range(per):
            h = step * per + j
            cl = slice(j * dim, (j + 1) * dim)
            c = slice(h * dim, (h + 1) * dim)
            run = dot(tri, logs[:, cl], precision=HIGHEST) + extra[:, h:h + 1]
            q, k, v = query[:, cl], key[:, cl], value[:, cl]
            qd[:, c] = (q * jnp.exp(run)).astype(BF16)
            state = jnp.zeros((dim, dim), F32)
            base = jnp.zeros((1, dim), F32)
            for b in range(length // BLOCK):
                r = slice(b * BLOCK, (b + 1) * BLOCK)
                g, qb, kb, vb = run[r], q[r], k[r], v[r]
                ref = g[mid - 1:mid]
                last = g[BLOCK - 1:BLOCK]
                qe = (qb * jnp.exp(g - ref)).astype(BF16)
                ke = (kb * jnp.exp(ref - g)).astype(BF16)
                scores = jnp.where(causal, dot(qe, ke, ((1,), (1,))), 0.0).astype(BF16)
                out = dot(scores, vb)
                if b:
                    qs = (qb * jnp.exp(g - base)).astype(BF16)
                    out += dot(qs, state.astype(BF16), ((1,), (1,)))
                lo[r, c] = out
                kd = (kb * jnp.exp(last - g)).astype(BF16)
                state = state * jnp.exp(last - base) + dot(vb, kd, ((0,), (0,)))
                base = last
            st[h, 0:dim, :] = state.astype(BF16)
            st[h, dim:, :] = jnp.broadcast_to(jnp.exp(base), (st.shape[1] - dim, dim)).astype(BF16)
            if h:
                poll(1)

    odd = lax.rem(me, PAIR)
    pair = lax.div(me, PAIR)
    swap = push(st, pst, sr.at[0], ep=1)
    own_half = pl.ds(odd * (heads // 2), heads // 2)
    other_half = pl.ds((1 - odd) * (heads // 2), heads // 2)
    trade = push(fst.at[own_half], fst.at[own_half], sr.at[1 + eps // PAIR], ep=1)

    def joined_copy(k):
        return push(cst, states.at[pair], sr.at[1 + pair], ep=k)

    def parts_of(ref, h):
        return ref[h, 0:dim, :].astype(F32), ref[h, dim:dim + 16, :].astype(F32)[0:1]

    def join_states():
        swap.wait_recv()
        for i in range(heads // 2):
            h = odd * (heads // 2) + i
            (own, keep), (other, pass_on) = parts_of(st, h), parts_of(pst, h)
            cst[i, 0:dim, :] = jnp.where(odd == 1, other * keep + own, own * pass_on + other).astype(BF16)
            cst[i, dim:, :] = jnp.broadcast_to(keep * pass_on, (st.shape[1] - dim, dim)).astype(BF16)
        for k in range(PAIR, eps, PAIR):
            @pl.when(ep_peer[k] > me)
            def _():
                joined_copy(k).start()

    def fold_states():
        @pl.loop(0, pair)
        def _(hop):
            pltpu.make_async_remote_copy(src_ref=cst, dst_ref=states.at[hop], send_sem=out_sem.at[0], recv_sem=sr.at[1 + hop],
                                         device_id={"ep": hop * PAIR + odd}, device_id_type=MESH).wait_recv()

        for i in range(heads // 2):
            def one(hop, state):
                own, pass_on = parts_of(states.at[hop], i)
                return state * pass_on + own

            state = lax.fori_loop(0, pair, one, jnp.zeros((dim, dim), F32))
            fst[odd * (heads // 2) + i] = state.astype(BF16)
        go(trade)

    def finish_mixer():
        push(fst.at[other_half], fst.at[other_half], sr.at[1 + eps // PAIR], ep=1).wait_recv()
        for h in range(heads):
            c = slice(h * dim, (h + 1) * dim)
            state = fst[h].astype(F32)
            other, pass_on = parts_of(pst, h)
            state = jnp.where(odd == 1, state * pass_on + other, state)
            out = lo[:, c] + dot(qd[:, c], state.astype(BF16), ((1,), (1,)))
            scale = lax.rsqrt(jnp.mean(out * out, axis=1, keepdims=True) + epsilon)
            gated[:, c] = (out * scale * hgain_ref[...].astype(F32) * og[:, c]).astype(BF16)
        loads[7].wait()
        for r in (3, 1, 2, 0):
            block = wm[:, pl.ds(pl.multiple_of(tp_peer[r] * cols, cols), cols)]
            mixed[r] = dot(gated[...], block).astype(BF16)

    tile = 256 if units % 256 == 0 else units
    def feed(chunks):
        for k in chunks:
            complete(k)
            r = chunk(k)
            squares = jnp.zeros((cap, 1), F32)
            for p in range(tps):
                v = gath[p, r, :].astype(F32)
                squares += jnp.sum(v * v, axis=1, keepdims=True)
            scale = lax.rsqrt(squares / depth + epsilon)
            for p in range(tps):
                for i in range(cols // lanes):
                    s = slice(i * lanes, (i + 1) * lanes)
                    n = p * (cols // lanes) + i
                    c = slice(n * lanes, (n + 1) * lanes)
                    enormed[r, c] = (gath[p, r, s].astype(F32) * scale * egain[n:n + 1]).astype(BF16)

    def chunk(k):
        return slice(k * cap, (k + 1) * cap)

    def span(chunks):
        return slice(chunks[0] * cap, (chunks[-1] + 1) * cap)

    def upward(chunks, polls=()):
        r = span(chunks)
        for u in range(units // tile):
            c = slice(u * tile, (u + 1) * tile)
            gate = dot(enormed[r, :], wg[:, c])
            up = dot(enormed[r, :], wu[:, c])
            hidden[0:len(chunks) * cap, c] = (gate * sigmoid(gate) * up).astype(BF16)
            if u in polls:
                poll(1)

    def downward(chunks, polls=()):
        r = span(chunks)
        for t in (3, 1, 2, 0):
            block = wd[:, pl.ds(pl.multiple_of(tp_peer[t] * cols, cols), cols)]
            psend[t, r, :] = dot(hidden[0:len(chunks) * cap, :], block).astype(BF16)
            if t in polls:
                poll(1)

    def summing(src, dst, a, b, recv):
        def part(n, index, target, r, tp):
            return push(src.at[index, r], dst.at[target, r], recv.at[n], tp=tp)

        first = [part(0, 3, 3, a, 1), part(1, 3, 3, b, 2), part(2, 1, 1, a, 1), part(2, 2, 2, b, 2)]
        second = [part(2, 2, 2, a, 2), part(2, 1, 1, b, 1)]
        landed = dst.at[pl.ds(1, 2), slice(a.start, b.stop)]

        def start(pieces=slice(0, 4)):
            for copy in first[pieces]:
                go(copy)

        def merge():
            first[0].wait_recv()
            src[2, a, :] = (src[2, a, :].astype(F32) + dst[3, a, :].astype(F32)).astype(BF16)
            first[1].wait_recv()
            src[1, b, :] = (src[1, b, :].astype(F32) + dst[3, b, :].astype(F32)).astype(BF16)
            for copy in second:
                go(copy)

        def finish():
            push(landed, landed, recv.at[2], tp=1).wait_recv()

        def value(r):
            return src[0, r, :].astype(F32) + dst[1, r, :].astype(F32) + dst[2, r, :].astype(F32)

        return start, merge, finish, value

    near = list(range(eps // 2))
    far = [[k, k + 1] for k in range(eps // 2, eps, 2)]
    nrows = len(near) * cap
    sums = [summing(psend, precv, chunk(a), chunk(b), pr.at[g]) for g, (a, b) in enumerate(far)]
    mixsum = summing(mixed, mixin, slice(0, half), slice(half, length), mr)
    toksum = summing(tok, tokin, slice(0, half), slice(half, length), tr)

    def near_copy(k):
        return push(psend.at[:, chunk(k)], nback.at[:, chunk(k)], br.at[0], ep=k)

    def give_near():
        for k in near[1:]:
            go(near_copy(k))
        nback[:, chunk(0), :] = psend[:, chunk(0), :]

    def take_near():
        landed = nback.at[:, span(near[1:])]
        push(landed, landed, br.at[0], ep=1).wait_recv()
        for t in (3, 1, 2, 0):
            value = jnp.zeros((length, cols), F32)
            for j in range(hits.shape[0]):
                value += dot(hits[j, :, 0:nrows], nback[t]) * weights[:, j:j + 1]
            tok[t] = value.astype(BF16)

    def give_far(g):
        _, _, finish, value = sums[g]
        finish()
        for k in far[g]:
            r = chunk(k)
            esum[r, :] = value(r).astype(BF16)
            go(push(esum.at[r], back.at[r], br.at[1 + g], ep=k))

    def take_far(g):
        r = span(far[g])
        push(back.at[r], back.at[r], br.at[1 + g], ep=1).wait_recv()
        value = jnp.zeros((length, cols), F32)
        for j in range(hits.shape[0]):
            value += dot(hits[j, :, r], back[r, :]) * weights[:, j:j + 1]
        return value

    scores = scores_ref[...]
    weights = dot(eye.astype(F32), scores / jnp.sum(scores, axis=0, keepdims=True), ((1,), (1,)), precision=HIGHEST)

    for step in range(heads // per):
        mix_step(step)
    go(swap)
    for load in loads[4:7]:
        load.wait()
    poll(len(agenda) - far_end)
    poll(2)
    join_states()
    feed(near)
    upward(near, polls=(1,))
    downward(near, polls=(1, 2))
    give_near()
    poll(len(agenda) - 1)
    fold_states()
    finish_mixer()
    mixsum[0](slice(0, 2))
    for g, chunks in enumerate(far):
        feed(chunks)
        upward(chunks, polls=(1,))
        if g:
            sums[g - 1][1]()
        downward(chunks)
        if g == 0:
            poll(len(agenda))
        sums[g][0]()
    mixsum[0](slice(2, 4))
    for g in range(len(far) - 1):
        give_far(g)
    sums[-1][1]()
    mixsum[1]()
    take_near()
    toksum[0]()
    give_far(len(far) - 1)
    toksum[1]()
    value = take_far(0)
    for g in range(1, len(far)):
        value += take_far(g)
    total[...] = value
    mixsum[2]()
    mix_out[...] = mixsum[3](slice(0, length)).astype(BF16)
    toksum[2]()
    moe_out[...] = (total[...] + toksum[3](slice(0, length))).astype(BF16)

    for copy in sent:
        copy.wait_send()
    for k in range(PAIR, eps, PAIR):
        @pl.when(ep_peer[k] > me)
        def _():
            joined_copy(k).wait_send()


def place_kernel(a_ref, b_ref, a_out, b_out, sem):
    copies = [pltpu.make_async_copy(a_ref, a_out, sem.at[0]), pltpu.make_async_copy(b_ref, b_out, sem.at[1])]
    for copy in copies:
        copy.start()
    for copy in copies:
        copy.wait()


def whole_block(mix_rows, mix_gain, wq, wf, wi, wo, gap, dec, hgain, wm, moe_rows, moe_gain, ids, scores, wg, wu, wd):
    eps, tps = lax.axis_size("ep"), lax.axis_size("tp")
    length, cols = mix_rows.shape
    top = ids.shape[1]
    cap = length * top * 3 // (2 * eps)
    rows = eps * cap
    heads = dec.shape[0]
    width = wq.shape[1]
    dim = width // heads
    depth, units = wg.shape[1:]
    dma = lambda *s: pltpu.SemaphoreType.DMA(s)
    out = jax.ShapeDtypeStruct((length, cols), BF16)
    scratch = [
        pltpu.VMEM((depth // 128, 128), BF16), pltpu.VMEM((1, width), F32), pltpu.VMEM(dec.shape, F32),
        pltpu.VMEM((1, dim), BF16), pltpu.VMEM((depth // 128, 128), BF16),
        pltpu.VMEM((top, length), jnp.int32), pltpu.VMEM((top, length), F32),
        pltpu.VMEM((length, cols), BF16), pltpu.VMEM((length, cols), BF16),
        pltpu.VMEM((4, depth, width), BF16), pltpu.VMEM((width, depth), BF16),
        pltpu.VMEM((depth, units), BF16), pltpu.VMEM((depth, units), BF16), pltpu.VMEM((units, depth), BF16),
        pltpu.VMEM((tps, length, cols), BF16), pltpu.VMEM((4, length, width), F32),
        pltpu.VMEM((length, width), F32), pltpu.VMEM((length, width), BF16), pltpu.VMEM((length, width), F32),
        pltpu.VMEM((heads, dim + 16, dim), BF16), pltpu.VMEM((heads, dim + 16, dim), BF16),
        pltpu.VMEM((heads // 2, dim + 16, dim), BF16), pltpu.VMEM((heads, dim, dim), BF16),
        pltpu.VMEM((eps // PAIR, heads // 2, dim + 16, dim), BF16),
        pltpu.VMEM((length, width), BF16), pltpu.VMEM((tps, length, cols), BF16), pltpu.VMEM((tps, length, cols), BF16),
        pltpu.VMEM((tps, rows, cols), BF16), pltpu.VMEM((rows, cols), BF16), pltpu.VMEM((top, length, rows), BF16),
        pltpu.VMEM((rows, depth), BF16), pltpu.VMEM((rows // 2, units), BF16),
        pltpu.VMEM((tps, rows, cols), BF16), pltpu.VMEM((tps, rows, cols), BF16),
        pltpu.VMEM((tps, rows // 2, cols), BF16), pltpu.VMEM((tps, length, cols), BF16), pltpu.VMEM((tps, length, cols), BF16),
        pltpu.VMEM((rows, cols), BF16), pltpu.VMEM((rows, cols), BF16), pltpu.VMEM((length, cols), F32),
        dma(14), pltpu.SemaphoreType.REGULAR, dma(1), dma(3), dma(eps), dma(eps, 3), dma(eps // 4, 3), dma(1 + eps // 4),
        dma(2 + eps // PAIR), dma(3), dma(3),
    ]
    results = pl.pallas_call(
        functools.partial(block_kernel, cap),
        in_specs=[pl.BlockSpec(memory_space=pltpu.HBM)] * 17,
        out_specs=[VMEM, VMEM],
        out_shape=[pltpu.VMEM((length, cols), BF16)] * 2,
        scratch_shapes=scratch,
        compiler_params=pltpu.CompilerParams(vmem_limit_bytes=LIMIT, collective_id=0, has_side_effects=True),
    )(mix_rows, mix_gain.reshape(-1, 128), wq, wf, wi, wo, gap.reshape(1, -1), dec, hgain.reshape(1, -1), wm,
      moe_rows, moe_gain.reshape(-1, 128), ids.T, scores.T, wg, wu, wd)
    return pl.pallas_call(
        place_kernel,
        in_specs=[VMEM, VMEM],
        out_specs=[ANY, ANY],
        out_shape=[out, out],
        scratch_shapes=[dma(2)],
        compiler_params=pltpu.CompilerParams(vmem_limit_bytes=1024 * 1024),
    )(*results)


def fits(eps, tps, mix_rows, dec, route_ids, w_gate):
    tokens, cols = mix_rows.shape
    top = route_ids.shape[1]
    cap = tokens * top * 3 // (2 * eps)
    square = tps == 4 and dec.shape[0] % 2 == 0 and eps >= 4 and eps & (eps - 1) == 0
    aligned = cap % 32 == 0 and cols % 128 == 0 and tokens % (2 * BLOCK) == 0 and w_gate.shape[2] % 128 == 0
    return square and aligned and w_gate.shape[0] == 1


def per_device(mix_rows, mix_gain, w_query, w_forget, w_input, w_outgate, forget_gap, decay_extra,
               head_gain, w_mixout, moe_rows, moe_gain, route_ids, route_scores, w_gate, w_up, w_down):
    eps, tps = lax.axis_size("ep"), lax.axis_size("tp")
    if fits(eps, tps, mix_rows, decay_extra, route_ids, w_gate):
        return whole_block(mix_rows, mix_gain, w_query, w_forget, w_input, w_outgate, forget_gap, decay_extra,
                           head_gain, w_mixout, moe_rows, moe_gain, route_ids, route_scores, w_gate, w_up, w_down)
    tokens, top = route_ids.shape
    experts = w_gate.shape[0] * eps
    capacity = tokens * top * 3 // (2 * experts)
    cols = mix_rows.shape[1]
    ids = route_ids.T
    slots = dispatch(ids, moe_rows, experts, capacity)
    arrived = lax.all_to_all(slots.reshape(eps, -1, cols), "ep", split_axis=0, concat_axis=0, tiled=True)
    gathered = lax.all_gather(arrived.reshape(-1, cols), "tp", axis=0)
    mix_whole = lax.all_gather(mix_rows, "tp", axis=0)
    lo, qd, og, st = mixer(mix_whole, mix_gain, w_query, w_forget, w_input, w_outgate, forget_gap, decay_extra.T)
    product = experts_call(gathered, moe_gain, w_gate, w_up, w_down)
    expert_sum = lax.psum_scatter(product, "tp", scatter_dimension=0)
    states = lax.all_gather(st, "ep", axis=0)
    mixed = tail(states, lo, qd, og, head_gain, w_mixout, tps)
    mix_out = lax.psum_scatter(mixed, "tp", scatter_dimension=0)
    back = lax.all_to_all(expert_sum.reshape(eps, -1, cols), "ep", split_axis=0, concat_axis=0, tiled=True)
    moe_out = combine(ids, route_scores, back.reshape(-1, cols), experts, capacity)
    return (mix_out, moe_out)


def solution(mesh):
    placed = (
        P("ep", "tp"), P(), P(None, "tp"), P(None, "tp"), P(None, "tp"), P(None, "tp"), P("tp"),
        P("tp", "ep"), P(), P("tp", None), P("ep", "tp"), P(), P("ep", None), P("ep", None),
        P("ep", None, "tp"), P("ep", None, "tp"), P("ep", "tp", None),
    )
    return jax.shard_map(
        per_device, mesh=mesh, in_specs=placed,
        out_specs=(P("ep", "tp"), P("ep", "tp")), check_vma=False,
    )
```

```python
import functools

import jax
import jax.numpy as jnp
from jax import lax
from jax.experimental import pallas as pl
from jax.experimental.pallas import tpu as pltpu
from jax.sharding import PartitionSpec as P

BLOCK = 64
epsilon = 1e-06
F32 = jnp.float32
BF16 = jnp.bfloat16
VMEM = pl.BlockSpec(memory_space=pltpu.VMEM)
LIMIT = 60 * 1024 * 1024


def dot(a, b, dims=((1,), (0,)), precision=None):
    return lax.dot_general(a, b, (dims, ((), ())), precision=precision, preferred_element_type=F32)


def sigmoid(x):
    return 1.0 / (1.0 + jnp.exp(-x))


def iota(shape, dim):
    return lax.broadcasted_iota(jnp.int32, shape, dim)


def mixer_kernel(per, x_ref, gain_ref, wq_ref, wf_ref, wi_ref, wo_ref, gap_ref, dec_ref,
                 lo_ref, qd_ref, og_ref, st_ref, normed):
    step = pl.program_id(0)
    length = normed.shape[0]
    dim = st_ref.shape[2]
    parts, _, cols = x_ref.shape

    @pl.when(step == 0)
    def _():
        total = jnp.zeros((length, 1), F32)
        for p in range(parts):
            v = x_ref[p].astype(F32)
            total += jnp.sum(v * v, axis=1, keepdims=True)
        scale = lax.rsqrt(total / (parts * cols) + epsilon)
        for p in range(parts):
            g = gain_ref[:, p * cols:(p + 1) * cols].astype(F32)
            normed[:, p * cols:(p + 1) * cols] = (x_ref[p].astype(F32) * scale * g).astype(BF16)

    n = normed[...]
    qp = dot(n, wq_ref[...])
    fp = dot(n, wf_ref[...])
    value = dot(n, wi_ref[...]).astype(BF16)
    op = dot(n, wo_ref[...])
    query = qp * sigmoid(qp)
    key = gap_ref[...] * sigmoid(-fp)
    og_ref[...] = op * sigmoid(op)
    logs = jnp.log1p(-key)
    dec = dec_ref[...]
    tri = (iota((length, length), 0) >= iota((length, length), 1)).astype(F32)
    causal = iota((BLOCK, BLOCK), 0) >= iota((BLOCK, BLOCK), 1)
    half = BLOCK // 2
    for j in range(per):
        c = slice(j * dim, (j + 1) * dim)
        extra = jnp.sum(jnp.where(iota(dec.shape, 1) == step * per + j, dec, 0.0), axis=1, keepdims=True)
        run = dot(tri, logs[:, c] + extra, precision=lax.Precision.HIGHEST)
        q, k, v = query[:, c], key[:, c], value[:, c]
        qd_ref[:, c] = (q * jnp.exp(run)).astype(BF16)
        state = jnp.zeros((dim, dim), F32)
        base = jnp.zeros((1, dim), F32)
        for b in range(length // BLOCK):
            r = slice(b * BLOCK, (b + 1) * BLOCK)
            g, qb, kb, vb = run[r], q[r], k[r], v[r]
            ref = g[half - 1:half]
            last = g[BLOCK - 1:BLOCK]
            qe = (qb * jnp.exp(g - ref)).astype(BF16)
            ke = (kb * jnp.exp(ref - g)).astype(BF16)
            scores = jnp.where(causal, dot(qe, ke, ((1,), (1,))), 0.0).astype(BF16)
            out = dot(scores, vb)
            if b:
                qs = (qb * jnp.exp(g - base)).astype(BF16)
                out += dot(qs, state.astype(BF16), ((1,), (1,)))
            lo_ref[r, c] = out
            kd = (kb * jnp.exp(last - g)).astype(BF16)
            state = state * jnp.exp(last - base) + dot(vb, kd, ((0,), (0,)))
            base = last
        st_ref[j, 0:dim, :] = state.astype(BF16)
        st_ref[j, dim:, :] = jnp.broadcast_to(jnp.exp(base), (st_ref.shape[1] - dim, dim)).astype(BF16)


def mixer(x, gain, wq, wf, wi, wo, gap, dec):
    parts, length, cols = x.shape
    heads, dim = dec.shape[1], wq.shape[1] // dec.shape[1]
    per = 2 if heads % 2 == 0 else 1
    width = per * dim
    depth = wq.shape[0]
    column = pl.BlockSpec((depth, width), lambda i: (0, i))
    rows = pl.BlockSpec((length, width), lambda i: (0, i))
    whole = lambda s: pl.BlockSpec(s, lambda i: (0,) * len(s))
    return pl.pallas_call(
        functools.partial(mixer_kernel, per),
        grid=(heads // per,),
        in_specs=[whole(x.shape), whole((1, depth)), column, column, column, column,
                  pl.BlockSpec((1, width), lambda i: (0, i)), whole(dec.shape)],
        out_specs=[rows, rows, rows, pl.BlockSpec((per, dim + 16, dim), lambda i: (i, 0, 0))],
        out_shape=[jax.ShapeDtypeStruct((length, heads * dim), F32),
                   jax.ShapeDtypeStruct((length, heads * dim), BF16),
                   jax.ShapeDtypeStruct((length, heads * dim), F32),
                   jax.ShapeDtypeStruct((heads, dim + 16, dim), BF16)],
        scratch_shapes=[pltpu.VMEM((length, depth), BF16)],
        compiler_params=pltpu.CompilerParams(vmem_limit_bytes=LIMIT),
        cost_estimate=pl.CostEstimate(flops=10 * 10**9, bytes_accessed=9 * 10**6, transcendentals=10**6),
    )(x, gain.reshape(1, -1), wq, wf, wi, wo, gap.reshape(1, -1), dec)


def tail_kernel(states_ref, lo_ref, qd_ref, og_ref, hg_ref, w_ref, out_ref, gated):
    place = lax.axis_index("ep")
    hops, heads, _, dim = states_ref.shape
    for h in range(heads):
        c = slice(h * dim, (h + 1) * dim)

        def one(hop, state):
            own = states_ref[hop, h, 0:dim, :].astype(F32)
            passing = states_ref[hop, h, dim:dim + 16, :].astype(F32)[0:1]
            return jnp.where(hop < place, state * passing + own, state)

        state = lax.fori_loop(0, hops, one, jnp.zeros((dim, dim), F32))
        out = lo_ref[:, c] + dot(qd_ref[:, c], state.astype(BF16), ((1,), (1,)))
        scale = lax.rsqrt(jnp.mean(out * out, axis=1, keepdims=True) + epsilon)
        gated[:, c] = (out * scale * hg_ref[...].astype(F32) * og_ref[:, c]).astype(BF16)
    parts, _, cols = out_ref.shape
    for p in range(parts):
        out_ref[p] = dot(gated[...], w_ref[:, p * cols:(p + 1) * cols]).astype(BF16)


def tail(states, lo, qd, og, hg, w, parts):
    length, width = lo.shape
    return pl.pallas_call(
        tail_kernel,
        in_specs=[VMEM] * 6,
        out_specs=VMEM,
        out_shape=jax.ShapeDtypeStruct((parts, length, w.shape[1] // parts), BF16),
        scratch_shapes=[pltpu.VMEM((length, width), BF16)],
        compiler_params=pltpu.CompilerParams(vmem_limit_bytes=LIMIT),
        cost_estimate=pl.CostEstimate(flops=10**9, bytes_accessed=5 * 10**6, transcendentals=10**5),
    )(states, lo, qd, og, hg.reshape(1, -1), w)


def ranks(ids, experts):
    tokens = ids.shape[1]
    names = iota((experts, tokens), 0)
    picks = [names == ids[k:k + 1, :] for k in range(ids.shape[0])]
    chosen = functools.reduce(jnp.logical_or, picks)
    before = (iota((tokens, tokens), 0) < iota((tokens, tokens), 1)).astype(BF16)
    return picks, chosen, dot(chosen.astype(BF16), before)


def slot_hits(mask, rank, experts, capacity):
    rows = experts * capacity
    owner = iota((rows, experts), 0) - iota((rows, experts), 1) * capacity
    owner = jnp.logical_and(owner >= 0, owner < capacity).astype(F32)
    tokens = rank.shape[1]
    spread = dot(owner, jnp.where(mask, rank, -1.0))
    spot = dot(owner, iota((experts, tokens), 0).astype(F32)) * capacity
    return (spread >= 0.0) & (spread + spot == iota((rows, tokens), 0).astype(F32))


def dispatch_kernel(experts, capacity, ids_ref, rows_ref, out_ref):
    _, chosen, rank = ranks(ids_ref[...], experts)
    hits = slot_hits(chosen, rank, experts, capacity).astype(BF16)
    out_ref[...] = dot(hits, rows_ref[...]).astype(BF16)


def dispatch(ids, rows, experts, capacity):
    return pl.pallas_call(
        functools.partial(dispatch_kernel, experts, capacity),
        in_specs=[VMEM] * 2,
        out_specs=VMEM,
        out_shape=jax.ShapeDtypeStruct((experts * capacity, rows.shape[1]), BF16),
    )(ids, rows)


def combine_kernel(experts, capacity, ids_ref, scores_ref, back_ref, out_ref):
    picks, _, rank = ranks(ids_ref[...], experts)
    scores = scores_ref[...]
    weights = scores / jnp.sum(scores, axis=1, keepdims=True)
    total = jnp.zeros(out_ref.shape, F32)
    for k, mask in enumerate(picks):
        hits = slot_hits(mask, rank, experts, capacity).astype(BF16)
        total += dot(hits, back_ref[...], ((0,), (0,))) * weights[:, k:k + 1]
    out_ref[...] = total.astype(BF16)


def combine(ids, scores, back, experts, capacity):
    return pl.pallas_call(
        functools.partial(combine_kernel, experts, capacity),
        in_specs=[VMEM] * 3,
        out_specs=VMEM,
        out_shape=jax.ShapeDtypeStruct((ids.shape[1], back.shape[1]), BF16),
    )(ids, scores, back)


def expert_kernel(x_ref, gain_ref, wg_ref, wu_ref, wd_ref, out_ref, normed, total):
    step = pl.program_id(0)
    parts, rows, cols = x_ref.shape

    @pl.when(step == 0)
    def _():
        squares = jnp.zeros((rows, 1), F32)
        for p in range(parts):
            v = x_ref[p].astype(F32)
            squares += jnp.sum(v * v, axis=1, keepdims=True)
        scale = lax.rsqrt(squares / (parts * cols) + epsilon)
        for p in range(parts):
            g = gain_ref[:, p * cols:(p + 1) * cols].astype(F32)
            normed[:, p * cols:(p + 1) * cols] = (x_ref[p].astype(F32) * scale * g).astype(BF16)

    gate = dot(normed[...], wg_ref[0])
    up = dot(normed[...], wu_ref[0])
    hidden = (gate * sigmoid(gate) * up).astype(BF16)
    last = pl.num_programs(0) - 1
    for p in range(parts):
        c = slice(p * cols, (p + 1) * cols)
        part = dot(hidden, wd_ref[0, :, c])

        @pl.when(jnp.logical_and(step == 0, last > 0))
        def _():
            total[:, c] = part

        @pl.when(jnp.logical_and(step > 0, step < last))
        def _():
            total[:, c] += part

        @pl.when(step == last)
        def _():
            out_ref[p] = (jnp.where(step > 0, total[:, c], 0.0) + part).astype(BF16)


def experts_call(x, gain, wg, wu, wd):
    parts, rows, cols = x.shape
    depth, units = wg.shape[1:]
    tile = 256 if units % 256 == 0 else units
    return pl.pallas_call(
        expert_kernel,
        grid=(units // tile,),
        in_specs=[pl.BlockSpec(x.shape, lambda i: (0, 0, 0)), pl.BlockSpec((1, depth), lambda i: (0, 0)),
                  pl.BlockSpec((1, depth, tile), lambda i: (0, 0, i)),
                  pl.BlockSpec((1, depth, tile), lambda i: (0, 0, i)),
                  pl.BlockSpec((1, tile, depth), lambda i: (0, i, 0))],
        out_specs=pl.BlockSpec(x.shape, lambda i: (0, 0, 0)),
        out_shape=jax.ShapeDtypeStruct(x.shape, BF16),
        scratch_shapes=[pltpu.VMEM((rows, depth), BF16), pltpu.VMEM((rows, depth), F32)],
        compiler_params=pltpu.CompilerParams(vmem_limit_bytes=LIMIT),
        cost_estimate=pl.CostEstimate(flops=8 * 10**9, bytes_accessed=10**7, transcendentals=10**6),
    )(x, gain.reshape(1, -1), wg, wu, wd)

MESH = pl.DeviceIdType.MESH
ANY = pl.BlockSpec(memory_space=pl.ANY)
HIGHEST = lax.Precision.HIGHEST
PAIR = 2


def flip(place, bits):
    bit = 1
    while bit <= bits:
        if bits & bit:
            place = place + bit - 2 * bit * lax.rem(lax.div(place, bit), 2)
        bit *= 2
    return place


def block_kernel(cap, mix_hbm, mgain_hbm, wq_hbm, wf_hbm, wi_hbm, wo_hbm, gap_hbm, dec_hbm, hgain_hbm, wm_hbm,
                 moe_hbm, egain_hbm, ids_hbm, scores_hbm, wg_hbm, wu_hbm, wd_hbm,
                 mix_out, moe_out, mgain_ref, gap_ref, dec_ref, hgain_ref, egain_ref, ids_ref, scores_ref,
                 mix_ref, moe_ref, wmix, wm, wg, wu, wd, xall, acc, lo, qd, og, st, pst, cst, fst, states, gated, mixed, mixin,
                 gath, slots, hits, enormed, hidden, psend, precv, nback, tok, tokin, esum, back, total,
                 wsem, free_sem, out_sem, xr, zr, gr, pr, br, sr, mr, tr):
    eps, tps = lax.axis_size("ep"), lax.axis_size("tp")
    me, mt = lax.axis_index("ep"), lax.axis_index("tp")
    length, cols = mix_ref.shape
    rows = eps * cap
    heads, _, dim = st.shape
    depth = tps * cols
    units = wg.shape[1]
    ep_peer = [flip(me, k) for k in range(eps)]
    tp_peer = [flip(mt, r) for r in range(tps)]

    def push(src, dst, recv, ep=None, tp=None):
        where = {"ep": ep_peer[ep]} if tp is None else {"tp": tp_peer[tp]}
        return pltpu.make_async_remote_copy(src_ref=src, dst_ref=dst, send_sem=out_sem.at[0], recv_sem=recv,
                                            device_id=where, device_id_type=MESH)

    sent = []

    def go(copy):
        copy.start()
        sent.append(copy)

    loads = [pltpu.make_async_copy(s, wmix.at[i], wsem.at[0]) for i, s in enumerate((wq_hbm, wf_hbm, wi_hbm, wo_hbm))]
    loads += [pltpu.make_async_copy(wg_hbm.at[0], wg, wsem.at[1]), pltpu.make_async_copy(wu_hbm.at[0], wu, wsem.at[2]),
              pltpu.make_async_copy(wd_hbm.at[0], wd, wsem.at[3]), pltpu.make_async_copy(wm_hbm, wm, wsem.at[4])]
    barrier = pltpu.get_barrier_semaphore()
    leader = tps - 1
    leads = jnp.logical_and(lax.rem(me, PAIR) == 0, mt == leader)
    for j in range(eps // PAIR):
        @pl.when(jnp.logical_or(me != j * PAIR, mt != leader))
        def _():
            pl.semaphore_signal(barrier, inc=1, device_id={"ep": j * PAIR, "tp": leader}, device_id_type=MESH)
    for r in (1, 2):
        pl.semaphore_signal(barrier, inc=1, device_id={"tp": tp_peer[r]}, device_id_type=MESH)
    pl.semaphore_signal(barrier, inc=1, device_id={"ep": ep_peer[1]}, device_id_type=MESH)
    small = [(mix_hbm, mix_ref), (ids_hbm, ids_ref), (moe_hbm, moe_ref), (mgain_hbm, mgain_ref), (gap_hbm, gap_ref),
             (dec_hbm, dec_ref), (hgain_hbm, hgain_ref), (egain_hbm, egain_ref), (scores_hbm, scores_ref)]
    rowload = [pltpu.make_async_copy(src, dst, wsem.at[5 + i]) for i, (src, dst) in enumerate(small)]
    for load in rowload + loads:
        load.start()
    rowload[0].wait()

    @pl.when(leads)
    def _():
        pl.semaphore_wait(barrier, 3 + eps * tps - 1)
        for c in range(PAIR):
            for t in range(tps):
                if c or t != leader:
                    pl.semaphore_signal(free_sem, inc=1, device_id={"ep": me + c, "tp": t}, device_id_type=MESH)

    @pl.when(jnp.logical_not(leads))
    def _():
        pl.semaphore_wait(barrier, 3)


    half = length // 2
    go(push(mix_ref, xall.at[mt], xr.at[0], tp=1))
    go(push(mix_ref, xall.at[mt], xr.at[1], tp=2))

    experts = eps
    names = iota((length, experts), 1)
    rowload[1].wait()
    eye = iota((length, length), 0) == iota((length, length), 1)
    ids = dot(eye.astype(BF16), ids_ref[...].astype(F32).astype(BF16), ((1,), (1,))).astype(jnp.int32)
    picks = [ids[:, j:j + 1] == names for j in range(ids.shape[1])]
    chosen = functools.reduce(jnp.logical_or, picks)
    before = (iota((length, length), 0) > iota((length, length), 1)).astype(BF16)
    rank = dot(before, chosen.astype(BF16)).astype(jnp.int32)
    spot = rank + jnp.bitwise_xor(names, me) * cap
    rowload[2].wait()
    both = None
    for j, pick in enumerate(picks):
        at = jnp.sum(jnp.where(pick, spot, 0), axis=1, keepdims=True)
        hit = (iota((length, rows), 1) == at).astype(F32)
        hits[j] = hit.astype(BF16)
        both = hit if both is None else both + hit
    made = dot(both.astype(BF16), moe_ref[...], ((0,), (0,))).astype(BF16)
    slots[...] = made
    gath[mt, 0:cap, :] = made[0:cap]
    def send_slots(k):
        r = slice(k * cap, (k + 1) * cap)
        go(push(slots.at[r], gath.at[mt, r], zr.at[k], ep=k))

    def rowsof(k, part=None):
        if part is None:
            return pl.ds(k * cap, cap)
        return pl.ds(k * cap + part * (cap // 2), cap // 2)

    def spread(k):
        if k:
            push(slots.at[rowsof(k)], gath.at[mt, rowsof(k)], zr.at[k], ep=k).wait_recv()
        for n, r in enumerate((1, 2)):
            ref = gath.at[mt, rowsof(k)]
            go(push(ref, ref, gr.at[k, n], tp=r))

    def relay(k):
        for n, (source, target) in enumerate(((1, 2), (2, 1))):
            whole = gath.at[tp_peer[source], rowsof(k)]
            push(whole, whole, gr.at[k, n], tp=source).wait_recv()
            ref = gath.at[tp_peer[source], rowsof(k, n)]
            go(push(ref, ref, gr.at[k, 2], tp=target))

    def complete(k):
        ref = gath.at[tp_peer[3], rowsof(k)]
        push(ref, ref, gr.at[k, 2], tp=1).wait_recv()

    def relay_mix():
        for n, (source, target) in enumerate(((1, 2), (2, 1))):
            whole = xall.at[tp_peer[source]]
            push(whole, whole, xr.at[n], tp=source).wait_recv()
            ref = xall.at[tp_peer[source], pl.ds(n * half, half)]
            go(push(ref, ref, xr.at[2], tp=target))

    def complete_mix():
        ref = xall.at[tp_peer[3]]
        push(ref, ref, xr.at[2], tp=1).wait_recv()

    S, R = (lambda k: functools.partial(spread, k)), (lambda k: functools.partial(relay, k))
    agenda, ahead = [], eps // 2
    for k in range(1, ahead):
        agenda += [S(k + 2), R(k)] if k + 2 < ahead else [R(k)]
    far_start = len(agenda)
    spreads, relays = [S(k) for k in range(max(ahead, 3), eps)], [R(k) for k in range(ahead, eps)]
    agenda += spreads[:3]
    agenda += relays[:2] + spreads[3:] + relays[2:]
    far_end = len(agenda) - far_start

    def poll(count=1):
        for _ in range(min(count, len(agenda))):
            agenda.pop(0)()

    for load in rowload[3:]:
        load.wait()
    mgain, egain = mgain_ref[...].astype(F32), egain_ref[...].astype(F32)
    lanes = mgain.shape[1]
    per_shard = cols // lanes
    squares = [jnp.zeros((length, 1), F32)]

    def project(r, ref, first):
        p = tp_peer[r]
        v = ref[...].astype(F32)
        squares[0] += jnp.sum(v * v, axis=1, keepdims=True)
        gains = mgain[0:per_shard]
        for i in range(1, tps):
            gains = jnp.where(p == i, mgain[i * per_shard:(i + 1) * per_shard], gains)
        v = jnp.concatenate([v[:, i * lanes:(i + 1) * lanes] * gains[i:i + 1] for i in range(per_shard)], axis=1)
        v = v.astype(BF16)
        w = pl.ds(pl.multiple_of(p * cols, cols), cols)
        for i in range(4):
            part = dot(v, wmix[i, w, :])
            acc[i] = part if first else acc[i] + part

    send_slots(1)
    S(0)()

    @pl.when(jnp.logical_not(leads))
    def _():
        pl.semaphore_wait(free_sem, 1)

    for k in range(2, eps):
        send_slots(k)
    pltpu.make_async_copy(wmix, wmix, wsem.at[0]).wait()
    project(0, mix_ref, True)
    S(1)()
    relay_mix()
    project(1, xall.at[tp_peer[1]], False)
    R(0)()
    S(2)()
    project(2, xall.at[tp_peer[2]], False)
    complete_mix()
    poll(1)
    project(3, xall.at[tp_peer[3]], False)
    scale = lax.rsqrt(squares[0] / depth + epsilon)
    poll(1)

    tri = (iota((length, length), 0) >= iota((length, length), 1)).astype(F32)
    extra = dot(tri, dec_ref[...], ((1,), (1,)), precision=HIGHEST)
    causal = iota((BLOCK, BLOCK), 0) >= iota((BLOCK, BLOCK), 1)
    mid = BLOCK // 2
    per = 2 if heads % 2 == 0 else 1

    def mix_step(step):
        w = slice(step * per * dim, (step + 1) * per * dim)
        qp, fp, value, op = [acc[i, :, w] * scale for i in range(4)]
        value = value.astype(BF16)
        query = qp * sigmoid(qp)
        key = gap_ref[:, w] * sigmoid(-fp)
        og[:, w] = op * sigmoid(op)
        logs = jnp.log1p(-key)
        for j in range(per):
            h = step * per + j
            cl = slice(j * dim, (j + 1) * dim)
            c = slice(h * dim, (h + 1) * dim)
            run = dot(tri, logs[:, cl], precision=HIGHEST) + extra[:, h:h + 1]
            q, k, v = query[:, cl], key[:, cl], value[:, cl]
            qd[:, c] = (q * jnp.exp(run)).astype(BF16)
            state = jnp.zeros((dim, dim), F32)
            base = jnp.zeros((1, dim), F32)
            for b in range(length // BLOCK):
                r = slice(b * BLOCK, (b + 1) * BLOCK)
                g, qb, kb, vb = run[r], q[r], k[r], v[r]
                ref = g[mid - 1:mid]
                last = g[BLOCK - 1:BLOCK]
                qe = (qb * jnp.exp(g - ref)).astype(BF16)
                ke = (kb * jnp.exp(ref - g)).astype(BF16)
                scores = jnp.where(causal, dot(qe, ke, ((1,), (1,))), 0.0).astype(BF16)
                out = dot(scores, vb)
                if b:
                    qs = (qb * jnp.exp(g - base)).astype(BF16)
                    out += dot(qs, state.astype(BF16), ((1,), (1,)))
                lo[r, c] = out
                kd = (kb * jnp.exp(last - g)).astype(BF16)
                state = state * jnp.exp(last - base) + dot(vb, kd, ((0,), (0,)))
                base = last
            st[h, 0:dim, :] = state.astype(BF16)
            st[h, dim:, :] = jnp.broadcast_to(jnp.exp(base), (st.shape[1] - dim, dim)).astype(BF16)
            if h:
                poll(1)

    odd = lax.rem(me, PAIR)
    pair = lax.div(me, PAIR)
    swap = push(st, pst, sr.at[0], ep=1)
    own_half = pl.ds(odd * (heads // 2), heads // 2)
    other_half = pl.ds((1 - odd) * (heads // 2), heads // 2)
    trade = push(fst.at[own_half], fst.at[own_half], sr.at[1 + eps // PAIR], ep=1)

    def joined_copy(k):
        return push(cst, states.at[pair], sr.at[1 + pair], ep=k)

    def parts_of(ref, h):
        return ref[h, 0:dim, :].astype(F32), ref[h, dim:dim + 16, :].astype(F32)[0:1]

    def join_states():
        swap.wait_recv()
        for i in range(heads // 2):
            h = odd * (heads // 2) + i
            (own, keep), (other, pass_on) = parts_of(st, h), parts_of(pst, h)
            cst[i, 0:dim, :] = jnp.where(odd == 1, other * keep + own, own * pass_on + other).astype(BF16)
            cst[i, dim:, :] = jnp.broadcast_to(keep * pass_on, (st.shape[1] - dim, dim)).astype(BF16)
        for k in range(PAIR, eps, PAIR):
            @pl.when(ep_peer[k] > me)
            def _():
                joined_copy(k).start()

    def fold_states():
        @pl.loop(0, pair)
        def _(hop):
            pltpu.make_async_remote_copy(src_ref=cst, dst_ref=states.at[hop], send_sem=out_sem.at[0], recv_sem=sr.at[1 + hop],
                                         device_id={"ep": hop * PAIR + odd}, device_id_type=MESH).wait_recv()

        for i in range(heads // 2):
            def one(hop, state):
                own, pass_on = parts_of(states.at[hop], i)
                return state * pass_on + own

            state = lax.fori_loop(0, pair, one, jnp.zeros((dim, dim), F32))
            fst[odd * (heads // 2) + i] = state.astype(BF16)
        go(trade)

    def finish_mixer():
        push(fst.at[other_half], fst.at[other_half], sr.at[1 + eps // PAIR], ep=1).wait_recv()
        for h in range(heads):
            c = slice(h * dim, (h + 1) * dim)
            state = fst[h].astype(F32)
            other, pass_on = parts_of(pst, h)
            state = jnp.where(odd == 1, state * pass_on + other, state)
            out = lo[:, c] + dot(qd[:, c], state.astype(BF16), ((1,), (1,)))
            scale = lax.rsqrt(jnp.mean(out * out, axis=1, keepdims=True) + epsilon)
            gated[:, c] = (out * scale * hgain_ref[...].astype(F32) * og[:, c]).astype(BF16)
        loads[7].wait()
        for r in (3, 1, 2, 0):
            block = wm[:, pl.ds(pl.multiple_of(tp_peer[r] * cols, cols), cols)]
            mixed[r] = dot(gated[...], block).astype(BF16)

    tile = 256 if units % 256 == 0 else units
    def feed(chunks):
        for k in chunks:
            complete(k)
            r = chunk(k)
            squares = jnp.zeros((cap, 1), F32)
            for p in range(tps):
                v = gath[p, r, :].astype(F32)
                squares += jnp.sum(v * v, axis=1, keepdims=True)
            scale = lax.rsqrt(squares / depth + epsilon)
            for p in range(tps):
                for i in range(cols // lanes):
                    s = slice(i * lanes, (i + 1) * lanes)
                    n = p * (cols // lanes) + i
                    c = slice(n * lanes, (n + 1) * lanes)
                    enormed[r, c] = (gath[p, r, s].astype(F32) * scale * egain[n:n + 1]).astype(BF16)

    def chunk(k):
        return slice(k * cap, (k + 1) * cap)

    def span(chunks):
        return slice(chunks[0] * cap, (chunks[-1] + 1) * cap)

    def upward(chunks, polls=(), skip=0):
        r = span(chunks)
        rows_to = slice(skip * cap, (skip + len(chunks)) * cap)
        for u in range(units // tile):
            c = slice(u * tile, (u + 1) * tile)
            gate = dot(enormed[r, :], wg[:, c])
            up = dot(enormed[r, :], wu[:, c])
            hidden[rows_to, c] = (gate * sigmoid(gate) * up).astype(BF16)
            if u in polls:
                poll(1)

    def downward(chunks, polls=()):
        r = span(chunks)
        for t in (3, 1, 2, 0):
            block = wd[:, pl.ds(pl.multiple_of(tp_peer[t] * cols, cols), cols)]
            psend[t, r, :] = dot(hidden[0:len(chunks) * cap, :], block).astype(BF16)
            if t in polls:
                poll(1)

    def summing(src, dst, a, b, recv):
        def part(n, index, target, r, tp):
            return push(src.at[index, r], dst.at[target, r], recv.at[n], tp=tp)

        first = [part(0, 3, 3, a, 1), part(1, 3, 3, b, 2), part(2, 1, 1, a, 1), part(2, 2, 2, b, 2)]
        second = [part(2, 2, 2, a, 2), part(2, 1, 1, b, 1)]
        landed = dst.at[pl.ds(1, 2), slice(a.start, b.stop)]

        def start(pieces=slice(0, 4)):
            for copy in first[pieces]:
                go(copy)

        def merge():
            first[0].wait_recv()
            src[2, a, :] = (src[2, a, :].astype(F32) + dst[3, a, :].astype(F32)).astype(BF16)
            first[1].wait_recv()
            src[1, b, :] = (src[1, b, :].astype(F32) + dst[3, b, :].astype(F32)).astype(BF16)
            for copy in second:
                go(copy)

        def finish():
            push(landed, landed, recv.at[2], tp=1).wait_recv()

        def value(r):
            return src[0, r, :].astype(F32) + dst[1, r, :].astype(F32) + dst[2, r, :].astype(F32)

        return start, merge, finish, value

    near = list(range(eps // 2))
    far = [[k, k + 1] for k in range(eps // 2, eps, 2)]
    nrows = len(near) * cap
    sums = [summing(psend, precv, chunk(a), chunk(b), pr.at[g]) for g, (a, b) in enumerate(far)]
    mixsum = summing(mixed, mixin, slice(0, half), slice(half, length), mr)
    toksum = summing(tok, tokin, slice(0, half), slice(half, length), tr)

    def near_copy(k):
        return push(psend.at[:, chunk(k)], nback.at[:, chunk(k)], br.at[0], ep=k)

    def give_near():
        for k in near[1:]:
            go(near_copy(k))
        nback[:, chunk(0), :] = psend[:, chunk(0), :]

    def take_near():
        landed = nback.at[:, span(near[1:])]
        push(landed, landed, br.at[0], ep=1).wait_recv()
        for t in (3, 1, 2, 0):
            value = jnp.zeros((length, cols), F32)
            for j in range(hits.shape[0]):
                value += dot(hits[j, :, 0:nrows], nback[t]) * weights[:, j:j + 1]
            tok[t] = value.astype(BF16)

    def give_far(g):
        _, _, finish, value = sums[g]
        finish()
        for k in far[g]:
            r = chunk(k)
            esum[r, :] = value(r).astype(BF16)
            go(push(esum.at[r], back.at[r], br.at[1 + g], ep=k))

    def take_far(g):
        r = span(far[g])
        push(back.at[r], back.at[r], br.at[1 + g], ep=1).wait_recv()
        value = jnp.zeros((length, cols), F32)
        for j in range(hits.shape[0]):
            value += dot(hits[j, :, r], back[r, :]) * weights[:, j:j + 1]
        return value

    scores = scores_ref[...]
    weights = dot(eye.astype(F32), scores / jnp.sum(scores, axis=0, keepdims=True), ((1,), (1,)), precision=HIGHEST)

    for step in range(heads // per):
        mix_step(step)
    go(swap)
    for load in loads[4:7]:
        load.wait()
    poll(len(agenda) - far_end)
    poll(2)
    join_states()
    feed(near[:-1])
    upward(near[:-1], polls=(2,))
    feed(near[-1:])
    upward(near[-1:], skip=len(near) - 1)
    downward(near, polls=(1, 2))
    give_near()
    poll(len(agenda) - 1)
    fold_states()
    finish_mixer()
    mixsum[0](slice(0, 2))
    for g, chunks in enumerate(far):
        feed(chunks)
        upward(chunks, polls=(1,))
        if g:
            sums[g - 1][1]()
        downward(chunks)
        if g == 0:
            poll(len(agenda))
        sums[g][0]()
    mixsum[0](slice(2, 4))
    for g in range(len(far) - 1):
        give_far(g)
    sums[-1][1]()
    mixsum[1]()
    take_near()
    toksum[0]()
    give_far(len(far) - 1)
    toksum[1]()
    value = take_far(0)
    for g in range(1, len(far)):
        value += take_far(g)
    total[...] = value
    mixsum[2]()
    mix_out[...] = mixsum[3](slice(0, length)).astype(BF16)
    toksum[2]()
    moe_out[...] = (total[...] + toksum[3](slice(0, length))).astype(BF16)

    for copy in sent:
        copy.wait_send()
    for k in range(PAIR, eps, PAIR):
        @pl.when(ep_peer[k] > me)
        def _():
            joined_copy(k).wait_send()


def place_kernel(a_ref, b_ref, a_out, b_out, sem):
    copies = [pltpu.make_async_copy(a_ref, a_out, sem.at[0]), pltpu.make_async_copy(b_ref, b_out, sem.at[1])]
    for copy in copies:
        copy.start()
    for copy in copies:
        copy.wait()


def whole_block(mix_rows, mix_gain, wq, wf, wi, wo, gap, dec, hgain, wm, moe_rows, moe_gain, ids, scores, wg, wu, wd):
    eps, tps = lax.axis_size("ep"), lax.axis_size("tp")
    length, cols = mix_rows.shape
    top = ids.shape[1]
    cap = length * top * 3 // (2 * eps)
    rows = eps * cap
    heads = dec.shape[0]
    width = wq.shape[1]
    dim = width // heads
    depth, units = wg.shape[1:]
    dma = lambda *s: pltpu.SemaphoreType.DMA(s)
    out = jax.ShapeDtypeStruct((length, cols), BF16)
    scratch = [
        pltpu.VMEM((depth // 128, 128), BF16), pltpu.VMEM((1, width), F32), pltpu.VMEM(dec.shape, F32),
        pltpu.VMEM((1, dim), BF16), pltpu.VMEM((depth // 128, 128), BF16),
        pltpu.VMEM((top, length), jnp.int32), pltpu.VMEM((top, length), F32),
        pltpu.VMEM((length, cols), BF16), pltpu.VMEM((length, cols), BF16),
        pltpu.VMEM((4, depth, width), BF16), pltpu.VMEM((width, depth), BF16),
        pltpu.VMEM((depth, units), BF16), pltpu.VMEM((depth, units), BF16), pltpu.VMEM((units, depth), BF16),
        pltpu.VMEM((tps, length, cols), BF16), pltpu.VMEM((4, length, width), F32),
        pltpu.VMEM((length, width), F32), pltpu.VMEM((length, width), BF16), pltpu.VMEM((length, width), F32),
        pltpu.VMEM((heads, dim + 16, dim), BF16), pltpu.VMEM((heads, dim + 16, dim), BF16),
        pltpu.VMEM((heads // 2, dim + 16, dim), BF16), pltpu.VMEM((heads, dim, dim), BF16),
        pltpu.VMEM((eps // PAIR, heads // 2, dim + 16, dim), BF16),
        pltpu.VMEM((length, width), BF16), pltpu.VMEM((tps, length, cols), BF16), pltpu.VMEM((tps, length, cols), BF16),
        pltpu.VMEM((tps, rows, cols), BF16), pltpu.VMEM((rows, cols), BF16), pltpu.VMEM((top, length, rows), BF16),
        pltpu.VMEM((rows, depth), BF16), pltpu.VMEM((rows // 2, units), BF16),
        pltpu.VMEM((tps, rows, cols), BF16), pltpu.VMEM((tps, rows, cols), BF16),
        pltpu.VMEM((tps, rows // 2, cols), BF16), pltpu.VMEM((tps, length, cols), BF16), pltpu.VMEM((tps, length, cols), BF16),
        pltpu.VMEM((rows, cols), BF16), pltpu.VMEM((rows, cols), BF16), pltpu.VMEM((length, cols), F32),
        dma(14), pltpu.SemaphoreType.REGULAR, dma(1), dma(3), dma(eps), dma(eps, 3), dma(eps // 4, 3), dma(1 + eps // 4),
        dma(2 + eps // PAIR), dma(3), dma(3),
    ]
    results = pl.pallas_call(
        functools.partial(block_kernel, cap),
        in_specs=[pl.BlockSpec(memory_space=pltpu.HBM)] * 17,
        out_specs=[VMEM, VMEM],
        out_shape=[pltpu.VMEM((length, cols), BF16)] * 2,
        scratch_shapes=scratch,
        compiler_params=pltpu.CompilerParams(vmem_limit_bytes=LIMIT, collective_id=0, has_side_effects=True),
    )(mix_rows, mix_gain.reshape(-1, 128), wq, wf, wi, wo, gap.reshape(1, -1), dec, hgain.reshape(1, -1), wm,
      moe_rows, moe_gain.reshape(-1, 128), ids.T, scores.T, wg, wu, wd)
    return pl.pallas_call(
        place_kernel,
        in_specs=[VMEM, VMEM],
        out_specs=[ANY, ANY],
        out_shape=[out, out],
        scratch_shapes=[dma(2)],
        compiler_params=pltpu.CompilerParams(vmem_limit_bytes=1024 * 1024),
    )(*results)


def fits(eps, tps, mix_rows, dec, route_ids, w_gate):
    tokens, cols = mix_rows.shape
    top = route_ids.shape[1]
    cap = tokens * top * 3 // (2 * eps)
    square = tps == 4 and dec.shape[0] % 2 == 0 and eps >= 4 and eps & (eps - 1) == 0
    aligned = cap % 32 == 0 and cols % 128 == 0 and tokens % (2 * BLOCK) == 0 and w_gate.shape[2] % 128 == 0
    return square and aligned and w_gate.shape[0] == 1


def per_device(mix_rows, mix_gain, w_query, w_forget, w_input, w_outgate, forget_gap, decay_extra,
               head_gain, w_mixout, moe_rows, moe_gain, route_ids, route_scores, w_gate, w_up, w_down):
    eps, tps = lax.axis_size("ep"), lax.axis_size("tp")
    if fits(eps, tps, mix_rows, decay_extra, route_ids, w_gate):
        return whole_block(mix_rows, mix_gain, w_query, w_forget, w_input, w_outgate, forget_gap, decay_extra,
                           head_gain, w_mixout, moe_rows, moe_gain, route_ids, route_scores, w_gate, w_up, w_down)
    tokens, top = route_ids.shape
    experts = w_gate.shape[0] * eps
    capacity = tokens * top * 3 // (2 * experts)
    cols = mix_rows.shape[1]
    ids = route_ids.T
    slots = dispatch(ids, moe_rows, experts, capacity)
    arrived = lax.all_to_all(slots.reshape(eps, -1, cols), "ep", split_axis=0, concat_axis=0, tiled=True)
    gathered = lax.all_gather(arrived.reshape(-1, cols), "tp", axis=0)
    mix_whole = lax.all_gather(mix_rows, "tp", axis=0)
    lo, qd, og, st = mixer(mix_whole, mix_gain, w_query, w_forget, w_input, w_outgate, forget_gap, decay_extra.T)
    product = experts_call(gathered, moe_gain, w_gate, w_up, w_down)
    expert_sum = lax.psum_scatter(product, "tp", scatter_dimension=0)
    states = lax.all_gather(st, "ep", axis=0)
    mixed = tail(states, lo, qd, og, head_gain, w_mixout, tps)
    mix_out = lax.psum_scatter(mixed, "tp", scatter_dimension=0)
    back = lax.all_to_all(expert_sum.reshape(eps, -1, cols), "ep", split_axis=0, concat_axis=0, tiled=True)
    moe_out = combine(ids, route_scores, back.reshape(-1, cols), experts, capacity)
    return (mix_out, moe_out)


def solution(mesh):
    placed = (
        P("ep", "tp"), P(), P(None, "tp"), P(None, "tp"), P(None, "tp"), P(None, "tp"), P("tp"),
        P("tp", "ep"), P(), P("tp", None), P("ep", "tp"), P(), P("ep", None), P("ep", None),
        P("ep", None, "tp"), P("ep", None, "tp"), P("ep", "tp", None),
    )
    return jax.shard_map(
        per_device, mesh=mesh, in_specs=placed,
        out_specs=(P("ep", "tp"), P("ep", "tp")), check_vma=False,
    )
```
